128 devices in a mesh: sp: 16 (over z, y), dp: 8 (over x, core).
Axes of the slice: x: 4, y: 4, z: 4, core: 2. Of those that a mesh axis runs over, the one named last changes fastest.
Arguments:
- query: bfloat16 [8, 3072, 3072], P('dp', 'sp'), may hold values from -18 to 18
- latent: bfloat16 [8, 3072, 1024], P('dp', 'sp'), may hold values from -6 to 6
- rope_key: bfloat16 [8, 3072, 32], P('dp', 'sp'), may hold values from -5 to 5
- latent_norm_gain: float32 [1024], replicated, may hold values from 0.1 to 1.9
- key_up_matrix: bfloat16 [2048, 1024], P('dp'), may hold values from -0.1875 to 0.1875
- value_up_matrix: bfloat16 [2048, 1024], P('dp'), may hold values from -0.1875 to 0.1875
- out_grad: bfloat16 [8, 3072, 2048], P('dp', 'sp'), may hold values from -6 to 6
Outputs:
- query_grad: bfloat16 [8, 3072, 3072], P('dp', 'sp')
- latent_grad: float32 [8, 3072, 1024], P('dp', 'sp')
- rope_key_grad: float32 [8, 3072, 32], P('dp', 'sp')
- key_weight_grad: float32 [2048, 1024], P('dp')
- value_weight_grad: float32 [2048, 1024], P('dp')
- gain_grad: float32 [1024], replicated
The draws below stay inside these ranges and needn't reach their ends.
All inputs are finite; a program needn't handle non-finite values.
Results may differ from the reference program's by a relative error of at most 0.011.
Values may be sent and summed in bfloat16 or wider, within the bound.
No kernel may reach another device: no remote copies, remote signals or barrier semaphores. Data moves between devices by JAX's collectives and lax.ppermute only.
A program may use at most 256 MiB of HBM per device.

```python
import jax
import jax.numpy as jnp
from jax import lax

ATTENTION_HEADS = 32
PLAIN_HEAD_WIDTH = 64
ROPE = 32
VALUE_HEAD_WIDTH = 64
LATENT_WIDTH = 1024
SPAN = 64
SEQUENCE_LENGTH = 3072
BATCH_SEQUENCES = 8


def draw_rope_key(key, part):
    own = jax.random.fold_in(key, 11)
    values = jnp.clip(jax.random.normal(own, (BATCH_SEQUENCES, SEQUENCE_LENGTH, ROPE), jnp.float32), -5.0, 5.0)
    return values.astype(jnp.bfloat16)


def draw_query(key, part):
    own = jax.random.fold_in(key, 23)
    shape = (BATCH_SEQUENCES, SEQUENCE_LENGTH, ATTENTION_HEADS, PLAIN_HEAD_WIDTH + ROPE)
    values = jnp.clip(jax.random.normal(own, shape, jnp.float32), -5.0, 5.0)
    return values.reshape(BATCH_SEQUENCES, SEQUENCE_LENGTH, ATTENTION_HEADS * (PLAIN_HEAD_WIDTH + ROPE)).astype(jnp.bfloat16)


def block_scale(own_key, shape, split, least, high):
    loudness, own = 1.0, jax.random.fold_in(own_key, 6)
    for axis_at, blocks in split:
        steps = jnp.exp(jax.random.uniform(jax.random.fold_in(own, axis_at), (blocks,), jnp.float32, least / len(split), high / len(split)))
        loudness = loudness * jnp.repeat(steps, shape[axis_at] // blocks).reshape([-1 if axis == axis_at else 1 for axis in range(len(shape))])
    return loudness


def centred(rng, dims, scale, reach, split=(), held_as=jnp.bfloat16):
    result = scale * jax.random.normal(rng, dims, jnp.float32)
    if split:
        result = result * block_scale(rng, dims, split, -0.22, 0.18)
    return jnp.clip(result, -reach, reach).astype(held_as)


def setup_inputs(seed: int = 0) -> dict:
    streams_of = jax.random.split(jax.random.key(seed), 8)
    query = draw_query(jax.random.fold_in(streams_of[7], 71), 0)
    latent = centred(streams_of[1], (BATCH_SEQUENCES, SEQUENCE_LENGTH, LATENT_WIDTH), 1.0, 6.0, ((0, 8), (1, 16)))
    rope_key = draw_rope_key(jax.random.fold_in(streams_of[7], 71), 0)
    latent_norm_gain = jnp.clip(1.0 + 0.18 * jax.random.normal(streams_of[3], (LATENT_WIDTH,), jnp.float32), 0.1, 1.9)
    key_up_matrix = centred(streams_of[4], (ATTENTION_HEADS * PLAIN_HEAD_WIDTH, LATENT_WIDTH), LATENT_WIDTH ** -0.5, 0.1875, ((0, 8),))
    value_up_matrix = centred(streams_of[5], (ATTENTION_HEADS * VALUE_HEAD_WIDTH, LATENT_WIDTH), LATENT_WIDTH ** -0.5, 0.1875, ((0, 8),))
    out_grad = centred(streams_of[6], (BATCH_SEQUENCES, SEQUENCE_LENGTH, ATTENTION_HEADS * VALUE_HEAD_WIDTH), 1.0, 6.0, ((0, 8), (1, 16)))
    return {"query": query, "latent": latent, "rope_key": rope_key, "latent_norm_gain": latent_norm_gain, "key_up_matrix": key_up_matrix, "value_up_matrix": value_up_matrix, "out_grad": out_grad}


eps = 1e-06
rope_base = 10000.0

def rotate(values, cosine, sine):
    half = values.shape[-1] // 2
    first = values[..., :half]
    second = values[..., half:]
    return jnp.concatenate([first * cosine - second * sine, second * cosine + first * sine], axis=-1)

def angles(length, width):
    inverse = 1.0 / rope_base ** (jnp.arange(0, width, 2, dtype=jnp.float32) / width)
    turned = jnp.arange(length, dtype=jnp.float32)[:, None] * inverse[None, :]
    return (jnp.cos(turned), jnp.sin(turned))

def reference(query, latent, rope_key, latent_norm_gain, key_up_matrix, value_up_matrix, out_grad):
    f32 = jnp.float32
    bf16 = jnp.bfloat16
    length = SEQUENCE_LENGTH
    width = PLAIN_HEAD_WIDTH + ROPE
    scale = width ** (-0.5)
    block = 512 if length % 512 == 0 else length
    cosine, sine = angles(length, ROPE)
    neg = jnp.finfo(f32).min

    def one_sequence(inputs):
        seq_query, seq_latent, seq_rope, seq_grad = inputs
        lat = seq_latent.astype(f32)
        inv_rms = lax.rsqrt(lax.optimization_barrier(jnp.mean(lat * lat, axis=-1, keepdims=True)) + eps)
        normed = lat * inv_rms
        nlat = (normed * latent_norm_gain).astype(bf16)
        key_nope = jnp.dot(nlat, key_up_matrix.T, preferred_element_type=f32).astype(bf16).reshape(length, ATTENTION_HEADS, PLAIN_HEAD_WIDTH)
        values = jnp.dot(nlat, value_up_matrix.T, preferred_element_type=f32).astype(bf16).reshape(length, ATTENTION_HEADS, VALUE_HEAD_WIDTH)
        heads_query = seq_query.reshape(length, ATTENTION_HEADS, width)
        q_nope = heads_query[:, :, :PLAIN_HEAD_WIDTH]
        q_rope = rotate(heads_query[:, :, PLAIN_HEAD_WIDTH:].astype(f32), cosine[:, None, :], sine[:, None, :]).astype(bf16)
        k_rope = rotate(seq_rope.astype(f32), cosine, sine).astype(bf16)
        d_out = seq_grad.reshape(length, ATTENTION_HEADS, VALUE_HEAD_WIDTH)
        dk_nope = jnp.zeros((length, ATTENTION_HEADS, PLAIN_HEAD_WIDTH), f32)
        dk_rope = jnp.zeros((length, ROPE), f32)
        d_vals = jnp.zeros((length, ATTENTION_HEADS, VALUE_HEAD_WIDTH), f32)
        dq_parts = []
        for begin in range(0, length, block):
            end = begin + block
            qn = q_nope[begin:end].astype(f32)
            qr = q_rope[begin:end].astype(f32)
            go = d_out[begin:end].astype(f32)
            kn = key_nope[:end].astype(f32)
            kr = k_rope[:end].astype(f32)
            vv = values[:end].astype(f32)
            scores = (jnp.einsum('qhd,khd->hqk', qn, kn) + jnp.einsum('qhd,kd->hqk', qr, kr)) * scale
            q_seg = jnp.arange(begin, end) // SPAN
            k_seg = jnp.arange(end) // SPAN
            allowed = k_seg[None, :] <= q_seg[:, None]
            scores = jnp.where(allowed[None], scores, neg)
            probs = jax.nn.softmax(scores, axis=-1)
            d_probs = jnp.einsum('qhd,khd->hqk', go, vv)
            d_scores = probs * (d_probs - lax.optimization_barrier(jnp.sum(probs * d_probs, axis=-1, keepdims=True)))
            ds_b = d_scores.astype(bf16).astype(f32)
            p_b = probs.astype(bf16).astype(f32)
            dq_n = jnp.einsum('hqk,khd->qhd', ds_b, kn) * scale
            dq_r = jnp.einsum('hqk,kd->qhd', ds_b, kr) * scale
            dq_r = rotate(dq_r, cosine[begin:end, None, :], -sine[begin:end, None, :])
            dq_parts.append(jnp.concatenate([dq_n, dq_r], axis=-1).astype(bf16))
            dk_nope = dk_nope.at[:end].add(jnp.einsum('hqk,qhd->khd', ds_b, qn) * scale)
            dk_rope = dk_rope.at[:end].add(jnp.einsum('hqk,qhd->kd', ds_b, qr) * scale)
            d_vals = d_vals.at[:end].add(jnp.einsum('hqk,qhd->khd', p_b, go))
        query_grad = jnp.concatenate(dq_parts, axis=0).reshape(length, ATTENTION_HEADS * width)
        rope_grad = rotate(dk_rope, cosine, -sine)
        dk_b = dk_nope.astype(bf16).reshape(length, ATTENTION_HEADS * PLAIN_HEAD_WIDTH)
        dv_b = d_vals.astype(bf16).reshape(length, ATTENTION_HEADS * VALUE_HEAD_WIDTH)
        d_nlat = jnp.dot(dk_b, key_up_matrix, preferred_element_type=f32) + jnp.dot(dv_b, value_up_matrix, preferred_element_type=f32)
        key_part = jnp.dot(dk_b.T, nlat, preferred_element_type=f32)
        value_part = jnp.dot(dv_b.T, nlat, preferred_element_type=f32)
        gain_part = lax.optimization_barrier(jnp.sum(d_nlat * normed, axis=0))
        scaled = d_nlat * latent_norm_gain
        latent_grad = inv_rms * (scaled - normed * lax.optimization_barrier(jnp.mean(scaled * normed, axis=-1, keepdims=True)))
        return (query_grad, latent_grad, rope_grad, key_part, value_part, gain_part)
    results = lax.map(one_sequence, (query, latent, rope_key, out_grad))
    query_grad, latent_grad, rope_grad, key_parts, value_parts, gain_parts = results
    return (query_grad, latent_grad, rope_grad, lax.optimization_barrier(jnp.sum(key_parts, axis=0)), lax.optimization_barrier(jnp.sum(value_parts, axis=0)), lax.optimization_barrier(jnp.sum(gain_parts, axis=0)))
```

```python
import functools

import jax
import jax.numpy as jnp
import numpy as np
from jax import lax
from jax.experimental import pallas as pl
from jax.experimental.pallas import tpu as pltpu
from jax.sharding import Mesh
from jax.sharding import PartitionSpec as P

ATTENTION_HEADS = 32
PLAIN = 64
ROPE = 32
HALF = ROPE // 2
WIDTH = PLAIN + ROPE
LATENT = 1024
SPAN = 64
LENGTH = 3072
DP = ("dp_0", "dp_1")
SP = ("sp_0", "sp_1")
ALL = SP + DP
NSP = 16
NDP = 8
TOKENS = LENGTH // NSP
BLOCK = 512
SCALE = WIDTH**-0.5
LOG2E = 1.4426950408889634

eps = 1e-06
rope_base = 10000.0
f32 = jnp.float32
bf16 = jnp.bfloat16


def angles(positions):
    inverse = 1.0 / rope_base ** (jnp.arange(0, ROPE, 2, dtype=f32) / ROPE)
    turned = positions.astype(f32)[:, None] * inverse[None, :]
    return jnp.cos(turned), jnp.sin(turned)


def lanes_of(shape):
    return lax.broadcasted_iota(jnp.int32, shape, 1)


def pack_body(q_ref, g_ref, kr_ref, cos_ref, sin_ref, out_ref):
    lane = lanes_of((TOKENS, 128))
    cosine = cos_ref[...]
    sine = sin_ref[...]

    def turn(x):
        inside = (lane % ROPE) < HALF
        swapped = jnp.where(inside, pltpu.roll(x, 128 - HALF, 1), pltpu.roll(x, HALF, 1))
        return x * cosine + swapped * sine

    key = turn(kr_ref[...])
    key = pltpu.roll(key, ROPE, 1)

    def emit(slot, qn0, qr0, qn1, qr1, grads):
        first = jnp.where(lane < PLAIN, qn0, pltpu.roll(grads, PLAIN, 1))
        second = jnp.where(lane < PLAIN, qn1, grads)
        third = turn(jnp.where(lane < ROPE, qr0, jnp.where(lane >= 96, qr1, 0.0)))
        third = jnp.where((lane >= ROPE) & (lane < 2 * ROPE), key, third)
        out_ref[slot, :, 0:128] = first.astype(bf16)
        out_ref[slot, :, 128:256] = second.astype(bf16)
        out_ref[slot, :, 256:384] = third.astype(bf16)

    for pair in range(NSP // 2):
        a0, a1, a2 = [
            q_ref[:, 384 * pair + 128 * k : 384 * pair + 128 * (k + 1)].astype(f32) for k in range(3)
        ]
        g0 = g_ref[:, 256 * pair : 256 * pair + 128].astype(f32)
        g1 = g_ref[:, 256 * pair + 128 : 256 * pair + 256].astype(f32)
        qn1 = jnp.where(lane < ROPE, pltpu.roll(a0, ROPE, 1), pltpu.roll(a1, ROPE, 1))
        emit(2 * pair, a0, pltpu.roll(a0, 64, 1), qn1, pltpu.roll(a1, 64, 1), g0)
        emit(2 * pair + 1, pltpu.roll(a1, 64, 1), a2, pltpu.roll(a2, 96, 1), a2, g1)


def pack(query, grads, key, cosine, sine):
    return pl.pallas_call(
        pack_body,
        out_shape=jax.ShapeDtypeStruct((NSP, TOKENS, 384), bf16),
        cost_estimate=pl.CostEstimate(flops=2_000_000_000, bytes_accessed=5_000_000, transcendentals=0),
        name="pack",
    )(query, grads, key, cosine, sine)


def attend_body(head, qd_ref, kv_ref, cos_ref, sin_ref, out_ref, p_buf, dp_buf, m_buf, kt_buf, acc, dq_acc):
    blocks = LENGTH // BLOCK
    lane = lanes_of((BLOCK, 128))
    factor = SCALE * LOG2E
    tile = 128 * head
    low = 0 if head == 0 else 96

    def prepare(j, carry):
        rows = pl.ds(pl.multiple_of(j * BLOCK, BLOCK), BLOCK)
        kt = kv_ref[rows, :].astype(f32).T
        rt = qd_ref[rows, 256:384].astype(f32).T
        kt_buf[:, rows] = jnp.concatenate([kt[0:PLAIN], rt[ROPE : 2 * ROPE]], axis=0).astype(bf16)
        acc[rows, :] = jnp.zeros((BLOCK, 256), f32)
        return carry

    lax.fori_loop(0, blocks, prepare, 0)
    key_seg = lax.broadcasted_iota(jnp.int32, (BLOCK, BLOCK), 0) // SPAN
    query_seg = lax.broadcasted_iota(jnp.int32, (BLOCK, BLOCK), 1) // SPAN
    allowed = key_seg <= query_seg

    def one_block(i, carry):
        rows = pl.ds(pl.multiple_of(i * BLOCK, BLOCK), BLOCK)
        qd = qd_ref[rows, tile : tile + 128].astype(f32)
        rt = qd_ref[rows, 256:384].astype(f32)
        qdt = qd.T
        rtt = rt.T
        none = jnp.zeros((32, BLOCK), f32)
        left = jnp.concatenate(
            [qdt[0:PLAIN], none, none, none, rtt[low : low + ROPE], none, none], axis=0
        ).astype(bf16)
        left_d = jnp.concatenate([none, none, qdt[PLAIN:128]], axis=0).astype(bf16)
        right = jnp.concatenate(
            [jnp.where(lane < PLAIN, qd, 0.0), jnp.where((lane >= low) & (lane < low + ROPE), rt, 0.0)], axis=1
        ).astype(bf16)
        right_d = jnp.where(lane < PLAIN, 0.0, qd).astype(bf16)

        def gather_stats(j, stats, masked):
            top, total, inner = stats
            keys = pl.ds(pl.multiple_of(j * BLOCK, BLOCK), BLOCK)
            kv = kv_ref[keys, :]
            both = jnp.concatenate([kv, qd_ref[keys, 256:384]], axis=1)
            scores = jnp.dot(both, left, preferred_element_type=f32) * factor
            if masked:
                scores = jnp.where(allowed, scores, -jnp.inf)
            d_probs = jnp.dot(kv, left_d, preferred_element_type=f32)
            new_top = jnp.maximum(top, jnp.max(scores, axis=0, keepdims=True))
            probs = jnp.exp2(scores - new_top)
            shrink = jnp.exp2(top - new_top)
            total = total * shrink + jnp.sum(probs, axis=0, keepdims=True)
            inner = inner * shrink + jnp.sum(probs * d_probs, axis=0, keepdims=True)
            p_buf[keys, :] = probs
            dp_buf[keys, :] = d_probs
            m_buf[j] = jnp.broadcast_to(new_top, (8, BLOCK))
            return new_top, total, inner

        start = (
            jnp.full((1, BLOCK), jnp.finfo(f32).min, f32),
            jnp.zeros((1, BLOCK), f32),
            jnp.zeros((1, BLOCK), f32),
        )
        stats = lax.fori_loop(0, i, functools.partial(gather_stats, masked=False), start)
        top, total, inner = gather_stats(i, stats, True)
        inverse = 1.0 / total
        inner = inner * inverse
        dq_acc[...] = jnp.zeros((WIDTH, BLOCK), f32)

        def gradients(j, carry):
            keys = pl.ds(pl.multiple_of(j * BLOCK, BLOCK), BLOCK)
            grow = jnp.exp2(m_buf[j][0:1] - top) * inverse
            probs = p_buf[keys, :] * grow
            ds = (probs * (dp_buf[keys, :] - inner)).astype(bf16)
            pb = probs.astype(bf16)
            dq_acc[...] += jnp.dot(kt_buf[:, keys], ds, preferred_element_type=f32)
            acc[keys, :] += jnp.dot(ds, right, preferred_element_type=f32)
            acc[keys, 0:128] += jnp.dot(pb, right_d, preferred_element_type=f32)
            return carry

        lax.fori_loop(0, i + 1, gradients, 0)
        dq = dq_acc[...] * SCALE
        cosine = cos_ref[:, rows]
        sine = sin_ref[:, rows]
        first, second = dq[PLAIN : PLAIN + HALF], dq[PLAIN + HALF : WIDTH]
        pieces = [dq[0:PLAIN], first * cosine + second * sine, second * cosine - first * sine]
        pieces = [none] + pieces if head == 0 else pieces + [none]
        out_ref[rows, 128:256] = jnp.concatenate(pieces, axis=0).T.astype(bf16)
        return carry

    lax.fori_loop(0, blocks, one_block, 0)

    def finish(j, carry):
        rows = pl.ds(pl.multiple_of(j * BLOCK, BLOCK), BLOCK)
        plain = acc[rows, 0:128]
        out_ref[rows, 0:128] = jnp.where(lane < PLAIN, plain * SCALE, plain).astype(bf16)
        turned = acc[rows, 128:256] * SCALE
        kept = out_ref[rows, 128:256].astype(f32)
        mine = (lane >= low) & (lane < low + ROPE)
        out_ref[rows, 128:256] = jnp.where(mine, turned, kept).astype(bf16)
        return carry

    lax.fori_loop(0, blocks, finish, 0)


def attend(head, arrived, kv, cosine, sine):
    return pl.pallas_call(
        functools.partial(attend_body, head),
        grid=(1,),
        in_specs=[
            pl.BlockSpec((LENGTH, 384), lambda g: (0, 0)),
            pl.BlockSpec((LENGTH, 128), lambda g: (0, head)),
            pl.BlockSpec((HALF, LENGTH), lambda g: (0, 0)),
            pl.BlockSpec((HALF, LENGTH), lambda g: (0, 0)),
        ],
        out_specs=pl.BlockSpec((LENGTH, 256), lambda g: (0, 0)),
        out_shape=jax.ShapeDtypeStruct((LENGTH, 256), bf16),
        scratch_shapes=[
            pltpu.VMEM((LENGTH, BLOCK), f32),
            pltpu.VMEM((LENGTH, BLOCK), f32),
            pltpu.VMEM((LENGTH // BLOCK, 8, BLOCK), f32),
            pltpu.VMEM((WIDTH, LENGTH), bf16),
            pltpu.VMEM((LENGTH, 256), f32),
            pltpu.VMEM((WIDTH, BLOCK), f32),
        ],
        compiler_params=pltpu.CompilerParams(vmem_limit_bytes=48 * 1024 * 1024),
        cost_estimate=pl.CostEstimate(
            flops=12_000_000_000, bytes_accessed=6_000_000, transcendentals=5_000_000
        ),
        name=f"attend{head}",
    )(arrived, kv, cosine, sine)


def finish_body(r0_ref, r1_ref, w_ref, lat_ref, gain_ref, cos_ref, sin_ref, dq_ref, dlat_ref, drope_ref, acc, rope):
    step = pl.program_id(0)
    lane = lanes_of((TOKENS, 128))

    @pl.when(step == 0)
    def _():
        acc[...] = jnp.zeros_like(acc)
        rope[...] = jnp.zeros_like(rope)

    tiles = []
    for half in range(2):
        r0 = r0_ref[half]
        r1 = r1_ref[half]
        both = jnp.concatenate([r0[:, 0:128], r1[:, 0:128]], axis=1)
        acc[...] += jnp.dot(both, w_ref[half], preferred_element_type=f32)
        t0 = r0[:, 128:256].astype(f32)
        t1 = r1[:, 128:256].astype(f32)
        rope[...] += jnp.where(lane < ROPE, t0, jnp.where(lane >= 96, t1, 0.0))
        tiles.append((t0, t1))
    (x0, x1), (y0, y1) = tiles
    dq_ref[:, 0:128] = jnp.where(lane < 96, pltpu.roll(x0, 96, 1), pltpu.roll(x1, 96, 1)).astype(bf16)
    dq_ref[:, 128:256] = jnp.where(lane < 64, pltpu.roll(x1, 96, 1), pltpu.roll(y0, 32, 1)).astype(bf16)
    dq_ref[:, 256:384] = jnp.where(lane < 32, pltpu.roll(y0, 32, 1), pltpu.roll(y1, 32, 1)).astype(bf16)

    @pl.when(step == NSP // 2 - 1)
    def _():
        lat = lat_ref[...].astype(f32)
        inv_rms = lax.rsqrt(jnp.mean(lat * lat, axis=-1, keepdims=True) + eps)
        normed = lat * inv_rms
        scaled = acc[...] * gain_ref[...]
        dlat_ref[...] = inv_rms * (scaled - normed * jnp.mean(scaled * normed, axis=-1, keepdims=True))
        x = rope[...]
        x = x + pltpu.roll(x, 32, 1)
        swapped = jnp.where(lane < HALF, pltpu.roll(x, 128 - HALF, 1), pltpu.roll(x, HALF, 1))
        drope_ref[...] = (x * cos_ref[...] - swapped * sin_ref[...])[:, 0:ROPE]


def finish(r0, r1, weights, latent, gain, cosine, sine):
    half = NSP // 2
    return pl.pallas_call(
        finish_body,
        grid=(half,),
        in_specs=[
            pl.BlockSpec((2, TOKENS, 256), lambda g: (g, 0, 0)),
            pl.BlockSpec((2, TOKENS, 256), lambda g: (g, 0, 0)),
            pl.BlockSpec((2, 256, LATENT), lambda g: (g, 0, 0)),
            pl.BlockSpec((TOKENS, LATENT), lambda g: (0, 0)),
            pl.BlockSpec((1, LATENT), lambda g: (0, 0)),
            pl.BlockSpec((TOKENS, 128), lambda g: (0, 0)),
            pl.BlockSpec((TOKENS, 128), lambda g: (0, 0)),
        ],
        out_specs=[
            pl.BlockSpec((TOKENS, 384), lambda g: (0, g)),
            pl.BlockSpec((TOKENS, LATENT), lambda g: (0, 0)),
            pl.BlockSpec((TOKENS, ROPE), lambda g: (0, 0)),
        ],
        out_shape=[
            jax.ShapeDtypeStruct((TOKENS, ATTENTION_HEADS * WIDTH), bf16),
            jax.ShapeDtypeStruct((TOKENS, LATENT), f32),
            jax.ShapeDtypeStruct((TOKENS, ROPE), f32),
        ],
        scratch_shapes=[pltpu.VMEM((TOKENS, LATENT), f32), pltpu.VMEM((TOKENS, 128), f32)],
        cost_estimate=pl.CostEstimate(flops=2_000_000_000, bytes_accessed=14_000_000, transcendentals=0),
        name="finish",
    )(r0, r1, weights, latent, gain, cosine, sine)


def to_heads():
    return [(NDP * a + d, NDP * (2 * d + a // 8) + a % 8) for a in range(NSP) for d in range(NDP)]


def to_rows():
    return [(b, a) for a, b in to_heads()]


def everyone(value, axes, size):
    return lax.all_to_all(jnp.broadcast_to(value[None], (size, *value.shape)), axes, 0, 0, tiled=True)


def local(query, latent, rope_key, gain, key_up, value_up, out_grad):
    place = lax.axis_index(SP)
    gain_row = gain[None, :]
    lat = latent[0].astype(f32)
    inv_rms = lax.rsqrt(jnp.mean(lat * lat, axis=-1, keepdims=True) + eps)
    nlat = (lat * inv_rms * gain_row).astype(bf16)
    nlat_all = lax.all_gather(nlat, SP, axis=0, tiled=True)

    rows = jnp.stack([key_up.reshape(4, 64, LATENT), value_up.reshape(4, 64, LATENT)], axis=1)
    rows = rows.reshape(512, LATENT)
    mine = lax.dynamic_slice_in_dim(rows, (place // 8) * 256, 256, axis=0)
    own = lax.ppermute(mine, ALL, to_heads())
    whole = lax.all_gather(rows, DP, axis=0, tiled=True)

    positions = place * TOKENS + jnp.arange(TOKENS)
    cosine, sine = angles(positions)
    cos_lanes = jnp.tile(cosine, (1, 8))
    sin_lanes = jnp.tile(jnp.concatenate([-sine, sine], axis=1), (1, 4))
    key = jnp.pad(rope_key[0].astype(f32), ((0, 0), (0, 96)))
    packed = pack(query[0], out_grad[0], key, cos_lanes, sin_lanes)
    arrived = lax.all_to_all(packed, SP, 0, 0, tiled=True).reshape(LENGTH, 384)

    kv = lax.dot_general(nlat_all, own, (((1,), (1,)), ((), ())), preferred_element_type=f32).astype(bf16)
    cos_all, sin_all = angles(jnp.arange(LENGTH))
    cos_all, sin_all = cos_all.T, sin_all.T
    g0 = attend(0, arrived, kv, cos_all, sin_all)
    r0 = lax.all_to_all(g0.reshape(NSP, TOKENS, 256), SP, 0, 0, tiled=True)
    g1 = attend(1, arrived, kv, cos_all, sin_all)
    r1 = lax.all_to_all(g1.reshape(NSP, TOKENS, 256), SP, 0, 0, tiled=True)

    parts = [
        lax.dot_general(g[:, 0:128], nlat_all, (((0,), (0,)), ((), ())), preferred_element_type=f32)
        for g in (g0, g1)
    ]
    part = jnp.concatenate(parts, axis=0)
    gain_part = jnp.sum(part * own.astype(f32), axis=0) / gain
    gain_part = everyone(gain_part.reshape(8, 128), DP, NDP).sum(axis=0)
    gain_grad = everyone(gain_part, SP, NSP).sum(axis=0).reshape(LATENT)

    pieces = part.astype(bf16).reshape(2, 2, 4, 16, LATENT).transpose(0, 2, 1, 3, 4).reshape(NDP, 32, LATENT)
    pieces = lax.all_to_all(pieces, DP, 0, 0, tiled=True)
    piece = pieces.astype(f32).sum(axis=0).astype(bf16)
    piece = lax.ppermute(piece, ALL, to_rows())
    grads = everyone(piece, SP, NSP).reshape(NSP, 2, 16, LATENT)
    key_grad = grads[:, 0].reshape(256, LATENT).astype(f32)
    value_grad = grads[:, 1].reshape(256, LATENT).astype(f32)

    dq, dlat, drope = finish(
        r0, r1, whole.reshape(NSP, 256, LATENT), latent[0], gain_row, cos_lanes, sin_lanes
    )
    return dq[None], dlat[None], drope[None], key_grad, value_grad, gain_grad


def solution(mesh):
    split = Mesh(mesh.devices.reshape(4, 4, 4, 2), ("sp_0", "sp_1", "dp_0", "dp_1"))
    in_specs = (
        P(DP, SP, None),
        P(DP, SP, None),
        P(DP, SP, None),
        P(),
        P(DP, None),
        P(DP, None),
        P(DP, SP, None),
    )
    out_specs = (P(DP, SP, None), P(DP, SP, None), P(DP, SP, None), P(DP, None), P(DP, None), P())
    return jax.shard_map(local, mesh=split, in_specs=in_specs, out_specs=out_specs, check_vma=False)
```

```python
import functools

import jax
import jax.numpy as jnp
from jax import lax
from jax.experimental import pallas as pl
from jax.experimental.pallas import tpu as pltpu
from jax.sharding import Mesh
from jax.sharding import PartitionSpec as P

ATTENTION_HEADS = 32
PLAIN = 64
ROPE = 32
HALF = ROPE // 2
WIDTH = PLAIN + ROPE
LATENT = 1024
SPAN = 64
LENGTH = 3072
DP = ("dp_0", "dp_1")
SP = ("sp_0", "sp_1")
ALL = SP + DP
NSP = 16
NDP = 8
TOKENS = LENGTH // NSP
BLOCK = 512
SCALE = WIDTH**-0.5
LOG2E = 1.4426950408889634

eps = 1e-06
rope_base = 10000.0
f32 = jnp.float32
bf16 = jnp.bfloat16


def angles(positions):
    inverse = 1.0 / rope_base ** (jnp.arange(0, ROPE, 2, dtype=f32) / ROPE)
    turned = positions.astype(f32)[:, None] * inverse[None, :]
    return jnp.cos(turned), jnp.sin(turned)


def lanes_of(shape):
    return lax.broadcasted_iota(jnp.int32, shape, 1)


def pack_body(q_ref, g_ref, kr_ref, cos_ref, sin_ref, out_ref, other_ref):
    lane = lanes_of((TOKENS, 128))
    cosine = cos_ref[...]
    sine = sin_ref[...]

    def turn(x):
        inside = (lane % ROPE) < HALF
        swapped = jnp.where(inside, pltpu.roll(x, 128 - HALF, 1), pltpu.roll(x, HALF, 1))
        return x * cosine + swapped * sine

    key = turn(kr_ref[...])
    key = pltpu.roll(key, ROPE, 1)

    def emit(slot, qn0, qr0, qn1, qr1, grads):
        first = jnp.where(lane < PLAIN, qn0, pltpu.roll(grads, PLAIN, 1))
        second = jnp.where(lane < PLAIN, qn1, grads)
        third = turn(jnp.where(lane < ROPE, qr0, jnp.where(lane >= 96, qr1, 0.0)))
        third = jnp.where((lane >= ROPE) & (lane < 2 * ROPE), key, third)
        out_ref[slot, :, 0:128] = first.astype(bf16)
        out_ref[slot, :, 128:256] = third.astype(bf16)
        other_ref[slot] = second.astype(bf16)

    for pair in range(NSP // 2):
        a0, a1, a2 = [
            q_ref[:, 384 * pair + 128 * k : 384 * pair + 128 * (k + 1)].astype(f32) for k in range(3)
        ]
        g0 = g_ref[:, 256 * pair : 256 * pair + 128].astype(f32)
        g1 = g_ref[:, 256 * pair + 128 : 256 * pair + 256].astype(f32)
        qn1 = jnp.where(lane < ROPE, pltpu.roll(a0, ROPE, 1), pltpu.roll(a1, ROPE, 1))
        emit(2 * pair, a0, pltpu.roll(a0, 64, 1), qn1, pltpu.roll(a1, 64, 1), g0)
        emit(2 * pair + 1, pltpu.roll(a1, 64, 1), a2, pltpu.roll(a2, 96, 1), a2, g1)


def pack(query, grads, key, cosine, sine):
    return pl.pallas_call(
        pack_body,
        out_shape=[
            jax.ShapeDtypeStruct((NSP, TOKENS, 256), bf16),
            jax.ShapeDtypeStruct((NSP, TOKENS, 128), bf16),
        ],
        cost_estimate=pl.CostEstimate(flops=2_000_000_000, bytes_accessed=5_000_000, transcendentals=0),
        name="pack",
    )(query, grads, key, cosine, sine)


def attend_body(head, qd_ref, rt_ref, kv_ref, cos_ref, sin_ref, out_ref, p_buf, dp_buf, m_buf, kt_buf, acc, dq_acc):
    blocks = LENGTH // BLOCK
    lane = lanes_of((BLOCK, 128))
    factor = SCALE * LOG2E
    low = 0 if head == 0 else 96

    def prepare(j, carry):
        rows = pl.ds(pl.multiple_of(j * BLOCK, BLOCK), BLOCK)
        kt = kv_ref[rows, :].astype(f32).T
        rt = rt_ref[rows, :].astype(f32).T
        kt_buf[:, rows] = jnp.concatenate([kt[0:PLAIN], rt[ROPE : 2 * ROPE]], axis=0).astype(bf16)
        acc[rows, :] = jnp.zeros((BLOCK, 256), f32)
        return carry

    lax.fori_loop(0, blocks, prepare, 0)
    key_seg = lax.broadcasted_iota(jnp.int32, (BLOCK, BLOCK), 0) // SPAN
    query_seg = lax.broadcasted_iota(jnp.int32, (BLOCK, BLOCK), 1) // SPAN
    allowed = key_seg <= query_seg

    def one_block(i, carry):
        rows = pl.ds(pl.multiple_of(i * BLOCK, BLOCK), BLOCK)
        qd = qd_ref[rows, :].astype(f32)
        rt = rt_ref[rows, :].astype(f32)
        qdt = qd.T
        rtt = rt.T
        none = jnp.zeros((32, BLOCK), f32)
        left = jnp.concatenate(
            [qdt[0:PLAIN], none, none, none, rtt[low : low + ROPE], none, none], axis=0
        ).astype(bf16)
        left_d = jnp.concatenate([none, none, qdt[PLAIN:128]], axis=0).astype(bf16)
        right = jnp.concatenate(
            [jnp.where(lane < PLAIN, qd, 0.0), jnp.where((lane >= low) & (lane < low + ROPE), rt, 0.0)], axis=1
        ).astype(bf16)
        right_d = jnp.where(lane < PLAIN, 0.0, qd).astype(bf16)

        def gather_stats(j, stats, masked):
            top, total, inner = stats
            keys = pl.ds(pl.multiple_of(j * BLOCK, BLOCK), BLOCK)
            kv = kv_ref[keys, :]
            both = jnp.concatenate([kv, rt_ref[keys, :]], axis=1)
            scores = jnp.dot(both, left, preferred_element_type=f32) * factor
            if masked:
                scores = jnp.where(allowed, scores, -jnp.inf)
            d_probs = jnp.dot(kv, left_d, preferred_element_type=f32)
            new_top = jnp.maximum(top, jnp.max(scores, axis=0, keepdims=True))
            probs = jnp.exp2(scores - new_top)
            shrink = jnp.exp2(top - new_top)
            total = total * shrink + jnp.sum(probs, axis=0, keepdims=True)
            inner = inner * shrink + jnp.sum(probs * d_probs, axis=0, keepdims=True)
            p_buf[keys, :] = probs
            dp_buf[keys, :] = d_probs
            m_buf[j] = jnp.broadcast_to(new_top, (8, BLOCK))
            return new_top, total, inner

        start = (
            jnp.full((1, BLOCK), jnp.finfo(f32).min, f32),
            jnp.zeros((1, BLOCK), f32),
            jnp.zeros((1, BLOCK), f32),
        )
        stats = lax.fori_loop(0, i, functools.partial(gather_stats, masked=False), start)
        top, total, inner = gather_stats(i, stats, True)
        inverse = 1.0 / total
        inner = inner * inverse
        dq_acc[...] = jnp.zeros((WIDTH, BLOCK), f32)

        def gradients(j, carry):
            keys = pl.ds(pl.multiple_of(j * BLOCK, BLOCK), BLOCK)
            grow = jnp.exp2(m_buf[j][0:1] - top) * inverse
            probs = p_buf[keys, :] * grow
            ds = (probs * (dp_buf[keys, :] - inner)).astype(bf16)
            pb = probs.astype(bf16)
            dq_acc[...] += jnp.dot(kt_buf[:, keys], ds, preferred_element_type=f32)
            acc[keys, :] += jnp.dot(ds, right, preferred_element_type=f32)
            acc[keys, 0:128] += jnp.dot(pb, right_d, preferred_element_type=f32)
            return carry

        lax.fori_loop(0, i + 1, gradients, 0)
        dq = dq_acc[...] * SCALE
        cosine = cos_ref[:, rows]
        sine = sin_ref[:, rows]
        first, second = dq[PLAIN : PLAIN + HALF], dq[PLAIN + HALF : WIDTH]
        pieces = [dq[0:PLAIN], first * cosine + second * sine, second * cosine - first * sine]
        pieces = [none] + pieces if head == 0 else pieces + [none]
        out_ref[rows, 128:256] = jnp.concatenate(pieces, axis=0).T.astype(bf16)
        return carry

    lax.fori_loop(0, blocks, one_block, 0)

    def finish(j, carry):
        rows = pl.ds(pl.multiple_of(j * BLOCK, BLOCK), BLOCK)
        plain = acc[rows, 0:128]
        out_ref[rows, 0:128] = jnp.where(lane < PLAIN, plain * SCALE, plain).astype(bf16)
        turned = acc[rows, 128:256] * SCALE
        kept = out_ref[rows, 128:256].astype(f32)
        mine = (lane >= low) & (lane < low + ROPE)
        out_ref[rows, 128:256] = jnp.where(mine, turned, kept).astype(bf16)
        return carry

    lax.fori_loop(0, blocks, finish, 0)


def attend(head, arrived, turned, kv, cosine, sine):
    return pl.pallas_call(
        functools.partial(attend_body, head),
        grid=(1,),
        in_specs=[
            pl.BlockSpec((LENGTH, 128), lambda g: (0, 0)),
            pl.BlockSpec((LENGTH, 128), lambda g: (0, 1)),
            pl.BlockSpec((LENGTH, 128), lambda g: (0, head)),
            pl.BlockSpec((HALF, LENGTH), lambda g: (0, 0)),
            pl.BlockSpec((HALF, LENGTH), lambda g: (0, 0)),
        ],
        out_specs=pl.BlockSpec((LENGTH, 256), lambda g: (0, 0)),
        out_shape=jax.ShapeDtypeStruct((LENGTH, 256), bf16),
        scratch_shapes=[
            pltpu.VMEM((LENGTH, BLOCK), f32),
            pltpu.VMEM((LENGTH, BLOCK), f32),
            pltpu.VMEM((LENGTH // BLOCK, 8, BLOCK), f32),
            pltpu.VMEM((WIDTH, LENGTH), bf16),
            pltpu.VMEM((LENGTH, 256), f32),
            pltpu.VMEM((WIDTH, BLOCK), f32),
        ],
        compiler_params=pltpu.CompilerParams(vmem_limit_bytes=48 * 1024 * 1024),
        cost_estimate=pl.CostEstimate(
            flops=12_000_000_000, bytes_accessed=6_000_000, transcendentals=5_000_000
        ),
    )(arrived, turned, kv, cosine, sine)


def finish_body(r0_ref, r1_ref, w_ref, lat_ref, gain_ref, cos_ref, sin_ref, dq_ref, dlat_ref, drope_ref, acc, rope):
    step = pl.program_id(0)
    lane = lanes_of((TOKENS, 128))

    @pl.when(step == 0)
    def _():
        acc[...] = jnp.zeros_like(acc)
        rope[...] = jnp.zeros_like(rope)

    tiles = []
    for half in range(2):
        r0 = r0_ref[half]
        r1 = r1_ref[half]
        both = jnp.concatenate([r0[:, 0:128], r1[:, 0:128]], axis=1)
        acc[...] += jnp.dot(both, w_ref[half], preferred_element_type=f32)
        t0 = r0[:, 128:256].astype(f32)
        t1 = r1[:, 128:256].astype(f32)
        rope[...] += jnp.where(lane < ROPE, t0, jnp.where(lane >= 96, t1, 0.0))
        tiles.append((t0, t1))
    (x0, x1), (y0, y1) = tiles
    dq_ref[:, 0:128] = jnp.where(lane < 96, pltpu.roll(x0, 96, 1), pltpu.roll(x1, 96, 1)).astype(bf16)
    dq_ref[:, 128:256] = jnp.where(lane < 64, pltpu.roll(x1, 96, 1), pltpu.roll(y0, 32, 1)).astype(bf16)
    dq_ref[:, 256:384] = jnp.where(lane < 32, pltpu.roll(y0, 32, 1), pltpu.roll(y1, 32, 1)).astype(bf16)

    @pl.when(step == NSP // 2 - 1)
    def _():
        lat = lat_ref[...].astype(f32)
        inv_rms = lax.rsqrt(jnp.mean(lat * lat, axis=-1, keepdims=True) + eps)
        normed = lat * inv_rms
        scaled = acc[...] * gain_ref[...]
        dlat_ref[...] = inv_rms * (scaled - normed * jnp.mean(scaled * normed, axis=-1, keepdims=True))
        x = rope[...]
        x = x + pltpu.roll(x, 32, 1)
        swapped = jnp.where(lane < HALF, pltpu.roll(x, 128 - HALF, 1), pltpu.roll(x, HALF, 1))
        drope_ref[...] = (x * cos_ref[...] - swapped * sin_ref[...])[:, 0:ROPE]


def finish(r0, r1, weights, latent, gain, cosine, sine):
    half = NSP // 2
    return pl.pallas_call(
        finish_body,
        grid=(half,),
        in_specs=[
            pl.BlockSpec((2, TOKENS, 256), lambda g: (g, 0, 0)),
            pl.BlockSpec((2, TOKENS, 256), lambda g: (g, 0, 0)),
            pl.BlockSpec((2, 256, LATENT), lambda g: (g, 0, 0)),
            pl.BlockSpec((TOKENS, LATENT), lambda g: (0, 0)),
            pl.BlockSpec((1, LATENT), lambda g: (0, 0)),
            pl.BlockSpec((TOKENS, 128), lambda g: (0, 0)),
            pl.BlockSpec((TOKENS, 128), lambda g: (0, 0)),
        ],
        out_specs=[
            pl.BlockSpec((TOKENS, 384), lambda g: (0, g)),
            pl.BlockSpec((TOKENS, LATENT), lambda g: (0, 0)),
            pl.BlockSpec((TOKENS, ROPE), lambda g: (0, 0)),
        ],
        out_shape=[
            jax.ShapeDtypeStruct((TOKENS, ATTENTION_HEADS * WIDTH), bf16),
            jax.ShapeDtypeStruct((TOKENS, LATENT), f32),
            jax.ShapeDtypeStruct((TOKENS, ROPE), f32),
        ],
        scratch_shapes=[pltpu.VMEM((TOKENS, LATENT), f32), pltpu.VMEM((TOKENS, 128), f32)],
        cost_estimate=pl.CostEstimate(flops=2_000_000_000, bytes_accessed=14_000_000, transcendentals=0),
        name="finish",
    )(r0, r1, weights, latent, gain, cosine, sine)


def to_heads():
    return [(NDP * a + d, NDP * (2 * d + a // 8) + a % 8) for a in range(NSP) for d in range(NDP)]


def to_rows():
    return [(b, a) for a, b in to_heads()]


def everyone(value, axes, size):
    return lax.all_to_all(jnp.broadcast_to(value[None], (size, *value.shape)), axes, 0, 0, tiled=True)


def shifted(value, axis, k):
    return lax.ppermute(value, axis, [(i, (i + k) % 4) for i in range(4)])


SWAP = [(0, 1), (1, 0)]


def sum_everywhere(value):
    value = value + lax.ppermute(value, "dp_1", SWAP)
    for axis in ("dp_0", "sp_1", "sp_0"):
        others = [shifted(value, axis, k) for k in (1, 2, 3)]
        value = (value + others[1]) + (others[0] + others[2])
    return value


def reduce_over_rows(pieces):
    across, core = lax.axis_index("dp_0"), lax.axis_index("dp_1")
    pairs = pieces.reshape(4, 2, *pieces.shape[1:])
    kept = lax.dynamic_index_in_dim(pairs, core, 1, keepdims=False)
    given = lax.dynamic_index_in_dim(pairs, 1 - core, 1, keepdims=False)
    given = lax.ppermute(given, "dp_1", SWAP)
    kept = kept.astype(f32) + given.astype(f32)
    total = lax.dynamic_index_in_dim(kept, across, 0, keepdims=False)
    kept = kept.astype(bf16)
    for k in (1, 2, 3):
        sent = lax.dynamic_index_in_dim(kept, (across + k) & 3, 0, keepdims=False)
        total = total + shifted(sent, "dp_0", k).astype(f32)
    return total.astype(bf16)


def program(query, latent, rope_key, gain, key_up, value_up, out_grad):
    place = lax.axis_index(SP)
    gain_row = gain[None, :]
    lat = latent[0].astype(f32)
    inv_rms = lax.rsqrt(jnp.mean(lat * lat, axis=-1, keepdims=True) + eps)
    nlat = (lat * inv_rms * gain_row).astype(bf16)
    nlat_all = lax.all_gather(nlat, SP, axis=0, tiled=True)

    rows = jnp.stack([key_up.reshape(4, 64, LATENT), value_up.reshape(4, 64, LATENT)], axis=1)
    rows = rows.reshape(512, LATENT)
    mine = lax.dynamic_slice_in_dim(rows, (place // 8) * 256, 256, axis=0)
    own = lax.ppermute(mine, ALL, to_heads())
    whole = lax.all_gather(rows, DP, axis=0, tiled=True)

    positions = place * TOKENS + jnp.arange(TOKENS)
    cosine, sine = angles(positions)
    cos_lanes = jnp.tile(cosine, (1, 8))
    sin_lanes = jnp.tile(jnp.concatenate([-sine, sine], axis=1), (1, 4))
    key = jnp.pad(rope_key[0].astype(f32), ((0, 0), (0, 96)))
    first, second = pack(query[0], out_grad[0], key, cos_lanes, sin_lanes)
    first = lax.all_to_all(first, SP, 0, 0, tiled=True).reshape(LENGTH, 256)
    kv = lax.dot_general(nlat_all, own, (((1,), (1,)), ((), ())), preferred_element_type=f32).astype(bf16)
    second, kv = lax.optimization_barrier((second, kv))
    second = lax.all_to_all(second, SP, 0, 0, tiled=True).reshape(LENGTH, 128)
    cos_all, sin_all = angles(jnp.arange(LENGTH))
    cos_all, sin_all = cos_all.T, sin_all.T
    g0 = attend(0, first, first, kv, cos_all, sin_all)
    kv, g0 = lax.optimization_barrier((kv, g0))
    r0 = lax.all_to_all(g0.reshape(NSP, TOKENS, 256), SP, 0, 0, tiled=True)
    g1 = attend(1, second, first, kv, cos_all, sin_all)
    r0, g1 = lax.optimization_barrier((r0, g1))
    r1 = lax.all_to_all(g1.reshape(NSP, TOKENS, 256), SP, 0, 0, tiled=True)

    parts = [
        lax.dot_general(g[:, 0:128], nlat_all, (((0,), (0,)), ((), ())), preferred_element_type=f32)
        for g in (g0, g1)
    ]
    part = jnp.concatenate(parts, axis=0)
    pieces = part.astype(bf16).reshape(2, 2, 4, 16, LATENT).transpose(0, 2, 1, 3, 4).reshape(NDP, 32, LATENT)
    piece = reduce_over_rows(pieces)
    gain_part = jnp.sum(part * own.astype(f32), axis=0) / gain
    gain_grad = sum_everywhere(gain_part.reshape(8, 128)).reshape(LATENT)
    piece = lax.ppermute(piece, ALL, to_rows())
    r1, piece = lax.optimization_barrier((r1, piece))
    grads = everyone(piece, SP, NSP).reshape(NSP, 2, 16, LATENT)
    key_grad = grads[:, 0].reshape(256, LATENT).astype(f32)
    value_grad = grads[:, 1].reshape(256, LATENT).astype(f32)

    dq, dlat, drope = finish(
        r0, r1, whole.reshape(NSP, 256, LATENT), latent[0], gain_row, cos_lanes, sin_lanes
    )
    return dq[None], dlat[None], drope[None], key_grad, value_grad, gain_grad


def solution(mesh):
    split = Mesh(mesh.devices.reshape(4, 4, 4, 2), ("sp_0", "sp_1", "dp_0", "dp_1"))
    in_specs = (
        P(DP, SP, None),
        P(DP, SP, None),
        P(DP, SP, None),
        P(),
        P(DP, None),
        P(DP, None),
        P(DP, SP, None),
    )
    out_specs = (P(DP, SP, None), P(DP, SP, None), P(DP, SP, None), P(DP, None), P(DP, None), P())
    return jax.shard_map(program, mesh=split, in_specs=in_specs, out_specs=out_specs, check_vma=False)
```

```python
import functools

import jax
import jax.numpy as jnp
from jax import lax
from jax.experimental import pallas as pl
from jax.experimental.pallas import tpu as pltpu
from jax.sharding import Mesh
from jax.sharding import PartitionSpec as P

ATTENTION_HEADS = 32
PLAIN = 64
ROPE = 32
HALF = ROPE // 2
WIDTH = PLAIN + ROPE
LATENT = 1024
SPAN = 64
LENGTH = 3072
DP = ("dp_0", "dp_1")
SP = ("sp_0", "sp_1")
ALL = SP + DP
NSP = 16
NDP = 8
TOKENS = LENGTH // NSP
BLOCK = 512
SCALE = WIDTH**-0.5
LOG2E = 1.4426950408889634

eps = 1e-06
rope_base = 10000.0
f32 = jnp.float32
bf16 = jnp.bfloat16


def angles(positions):
    inverse = 1.0 / rope_base ** (jnp.arange(0, ROPE, 2, dtype=f32) / ROPE)
    turned = positions.astype(f32)[:, None] * inverse[None, :]
    return jnp.cos(turned), jnp.sin(turned)


def lanes_of(shape):
    return lax.broadcasted_iota(jnp.int32, shape, 1)


def pack_body(q_ref, g_ref, kr_ref, cos_ref, sin_ref, out_ref, other_ref):
    lane = lanes_of((TOKENS, 128))
    cosine = cos_ref[...]
    sine = sin_ref[...]

    def turn(x):
        inside = (lane % ROPE) < HALF
        swapped = jnp.where(inside, pltpu.roll(x, 128 - HALF, 1), pltpu.roll(x, HALF, 1))
        return x * cosine + swapped * sine

    key = turn(kr_ref[...])
    key = pltpu.roll(key, ROPE, 1)

    def emit(slot, qn0, qr0, qn1, qr1, grads):
        first = jnp.where(lane < PLAIN, qn0, pltpu.roll(grads, PLAIN, 1))
        second = jnp.where(lane < PLAIN, qn1, grads)
        third = turn(jnp.where(lane < ROPE, qr0, jnp.where(lane >= 96, qr1, 0.0)))
        third = jnp.where((lane >= ROPE) & (lane < 2 * ROPE), key, third)
        out_ref[slot, :, 0:128] = first.astype(bf16)
        out_ref[slot, :, 128:256] = third.astype(bf16)
        other_ref[slot] = second.astype(bf16)

    for pair in range(NSP // 2):
        a0, a1, a2 = [
            q_ref[:, 384 * pair + 128 * k : 384 * pair + 128 * (k + 1)].astype(f32) for k in range(3)
        ]
        g0 = g_ref[:, 256 * pair : 256 * pair + 128].astype(f32)
        g1 = g_ref[:, 256 * pair + 128 : 256 * pair + 256].astype(f32)
        qn1 = jnp.where(lane < ROPE, pltpu.roll(a0, ROPE, 1), pltpu.roll(a1, ROPE, 1))
        emit(2 * pair, a0, pltpu.roll(a0, 64, 1), qn1, pltpu.roll(a1, 64, 1), g0)
        emit(2 * pair + 1, pltpu.roll(a1, 64, 1), a2, pltpu.roll(a2, 96, 1), a2, g1)


def pack(query, grads, key, cosine, sine):
    return pl.pallas_call(
        pack_body,
        out_shape=[
            jax.ShapeDtypeStruct((NSP, TOKENS, 256), bf16),
            jax.ShapeDtypeStruct((NSP, TOKENS, 128), bf16),
        ],
        cost_estimate=pl.CostEstimate(flops=2_000_000_000, bytes_accessed=5_000_000, transcendentals=0),
        name="pack",
    )(query, grads, key, cosine, sine)


def attend_body(head, qd_ref, rt_ref, kv_ref, cos_ref, sin_ref, out_ref, p_buf, dp_buf, m_buf, kt_buf, acc, dq_acc):
    blocks = LENGTH // BLOCK
    lane = lanes_of((BLOCK, 128))
    factor = SCALE * LOG2E
    low = 0 if head == 0 else 96

    def prepare(j, carry):
        rows = pl.ds(pl.multiple_of(j * BLOCK, BLOCK), BLOCK)
        kt = kv_ref[rows, :].astype(f32).T
        rt = rt_ref[rows, :].astype(f32).T
        kt_buf[:, rows] = jnp.concatenate([kt[0:PLAIN], rt[ROPE : 2 * ROPE]], axis=0).astype(bf16)
        acc[rows, :] = jnp.zeros((BLOCK, 256), f32)
        return carry

    lax.fori_loop(0, blocks, prepare, 0)
    key_seg = lax.broadcasted_iota(jnp.int32, (BLOCK, BLOCK), 0) // SPAN
    query_seg = lax.broadcasted_iota(jnp.int32, (BLOCK, BLOCK), 1) // SPAN
    allowed = key_seg <= query_seg

    def one_block(i, carry):
        rows = pl.ds(pl.multiple_of(i * BLOCK, BLOCK), BLOCK)
        qd = qd_ref[rows, :].astype(f32)
        rt = rt_ref[rows, :].astype(f32)
        qdt = qd.T
        rtt = rt.T
        none = jnp.zeros((32, BLOCK), f32)
        left = jnp.concatenate(
            [qdt[0:PLAIN], none, none, none, rtt[low : low + ROPE], none, none], axis=0
        ).astype(bf16)
        left_d = jnp.concatenate([none, none, qdt[PLAIN:128]], axis=0).astype(bf16)
        right = jnp.concatenate(
            [jnp.where(lane < PLAIN, qd, 0.0), jnp.where((lane >= low) & (lane < low + ROPE), rt, 0.0)], axis=1
        ).astype(bf16)
        right_d = jnp.where(lane < PLAIN, 0.0, qd).astype(bf16)

        def gather_stats(j, stats, masked):
            top, total, inner = stats
            keys = pl.ds(pl.multiple_of(j * BLOCK, BLOCK), BLOCK)
            kv = kv_ref[keys, :]
            both = jnp.concatenate([kv, rt_ref[keys, :]], axis=1)
            scores = jnp.dot(both, left, preferred_element_type=f32) * factor
            if masked:
                scores = jnp.where(allowed, scores, -jnp.inf)
            d_probs = jnp.dot(kv, left_d, preferred_element_type=f32)
            new_top = jnp.maximum(top, jnp.max(scores, axis=0, keepdims=True))
            probs = jnp.exp2(scores - new_top)
            shrink = jnp.exp2(top - new_top)
            total = total * shrink + jnp.sum(probs, axis=0, keepdims=True)
            inner = inner * shrink + jnp.sum(probs * d_probs, axis=0, keepdims=True)
            p_buf[keys, :] = probs
            dp_buf[keys, :] = d_probs
            m_buf[j] = jnp.broadcast_to(new_top, (8, BLOCK))
            return new_top, total, inner

        start = (
            jnp.full((1, BLOCK), jnp.finfo(f32).min, f32),
            jnp.zeros((1, BLOCK), f32),
            jnp.zeros((1, BLOCK), f32),
        )
        stats = lax.fori_loop(0, i, functools.partial(gather_stats, masked=False), start)
        top, total, inner = gather_stats(i, stats, True)
        inverse = 1.0 / total
        inner = inner * inverse
        dq_acc[...] = jnp.zeros((WIDTH, BLOCK), f32)

        def gradients(j, carry):
            keys = pl.ds(pl.multiple_of(j * BLOCK, BLOCK), BLOCK)
            grow = jnp.exp2(m_buf[j][0:1] - top) * inverse
            probs = p_buf[keys, :] * grow
            ds = (probs * (dp_buf[keys, :] - inner)).astype(bf16)
            pb = probs.astype(bf16)
            dq_acc[...] += jnp.dot(kt_buf[:, keys], ds, preferred_element_type=f32)
            acc[keys, :] += jnp.dot(ds, right, preferred_element_type=f32)
            acc[keys, 0:128] += jnp.dot(pb, right_d, preferred_element_type=f32)
            return carry

        lax.fori_loop(0, i + 1, gradients, 0)
        dq = dq_acc[...] * SCALE
        cosine = cos_ref[:, rows]
        sine = sin_ref[:, rows]
        first, second = dq[PLAIN : PLAIN + HALF], dq[PLAIN + HALF : WIDTH]
        pieces = [dq[0:PLAIN], first * cosine + second * sine, second * cosine - first * sine]
        pieces = [none] + pieces if head == 0 else pieces + [none]
        out_ref[rows, 128:256] = jnp.concatenate(pieces, axis=0).T.astype(bf16)
        return carry

    lax.fori_loop(0, blocks, one_block, 0)

    def finish(j, carry):
        rows = pl.ds(pl.multiple_of(j * BLOCK, BLOCK), BLOCK)
        plain = acc[rows, 0:128]
        out_ref[rows, 0:128] = jnp.where(lane < PLAIN, plain * SCALE, plain).astype(bf16)
        turned = acc[rows, 128:256] * SCALE
        kept = out_ref[rows, 128:256].astype(f32)
        mine = (lane >= low) & (lane < low + ROPE)
        out_ref[rows, 128:256] = jnp.where(mine, turned, kept).astype(bf16)
        return carry

    lax.fori_loop(0, blocks, finish, 0)


def attend(head, arrived, turned, kv, cosine, sine):
    return pl.pallas_call(
        functools.partial(attend_body, head),
        grid=(1,),
        in_specs=[
            pl.BlockSpec((LENGTH, 128), lambda g: (0, 0)),
            pl.BlockSpec((LENGTH, 128), lambda g: (0, 1)),
            pl.BlockSpec((LENGTH, 128), lambda g: (0, head)),
            pl.BlockSpec((HALF, LENGTH), lambda g: (0, 0)),
            pl.BlockSpec((HALF, LENGTH), lambda g: (0, 0)),
        ],
        out_specs=pl.BlockSpec((LENGTH, 256), lambda g: (0, 0)),
        out_shape=jax.ShapeDtypeStruct((LENGTH, 256), bf16),
        scratch_shapes=[
            pltpu.VMEM((LENGTH, BLOCK), f32),
            pltpu.VMEM((LENGTH, BLOCK), f32),
            pltpu.VMEM((LENGTH // BLOCK, 8, BLOCK), f32),
            pltpu.VMEM((WIDTH, LENGTH), bf16),
            pltpu.VMEM((LENGTH, 256), f32),
            pltpu.VMEM((WIDTH, BLOCK), f32),
        ],
        compiler_params=pltpu.CompilerParams(vmem_limit_bytes=48 * 1024 * 1024),
        cost_estimate=pl.CostEstimate(
            flops=12_000_000_000, bytes_accessed=6_000_000, transcendentals=5_000_000
        ),
    )(arrived, turned, kv, cosine, sine)


def finish_body(r0_ref, r1_ref, w_ref, lat_ref, gain_ref, cos_ref, sin_ref, dq_ref, dlat_ref, drope_ref, acc, rope):
    step = pl.program_id(0)
    lane = lanes_of((TOKENS, 128))

    @pl.when(step == 0)
    def _():
        acc[...] = jnp.zeros_like(acc)
        rope[...] = jnp.zeros_like(rope)

    tiles = []
    for half in range(2):
        r0 = r0_ref[half]
        r1 = r1_ref[half]
        both = jnp.concatenate([r0[:, 0:128], r1[:, 0:128]], axis=1)
        acc[...] += jnp.dot(both, w_ref[half], preferred_element_type=f32)
        t0 = r0[:, 128:256].astype(f32)
        t1 = r1[:, 128:256].astype(f32)
        rope[...] += jnp.where(lane < ROPE, t0, jnp.where(lane >= 96, t1, 0.0))
        tiles.append((t0, t1))
    (x0, x1), (y0, y1) = tiles
    dq_ref[:, 0:128] = jnp.where(lane < 96, pltpu.roll(x0, 96, 1), pltpu.roll(x1, 96, 1)).astype(bf16)
    dq_ref[:, 128:256] = jnp.where(lane < 64, pltpu.roll(x1, 96, 1), pltpu.roll(y0, 32, 1)).astype(bf16)
    dq_ref[:, 256:384] = jnp.where(lane < 32, pltpu.roll(y0, 32, 1), pltpu.roll(y1, 32, 1)).astype(bf16)

    @pl.when(step == NSP // 2 - 1)
    def _():
        lat = lat_ref[...].astype(f32)
        inv_rms = lax.rsqrt(jnp.mean(lat * lat, axis=-1, keepdims=True) + eps)
        normed = lat * inv_rms
        scaled = acc[...] * gain_ref[...]
        dlat_ref[...] = inv_rms * (scaled - normed * jnp.mean(scaled * normed, axis=-1, keepdims=True))
        x = rope[...]
        x = x + pltpu.roll(x, 32, 1)
        swapped = jnp.where(lane < HALF, pltpu.roll(x, 128 - HALF, 1), pltpu.roll(x, HALF, 1))
        drope_ref[...] = (x * cos_ref[...] - swapped * sin_ref[...])[:, 0:ROPE]


def finish(r0, r1, weights, latent, gain, cosine, sine):
    half = NSP // 2
    return pl.pallas_call(
        finish_body,
        grid=(half,),
        in_specs=[
            pl.BlockSpec((2, TOKENS, 256), lambda g: (g, 0, 0)),
            pl.BlockSpec((2, TOKENS, 256), lambda g: (g, 0, 0)),
            pl.BlockSpec((2, 256, LATENT), lambda g: (g, 0, 0)),
            pl.BlockSpec((TOKENS, LATENT), lambda g: (0, 0)),
            pl.BlockSpec((1, LATENT), lambda g: (0, 0)),
            pl.BlockSpec((TOKENS, 128), lambda g: (0, 0)),
            pl.BlockSpec((TOKENS, 128), lambda g: (0, 0)),
        ],
        out_specs=[
            pl.BlockSpec((TOKENS, 384), lambda g: (0, g)),
            pl.BlockSpec((TOKENS, LATENT), lambda g: (0, 0)),
            pl.BlockSpec((TOKENS, ROPE), lambda g: (0, 0)),
        ],
        out_shape=[
            jax.ShapeDtypeStruct((TOKENS, ATTENTION_HEADS * WIDTH), bf16),
            jax.ShapeDtypeStruct((TOKENS, LATENT), f32),
            jax.ShapeDtypeStruct((TOKENS, ROPE), f32),
        ],
        scratch_shapes=[pltpu.VMEM((TOKENS, LATENT), f32), pltpu.VMEM((TOKENS, 128), f32)],
        cost_estimate=pl.CostEstimate(flops=2_000_000_000, bytes_accessed=14_000_000, transcendentals=0),
        name="finish",
    )(r0, r1, weights, latent, gain, cosine, sine)


def to_heads():
    return [(NDP * a + d, NDP * (2 * d + a // 8) + a % 8) for a in range(NSP) for d in range(NDP)]


def to_rows():
    return [(b, a) for a, b in to_heads()]


def everyone(value, axes, size):
    return lax.all_to_all(jnp.broadcast_to(value[None], (size, *value.shape)), axes, 0, 0, tiled=True)


def shifted(value, axis, k):
    return lax.ppermute(value, axis, [(i, (i + k) % 4) for i in range(4)])


SWAP = [(0, 1), (1, 0)]


def sum_of_four(value, axis):
    others = [shifted(value, axis, k) for k in (1, 2, 3)]
    return (value + others[1]) + (others[0] + others[2])


def reduce_over_rows(pieces, small):
    across, core = lax.axis_index("dp_0"), lax.axis_index("dp_1")
    pairs = pieces.reshape(4, 2, *pieces.shape[1:])
    kept = lax.dynamic_index_in_dim(pairs, core, 1, keepdims=False)
    given = lax.dynamic_index_in_dim(pairs, 1 - core, 1, keepdims=False)
    given, small = lax.optimization_barrier((given, small))
    given = lax.ppermute(given, "dp_1", SWAP)
    small = small + lax.ppermute(small, "dp_1", SWAP)
    kept = kept.astype(f32) + given.astype(f32)
    total = lax.dynamic_index_in_dim(kept, across, 0, keepdims=False)
    kept = kept.astype(bf16)
    kept, small = lax.optimization_barrier((kept, small))
    for k in (1, 2, 3):
        sent = lax.dynamic_index_in_dim(kept, (across + k) & 3, 0, keepdims=False)
        total = total + shifted(sent, "dp_0", k).astype(f32)
    small = sum_of_four(small, "dp_0")
    return lax.optimization_barrier((total.astype(bf16), small))


def program(query, latent, rope_key, gain, key_up, value_up, out_grad):
    place = lax.axis_index(SP)
    gain_row = gain[None, :]
    lat = latent[0].astype(f32)
    inv_rms = lax.rsqrt(jnp.mean(lat * lat, axis=-1, keepdims=True) + eps)
    nlat = (lat * inv_rms * gain_row).astype(bf16)
    rows = jnp.stack([key_up.reshape(4, 64, LATENT), value_up.reshape(4, 64, LATENT)], axis=1)
    rows = rows.reshape(512, LATENT)
    mine = lax.dynamic_slice_in_dim(rows, (place // 8) * 256, 256, axis=0)
    own = lax.ppermute(mine, ALL, to_heads())
    nlat_all = lax.all_gather(nlat, SP, axis=0, tiled=True)
    whole = lax.all_gather(rows, DP, axis=0, tiled=True)

    positions = place * TOKENS + jnp.arange(TOKENS)
    cosine, sine = angles(positions)
    cos_lanes = jnp.tile(cosine, (1, 8))
    sin_lanes = jnp.tile(jnp.concatenate([-sine, sine], axis=1), (1, 4))
    key = jnp.pad(rope_key[0].astype(f32), ((0, 0), (0, 96)))
    first, second = pack(query[0], out_grad[0], key, cos_lanes, sin_lanes)
    first, nlat_all, own = lax.optimization_barrier((first, nlat_all, own))
    first = lax.all_to_all(first, SP, 0, 0, tiled=True).reshape(LENGTH, 256)
    kv = lax.dot_general(nlat_all, own, (((1,), (1,)), ((), ())), preferred_element_type=f32).astype(bf16)
    second, kv = lax.optimization_barrier((second, kv))
    second = lax.all_to_all(second, SP, 0, 0, tiled=True).reshape(LENGTH, 128)
    cos_all, sin_all = angles(jnp.arange(LENGTH))
    cos_all, sin_all = cos_all.T, sin_all.T
    g0 = attend(0, first, first, kv, cos_all, sin_all)
    kv, g0 = lax.optimization_barrier((kv, g0))
    r0 = lax.all_to_all(g0.reshape(NSP, TOKENS, 256), SP, 0, 0, tiled=True)
    g1 = attend(1, second, first, kv, cos_all, sin_all)
    r0, g1 = lax.optimization_barrier((r0, g1))
    r1 = lax.all_to_all(g1.reshape(NSP, TOKENS, 256), SP, 0, 0, tiled=True)

    parts = [
        lax.dot_general(g[:, 0:128], nlat_all, (((0,), (0,)), ((), ())), preferred_element_type=f32)
        for g in (g0, g1)
    ]
    part = jnp.concatenate(parts, axis=0)
    pieces = part.astype(bf16).reshape(2, 2, 4, 16, LATENT).transpose(0, 2, 1, 3, 4).reshape(NDP, 32, LATENT)
    gain_part = (jnp.sum(part * own.astype(f32), axis=0) / gain).reshape(8, 128)
    piece, gain_part = reduce_over_rows(pieces, gain_part)
    piece = lax.ppermute(piece, ALL, to_rows())
    gain_part = sum_of_four(gain_part, "sp_1")
    piece, gain_part = lax.optimization_barrier((piece, gain_part))
    gain_grad = sum_of_four(gain_part, "sp_0").reshape(LATENT)
    r1, piece = lax.optimization_barrier((r1, piece))
    grads = everyone(piece, SP, NSP).reshape(NSP, 2, 16, LATENT)
    key_grad = grads[:, 0].reshape(256, LATENT).astype(f32)
    value_grad = grads[:, 1].reshape(256, LATENT).astype(f32)

    dq, dlat, drope = finish(
        r0, r1, whole.reshape(NSP, 256, LATENT), latent[0], gain_row, cos_lanes, sin_lanes
    )
    return dq[None], dlat[None], drope[None], key_grad, value_grad, gain_grad


def solution(mesh):
    split = Mesh(mesh.devices.reshape(4, 4, 4, 2), ("sp_0", "sp_1", "dp_0", "dp_1"))
    in_specs = (
        P(DP, SP, None),
        P(DP, SP, None),
        P(DP, SP, None),
        P(),
        P(DP, None),
        P(DP, None),
        P(DP, SP, None),
    )
    out_specs = (P(DP, SP, None), P(DP, SP, None), P(DP, SP, None), P(DP, None), P(DP, None), P())
    return jax.shard_map(program, mesh=split, in_specs=in_specs, out_specs=out_specs, check_vma=False)
```

```python
import functools

import jax
import jax.numpy as jnp
from jax import lax
from jax.experimental import pallas as pl
from jax.experimental.pallas import tpu as pltpu
from jax.sharding import Mesh
from jax.sharding import PartitionSpec as P

ATTENTION_HEADS = 32
PLAIN = 64
ROPE = 32
HALF = ROPE // 2
WIDTH = PLAIN + ROPE
LATENT = 1024
SPAN = 64
LENGTH = 3072
DP = ("dp_0", "dp_1")
SP = ("sp_0", "sp_1")
ALL = SP + DP
NSP = 16
NDP = 8
TOKENS = LENGTH // NSP
BLOCK = 512
SCALE = WIDTH**-0.5
LOG2E = 1.4426950408889634

eps = 1e-06
rope_base = 10000.0
f32 = jnp.float32
bf16 = jnp.bfloat16


def angles(positions):
    inverse = 1.0 / rope_base ** (jnp.arange(0, ROPE, 2, dtype=f32) / ROPE)
    turned = positions.astype(f32)[:, None] * inverse[None, :]
    return jnp.cos(turned), jnp.sin(turned)


def lanes_of(shape):
    return lax.broadcasted_iota(jnp.int32, shape, 1)


def pack_body(q_ref, g_ref, kr_ref, cos_ref, sin_ref, out_ref, other_ref):
    lane = lanes_of((TOKENS, 128))
    cosine = cos_ref[...]
    sine = sin_ref[...]

    def turn(x):
        inside = (lane % ROPE) < HALF
        swapped = jnp.where(inside, pltpu.roll(x, 128 - HALF, 1), pltpu.roll(x, HALF, 1))
        return x * cosine + swapped * sine

    key = turn(kr_ref[...])
    key = pltpu.roll(key, ROPE, 1)

    def emit(slot, qn0, qr0, qn1, qr1, grads):
        first = jnp.where(lane < PLAIN, qn0, pltpu.roll(grads, PLAIN, 1))
        second = jnp.where(lane < PLAIN, qn1, grads)
        third = turn(jnp.where(lane < ROPE, qr0, jnp.where(lane >= 96, qr1, 0.0)))
        third = jnp.where((lane >= ROPE) & (lane < 2 * ROPE), key, third)
        out_ref[slot, :, 0:128] = first.astype(bf16)
        out_ref[slot, :, 128:256] = third.astype(bf16)
        other_ref[slot] = second.astype(bf16)

    for pair in range(NSP // 2):
        a0, a1, a2 = [
            q_ref[:, 384 * pair + 128 * k : 384 * pair + 128 * (k + 1)].astype(f32) for k in range(3)
        ]
        g0 = g_ref[:, 256 * pair : 256 * pair + 128].astype(f32)
        g1 = g_ref[:, 256 * pair + 128 : 256 * pair + 256].astype(f32)
        qn1 = jnp.where(lane < ROPE, pltpu.roll(a0, ROPE, 1), pltpu.roll(a1, ROPE, 1))
        emit(2 * pair, a0, pltpu.roll(a0, 64, 1), qn1, pltpu.roll(a1, 64, 1), g0)
        emit(2 * pair + 1, pltpu.roll(a1, 64, 1), a2, pltpu.roll(a2, 96, 1), a2, g1)


def pack(query, grads, key, cosine, sine):
    return pl.pallas_call(
        pack_body,
        out_shape=[
            jax.ShapeDtypeStruct((NSP, TOKENS, 256), bf16),
            jax.ShapeDtypeStruct((NSP, TOKENS, 128), bf16),
        ],
        cost_estimate=pl.CostEstimate(flops=2_000_000_000, bytes_accessed=5_000_000, transcendentals=0),
        name="pack",
    )(query, grads, key, cosine, sine)


def attend_body(head, qd_ref, rt_ref, kv_ref, cos_ref, sin_ref, out_ref, p_buf, dp_buf, m_buf, kt_buf, acc, dq_acc):
    blocks = LENGTH // BLOCK
    lane = lanes_of((BLOCK, 128))
    factor = SCALE * LOG2E
    low = 0 if head == 0 else 96

    def prepare(j, carry):
        rows = pl.ds(pl.multiple_of(j * BLOCK, BLOCK), BLOCK)
        kt = kv_ref[rows, :].astype(f32).T
        rt = rt_ref[rows, :].astype(f32).T
        kt_buf[:, rows] = jnp.concatenate([kt[0:PLAIN], rt[ROPE : 2 * ROPE]], axis=0).astype(bf16)
        acc[rows, :] = jnp.zeros((BLOCK, 256), f32)
        return carry

    lax.fori_loop(0, blocks, prepare, 0)
    key_seg = lax.broadcasted_iota(jnp.int32, (BLOCK, BLOCK), 0) // SPAN
    query_seg = lax.broadcasted_iota(jnp.int32, (BLOCK, BLOCK), 1) // SPAN
    allowed = key_seg <= query_seg

    def one_block(i, carry):
        rows = pl.ds(pl.multiple_of(i * BLOCK, BLOCK), BLOCK)
        qd = qd_ref[rows, :].astype(f32)
        rt = rt_ref[rows, :].astype(f32)
        qdt = qd.T
        rtt = rt.T
        none = jnp.zeros((32, BLOCK), f32)
        left = jnp.concatenate(
            [qdt[0:PLAIN], none, none, none, rtt[low : low + ROPE], none, none], axis=0
        ).astype(bf16)
        left_d = jnp.concatenate([none, none, qdt[PLAIN:128]], axis=0).astype(bf16)
        right = jnp.concatenate(
            [jnp.where(lane < PLAIN, qd, 0.0), jnp.where((lane >= low) & (lane < low + ROPE), rt, 0.0)], axis=1
        ).astype(bf16)
        right_d = jnp.where(lane < PLAIN, 0.0, qd).astype(bf16)

        def gather_stats(j, stats, masked):
            top, total, inner = stats
            keys = pl.ds(pl.multiple_of(j * BLOCK, BLOCK), BLOCK)
            kv = kv_ref[keys, :]
            both = jnp.concatenate([kv, rt_ref[keys, :]], axis=1)
            scores = jnp.dot(both, left, preferred_element_type=f32) * factor
            if masked:
                scores = jnp.where(allowed, scores, -jnp.inf)
            d_probs = jnp.dot(kv, left_d, preferred_element_type=f32)
            new_top = jnp.maximum(top, jnp.max(scores, axis=0, keepdims=True))
            probs = jnp.exp2(scores - new_top)
            shrink = jnp.exp2(top - new_top)
            total = total * shrink + jnp.sum(probs, axis=0, keepdims=True)
            inner = inner * shrink + jnp.sum(probs * d_probs, axis=0, keepdims=True)
            p_buf[keys, :] = probs
            dp_buf[keys, :] = d_probs
            m_buf[j] = jnp.broadcast_to(new_top, (8, BLOCK))
            return new_top, total, inner

        start = (
            jnp.full((1, BLOCK), jnp.finfo(f32).min, f32),
            jnp.zeros((1, BLOCK), f32),
            jnp.zeros((1, BLOCK), f32),
        )
        stats = lax.fori_loop(0, i, functools.partial(gather_stats, masked=False), start)
        top, total, inner = gather_stats(i, stats, True)
        inverse = 1.0 / total
        inner = inner * inverse
        dq_acc[...] = jnp.zeros((WIDTH, BLOCK), f32)

        def gradients(j, carry):
            keys = pl.ds(pl.multiple_of(j * BLOCK, BLOCK), BLOCK)
            grow = jnp.exp2(m_buf[j][0:1] - top) * inverse
            probs = p_buf[keys, :] * grow
            ds = (probs * (dp_buf[keys, :] - inner)).astype(bf16)
            pb = probs.astype(bf16)
            dq_acc[...] += jnp.dot(kt_buf[:, keys], ds, preferred_element_type=f32)
            acc[keys, :] += jnp.dot(ds, right, preferred_element_type=f32)
            acc[keys, 0:128] += jnp.dot(pb, right_d, preferred_element_type=f32)
            return carry

        lax.fori_loop(0, i + 1, gradients, 0)
        dq = dq_acc[...] * SCALE
        cosine = cos_ref[:, rows]
        sine = sin_ref[:, rows]
        first, second = dq[PLAIN : PLAIN + HALF], dq[PLAIN + HALF : WIDTH]
        pieces = [dq[0:PLAIN], first * cosine + second * sine, second * cosine - first * sine]
        pieces = [none] + pieces if head == 0 else pieces + [none]
        out_ref[rows, 128:256] = jnp.concatenate(pieces, axis=0).T.astype(bf16)
        return carry

    lax.fori_loop(0, blocks, one_block, 0)

    def finish(j, carry):
        rows = pl.ds(pl.multiple_of(j * BLOCK, BLOCK), BLOCK)
        plain = acc[rows, 0:128]
        out_ref[rows, 0:128] = jnp.where(lane < PLAIN, plain * SCALE, plain).astype(bf16)
        turned = acc[rows, 128:256] * SCALE
        kept = out_ref[rows, 128:256].astype(f32)
        mine = (lane >= low) & (lane < low + ROPE)
        out_ref[rows, 128:256] = jnp.where(mine, turned, kept).astype(bf16)
        return carry

    lax.fori_loop(0, blocks, finish, 0)


def attend(head, arrived, turned, kv, cosine, sine):
    return pl.pallas_call(
        functools.partial(attend_body, head),
        grid=(1,),
        in_specs=[
            pl.BlockSpec((LENGTH, 128), lambda g: (0, 0)),
            pl.BlockSpec((LENGTH, 128), lambda g: (0, 1)),
            pl.BlockSpec((LENGTH, 128), lambda g: (0, head)),
            pl.BlockSpec((HALF, LENGTH), lambda g: (0, 0)),
            pl.BlockSpec((HALF, LENGTH), lambda g: (0, 0)),
        ],
        out_specs=pl.BlockSpec((LENGTH, 256), lambda g: (0, 0)),
        out_shape=jax.ShapeDtypeStruct((LENGTH, 256), bf16),
        scratch_shapes=[
            pltpu.VMEM((LENGTH, BLOCK), f32),
            pltpu.VMEM((LENGTH, BLOCK), f32),
            pltpu.VMEM((LENGTH // BLOCK, 8, BLOCK), f32),
            pltpu.VMEM((WIDTH, LENGTH), bf16),
            pltpu.VMEM((LENGTH, 256), f32),
            pltpu.VMEM((WIDTH, BLOCK), f32),
        ],
        compiler_params=pltpu.CompilerParams(vmem_limit_bytes=48 * 1024 * 1024),
        cost_estimate=pl.CostEstimate(
            flops=12_000_000_000, bytes_accessed=6_000_000, transcendentals=5_000_000
        ),
    )(arrived, turned, kv, cosine, sine)


def project_body(order_ref, nlat_ref, *refs):
    weights, rest = refs[:NDP], refs[NDP:]
    nlat = nlat_ref[...]
    if len(rest) == 2:
        rest[1][:, :, 0:128] = rest[0][...]
    out_ref = rest[-1]
    base = out_ref.shape[2] - 128
    for step in range(NDP):
        made = lax.dot_general(nlat, weights[step][...], (((1,), (1,)), ((), ())), preferred_element_type=f32)
        slot = 2 * order_ref[step]
        out_ref[slot, :, base : base + 128] = made[:, 0:128].astype(bf16)
        out_ref[slot + 1, :, base : base + 128] = made[:, 128:256].astype(bf16)


def project(order, nlat, weights, extra):
    extras = [] if extra is None else [extra]
    memory = pl.BlockSpec(memory_space=pltpu.VMEM)
    return pl.pallas_call(
        project_body,
        in_specs=[pl.BlockSpec(memory_space=pltpu.SMEM)] + [memory] * (1 + NDP + len(extras)),
        out_specs=memory,
        out_shape=jax.ShapeDtypeStruct((NSP, TOKENS, 128 * (1 + len(extras))), bf16),
        cost_estimate=pl.CostEstimate(flops=2_000_000_000, bytes_accessed=6_000_000, transcendentals=0),
        name="project",
    )(order, nlat, *weights, *extras)


def finish_body(order_ref, r0_ref, r1_ref, lat_ref, gain_ref, cos_ref, sin_ref, *refs):
    evens, odds = refs[:NDP], refs[NDP : 2 * NDP]
    dq_ref, dlat_ref, drope_ref, acc = refs[2 * NDP :]
    lane = lanes_of((TOKENS, 128))
    rope = jnp.zeros((TOKENS, 128), f32)
    for step in range(NDP):
        slot = 2 * order_ref[step]
        tiles = []
        for half in range(2):
            r0 = r0_ref[slot + half]
            r1 = r1_ref[slot + half]
            rows = slice(128 * half, 128 * half + 128)
            both = jnp.concatenate([r0[:, 0:128], r1[:, 0:128]], axis=1)
            weights = jnp.concatenate([evens[step][rows, :], odds[step][rows, :]], axis=0)
            added = jnp.dot(both, weights, preferred_element_type=f32)
            if step == 0 and half == 0:
                acc[...] = added
            else:
                acc[...] += added
            t0 = r0[:, 128:256].astype(f32)
            t1 = r1[:, 128:256].astype(f32)
            rope = rope + jnp.where(lane < ROPE, t0, jnp.where(lane >= 96, t1, 0.0))
            tiles.append((t0, t1))
        (x0, x1), (y0, y1) = tiles
        dq = [
            jnp.where(lane < 96, pltpu.roll(x0, 96, 1), pltpu.roll(x1, 96, 1)),
            jnp.where(lane < 64, pltpu.roll(x1, 96, 1), pltpu.roll(y0, 32, 1)),
            jnp.where(lane < 32, pltpu.roll(y0, 32, 1), pltpu.roll(y1, 32, 1)),
        ]
        start = pl.multiple_of(384 * order_ref[step], 128)
        dq_ref[:, pl.ds(start, 384)] = jnp.concatenate(dq, axis=1).astype(bf16)

    lat = lat_ref[...].astype(f32)
    inv_rms = lax.rsqrt(jnp.mean(lat * lat, axis=-1, keepdims=True) + eps)
    normed = lat * inv_rms
    scaled = acc[...] * gain_ref[...]
    dlat_ref[...] = inv_rms * (scaled - normed * jnp.mean(scaled * normed, axis=-1, keepdims=True))
    x = rope + pltpu.roll(rope, 32, 1)
    swapped = jnp.where(lane < HALF, pltpu.roll(x, 128 - HALF, 1), pltpu.roll(x, HALF, 1))
    drope_ref[...] = (x * cos_ref[...] - swapped * sin_ref[...])[:, 0:ROPE]


def finish(order, r0, r1, latent, gain, cosine, sine, evens, odds):
    memory = pl.BlockSpec(memory_space=pltpu.VMEM)
    return pl.pallas_call(
        finish_body,
        in_specs=[pl.BlockSpec(memory_space=pltpu.SMEM)] + [memory] * (6 + 2 * NDP),
        out_specs=[memory] * 3,
        out_shape=[
            jax.ShapeDtypeStruct((TOKENS, ATTENTION_HEADS * WIDTH), bf16),
            jax.ShapeDtypeStruct((TOKENS, LATENT), f32),
            jax.ShapeDtypeStruct((TOKENS, ROPE), f32),
        ],
        scratch_shapes=[pltpu.VMEM((TOKENS, LATENT), f32)],
        cost_estimate=pl.CostEstimate(flops=2_000_000_000, bytes_accessed=14_000_000, transcendentals=0),
        name="finish",
    )(order, r0, r1, latent, gain, cosine, sine, *evens, *odds)


def to_heads():
    return [(NDP * a + d, NDP * (2 * d + a // 8) + a % 8) for a in range(NSP) for d in range(NDP)]


def to_rows():
    return [(b, a) for a, b in to_heads()]


def everyone(value, axes, size):
    return lax.all_to_all(jnp.broadcast_to(value[None], (size, *value.shape)), axes, 0, 0, tiled=True)


def shifted(value, axis, k):
    return lax.ppermute(value, axis, [(i, (i + k) % 4) for i in range(4)])


SWAP = [(0, 1), (1, 0)]


def all_shards(rows):
    near = [rows] + [shifted(rows, "dp_0", k) for k in (1, 3, 2)]
    return near + [lax.ppermute(piece, "dp_1", SWAP) for piece in near]


def sum_of_four(value, axis):
    others = [shifted(value, axis, k) for k in (1, 2, 3)]
    return (value + others[1]) + (others[0] + others[2])


def reduce_over_rows(pieces, small):
    across, core = lax.axis_index("dp_0"), lax.axis_index("dp_1")
    pairs = pieces.reshape(4, 2, *pieces.shape[1:])
    kept = lax.dynamic_index_in_dim(pairs, core, 1, keepdims=False)
    given = lax.dynamic_index_in_dim(pairs, 1 - core, 1, keepdims=False)
    given, small = lax.optimization_barrier((given, small))
    given = lax.ppermute(given, "dp_1", SWAP)
    small = small + lax.ppermute(small, "dp_1", SWAP)
    kept = kept.astype(f32) + given.astype(f32)
    total = lax.dynamic_index_in_dim(kept, across, 0, keepdims=False)
    kept = kept.astype(bf16)
    kept, small = lax.optimization_barrier((kept, small))
    for k in (1, 2, 3):
        sent = lax.dynamic_index_in_dim(kept, (across + k) & 3, 0, keepdims=False)
        total = total + shifted(sent, "dp_0", k).astype(f32)
    small = sum_of_four(small, "dp_0")
    return lax.optimization_barrier((total.astype(bf16), small))


def program(query, latent, rope_key, gain, key_up, value_up, out_grad):
    place = lax.axis_index(SP)
    gain_row = gain[None, :]
    lat = latent[0].astype(f32)
    inv_rms = lax.rsqrt(jnp.mean(lat * lat, axis=-1, keepdims=True) + eps)
    nlat = (lat * inv_rms * gain_row).astype(bf16)
    rows = jnp.stack([key_up.reshape(4, 64, LATENT), value_up.reshape(4, 64, LATENT)], axis=1)
    rows = rows.reshape(512, LATENT)
    across, core = lax.axis_index("dp_0"), lax.axis_index("dp_1")
    shards = ((across + jnp.array([0, -1, 1, 2], jnp.int32)) & 3) * 2
    order = jnp.concatenate([shards + core, shards + 1 - core])
    by_head = rows.reshape(2, 2, 128, LATENT)
    evens = all_shards(by_head[:, 0].reshape(256, LATENT))
    odds = all_shards(by_head[:, 1].reshape(256, LATENT))
    nlat_all = lax.all_gather(nlat, SP, axis=0, tiled=True)
    mine = lax.dynamic_slice_in_dim(rows, (place // 8) * 256, 256, axis=0)
    own = lax.ppermute(mine, ALL, to_heads())

    positions = place * TOKENS + jnp.arange(TOKENS)
    cosine, sine = angles(positions)
    cos_lanes = jnp.tile(cosine, (1, 8))
    sin_lanes = jnp.tile(jnp.concatenate([-sine, sine], axis=1), (1, 4))
    key = jnp.pad(rope_key[0].astype(f32), ((0, 0), (0, 96)))
    first, second = pack(query[0], out_grad[0], key, cos_lanes, sin_lanes)
    first = lax.all_to_all(first, SP, 0, 0, tiled=True).reshape(LENGTH, 256)
    kv0 = project(order, nlat, evens, None)
    kv0 = lax.all_to_all(kv0, SP, 0, 0, tiled=True).reshape(LENGTH, 128)
    second = project(order, nlat, odds, second)
    second = lax.all_to_all(second, SP, 0, 0, tiled=True).reshape(LENGTH, 256)
    cos_all, sin_all = angles(jnp.arange(LENGTH))
    cos_all, sin_all = cos_all.T, sin_all.T
    g0 = attend(0, first, first, kv0, cos_all, sin_all)
    second, g0 = lax.optimization_barrier((second, g0))
    r0 = lax.all_to_all(g0.reshape(NSP, TOKENS, 256), SP, 0, 0, tiled=True)
    g1 = attend(1, second, first, second, cos_all, sin_all)
    r0, g1 = lax.optimization_barrier((r0, g1))
    r1 = lax.all_to_all(g1.reshape(NSP, TOKENS, 256), SP, 0, 0, tiled=True)

    parts = [
        lax.dot_general(g[:, 0:128], nlat_all, (((0,), (0,)), ((), ())), preferred_element_type=f32)
        for g in (g0, g1)
    ]
    part = jnp.concatenate(parts, axis=0)
    pieces = part.astype(bf16).reshape(2, 2, 4, 16, LATENT).transpose(0, 2, 1, 3, 4).reshape(NDP, 32, LATENT)
    gain_part = (jnp.sum(part * own.astype(f32), axis=0) / gain).reshape(8, 128)
    piece, gain_part = reduce_over_rows(pieces, gain_part)
    piece = lax.ppermute(piece, ALL, to_rows())
    gain_part = sum_of_four(gain_part, "sp_1")
    piece, gain_part = lax.optimization_barrier((piece, gain_part))
    gain_grad = sum_of_four(gain_part, "sp_0").reshape(LATENT)
    r1, piece = lax.optimization_barrier((r1, piece))
    grads = everyone(piece, SP, NSP).reshape(NSP, 2, 16, LATENT)
    key_grad = grads[:, 0].reshape(256, LATENT).astype(f32)
    value_grad = grads[:, 1].reshape(256, LATENT).astype(f32)

    dq, dlat, drope = finish(order, r0, r1, latent[0], gain_row, cos_lanes, sin_lanes, evens, odds)
    return dq[None], dlat[None], drope[None], key_grad, value_grad, gain_grad


def solution(mesh):
    split = Mesh(mesh.devices.reshape(4, 4, 4, 2), ("sp_0", "sp_1", "dp_0", "dp_1"))
    in_specs = (
        P(DP, SP, None),
        P(DP, SP, None),
        P(DP, SP, None),
        P(),
        P(DP, None),
        P(DP, None),
        P(DP, SP, None),
    )
    out_specs = (P(DP, SP, None), P(DP, SP, None), P(DP, SP, None), P(DP, None), P(DP, None), P())
    return jax.shard_map(program, mesh=split, in_specs=in_specs, out_specs=out_specs, check_vma=False)
```

```python
import functools

import jax
import jax.numpy as jnp
from jax import lax
from jax.experimental import pallas as pl
from jax.experimental.pallas import tpu as pltpu
from jax.sharding import Mesh
from jax.sharding import PartitionSpec as P

ATTENTION_HEADS = 32
PLAIN = 64
ROPE = 32
HALF = ROPE // 2
WIDTH = PLAIN + ROPE
LATENT = 1024
SPAN = 64
LENGTH = 3072
DP = ("dp_0", "dp_1")
SP = ("sp_0", "sp_1")
ALL = SP + DP
NSP = 16
NDP = 8
TOKENS = LENGTH // NSP
BLOCK = 512
SCALE = WIDTH**-0.5
LOG2E = 1.4426950408889634

eps = 1e-06
rope_base = 10000.0
f32 = jnp.float32
bf16 = jnp.bfloat16


def inverse_of(index):
    return 1.0 / rope_base ** ((2 * (index % HALF)).astype(f32) / ROPE)


def lanes_of(shape):
    return lax.broadcasted_iota(jnp.int32, shape, 1)


def pack_body(q_ref, g_ref, kr_ref, cos_ref, sin_ref, out_ref, other_ref):
    lane = lanes_of((TOKENS, 128))
    cosine = cos_ref[...]
    sine = sin_ref[...]

    def turn(x):
        inside = (lane % ROPE) < HALF
        swapped = jnp.where(inside, pltpu.roll(x, 128 - HALF, 1), pltpu.roll(x, HALF, 1))
        return x * cosine + swapped * sine

    key = turn(kr_ref[...])
    key = pltpu.roll(key, ROPE, 1)

    def emit(slot, qn0, qr0, qn1, qr1, grads):
        first = jnp.where(lane < PLAIN, qn0, pltpu.roll(grads, PLAIN, 1))
        second = jnp.where(lane < PLAIN, qn1, grads)
        third = turn(jnp.where(lane < ROPE, qr0, jnp.where(lane >= 96, qr1, 0.0)))
        third = jnp.where((lane >= ROPE) & (lane < 2 * ROPE), key, third)
        out_ref[slot, :, 0:128] = first.astype(bf16)
        out_ref[slot, :, 128:256] = third.astype(bf16)
        other_ref[slot] = second.astype(bf16)

    for pair in range(NSP // 2):
        a0, a1, a2 = [
            q_ref[:, 384 * pair + 128 * k : 384 * pair + 128 * (k + 1)].astype(f32) for k in range(3)
        ]
        g0 = g_ref[:, 256 * pair : 256 * pair + 128].astype(f32)
        g1 = g_ref[:, 256 * pair + 128 : 256 * pair + 256].astype(f32)
        qn1 = jnp.where(lane < ROPE, pltpu.roll(a0, ROPE, 1), pltpu.roll(a1, ROPE, 1))
        emit(2 * pair, a0, pltpu.roll(a0, 64, 1), qn1, pltpu.roll(a1, 64, 1), g0)
        emit(2 * pair + 1, pltpu.roll(a1, 64, 1), a2, pltpu.roll(a2, 96, 1), a2, g1)


def pack(query, grads, key, cosine, sine):
    return pl.pallas_call(
        pack_body,
        out_shape=[
            jax.ShapeDtypeStruct((NSP, TOKENS, 256), bf16),
            jax.ShapeDtypeStruct((NSP, TOKENS, 128), bf16),
        ],
        cost_estimate=pl.CostEstimate(flops=2_000_000_000, bytes_accessed=5_000_000, transcendentals=0),
        name="pack",
    )(query, grads, key, cosine, sine)


def attend_body(head, qd_ref, rt_ref, kv_ref, cos_ref, sin_ref, out_ref, p_buf, dp_buf, m_buf, kt_buf, acc, dq_acc):
    blocks = LENGTH // BLOCK
    lane = lanes_of((BLOCK, 128))
    factor = SCALE * LOG2E
    low = 0 if head == 0 else 96

    def prepare(j, carry):
        rows = pl.ds(pl.multiple_of(j * BLOCK, BLOCK), BLOCK)
        kt = kv_ref[rows, :].astype(f32).T
        rt = rt_ref[rows, :].astype(f32).T
        kt_buf[:, rows] = jnp.concatenate([kt[0:PLAIN], rt[ROPE : 2 * ROPE]], axis=0).astype(bf16)
        acc[rows, :] = jnp.zeros((BLOCK, 256), f32)
        return carry

    lax.fori_loop(0, blocks, prepare, 0)
    key_seg = lax.broadcasted_iota(jnp.int32, (BLOCK, BLOCK), 0) // SPAN
    query_seg = lax.broadcasted_iota(jnp.int32, (BLOCK, BLOCK), 1) // SPAN
    allowed = key_seg <= query_seg

    def one_block(i, carry):
        rows = pl.ds(pl.multiple_of(i * BLOCK, BLOCK), BLOCK)
        qd = qd_ref[rows, :].astype(f32)
        rt = rt_ref[rows, :].astype(f32)
        qdt = qd.T
        rtt = rt.T
        none = jnp.zeros((32, BLOCK), f32)
        left = jnp.concatenate(
            [qdt[0:PLAIN], none, none, none, rtt[low : low + ROPE], none, none], axis=0
        ).astype(bf16)
        left_d = jnp.concatenate([none, none, qdt[PLAIN:128]], axis=0).astype(bf16)
        right = jnp.concatenate(
            [jnp.where(lane < PLAIN, qd, 0.0), jnp.where((lane >= low) & (lane < low + ROPE), rt, 0.0)], axis=1
        ).astype(bf16)
        right_d = jnp.where(lane < PLAIN, 0.0, qd).astype(bf16)

        def gather_stats(j, stats, masked):
            top, total, inner = stats
            keys = pl.ds(pl.multiple_of(j * BLOCK, BLOCK), BLOCK)
            kv = kv_ref[keys, :]
            both = jnp.concatenate([kv, rt_ref[keys, :]], axis=1)
            scores = jnp.dot(both, left, preferred_element_type=f32) * factor
            if masked:
                scores = jnp.where(allowed, scores, -jnp.inf)
            d_probs = jnp.dot(kv, left_d, preferred_element_type=f32)
            new_top = jnp.maximum(top, jnp.max(scores, axis=0, keepdims=True))
            probs = jnp.exp2(scores - new_top)
            shrink = jnp.exp2(top - new_top)
            total = total * shrink + jnp.sum(probs, axis=0, keepdims=True)
            inner = inner * shrink + jnp.sum(probs * d_probs, axis=0, keepdims=True)
            p_buf[keys, :] = probs
            dp_buf[keys, :] = d_probs
            m_buf[j] = jnp.broadcast_to(new_top, (8, BLOCK))
            return new_top, total, inner

        start = (
            jnp.full((1, BLOCK), jnp.finfo(f32).min, f32),
            jnp.zeros((1, BLOCK), f32),
            jnp.zeros((1, BLOCK), f32),
        )
        stats = lax.fori_loop(0, i, functools.partial(gather_stats, masked=False), start)
        top, total, inner = gather_stats(i, stats, True)
        inverse = 1.0 / total
        inner = inner * inverse
        dq_acc[...] = jnp.zeros((WIDTH, BLOCK), f32)

        def gradients(j, carry):
            keys = pl.ds(pl.multiple_of(j * BLOCK, BLOCK), BLOCK)
            grow = jnp.exp2(m_buf[j][0:1] - top) * inverse
            probs = p_buf[keys, :] * grow
            ds = (probs * (dp_buf[keys, :] - inner)).astype(bf16)
            pb = probs.astype(bf16)
            dq_acc[...] += jnp.dot(kt_buf[:, keys], ds, preferred_element_type=f32)
            acc[keys, :] += jnp.dot(ds, right, preferred_element_type=f32)
            acc[keys, 0:128] += jnp.dot(pb, right_d, preferred_element_type=f32)
            return carry

        lax.fori_loop(0, i + 1, gradients, 0)
        dq = dq_acc[...] * SCALE
        cosine = cos_ref[:, rows]
        sine = sin_ref[:, rows]
        first, second = dq[PLAIN : PLAIN + HALF], dq[PLAIN + HALF : WIDTH]
        pieces = [dq[0:PLAIN], first * cosine + second * sine, second * cosine - first * sine]
        pieces = [none] + pieces if head == 0 else pieces + [none]
        out_ref[rows, 128:256] = jnp.concatenate(pieces, axis=0).T.astype(bf16)
        return carry

    lax.fori_loop(0, blocks, one_block, 0)

    def finish(j, carry):
        rows = pl.ds(pl.multiple_of(j * BLOCK, BLOCK), BLOCK)
        plain = acc[rows, 0:128]
        out_ref[rows, 0:128] = jnp.where(lane < PLAIN, plain * SCALE, plain).astype(bf16)
        turned = acc[rows, 128:256] * SCALE
        kept = out_ref[rows, 128:256].astype(f32)
        mine = (lane >= low) & (lane < low + ROPE)
        out_ref[rows, 128:256] = jnp.where(mine, turned, kept).astype(bf16)
        return carry

    lax.fori_loop(0, blocks, finish, 0)


def attend(head, arrived, turned, kv, cosine, sine):
    return pl.pallas_call(
        functools.partial(attend_body, head),
        grid=(1,),
        in_specs=[
            pl.BlockSpec((LENGTH, 128), lambda g: (0, 0)),
            pl.BlockSpec((LENGTH, 128), lambda g: (0, 1)),
            pl.BlockSpec((LENGTH, 128), lambda g: (0, head)),
            pl.BlockSpec((HALF, LENGTH), lambda g: (0, 0)),
            pl.BlockSpec((HALF, LENGTH), lambda g: (0, 0)),
        ],
        out_specs=pl.BlockSpec((LENGTH, 256), lambda g: (0, 0)),
        out_shape=jax.ShapeDtypeStruct((LENGTH, 256), bf16),
        scratch_shapes=[
            pltpu.VMEM((LENGTH, BLOCK), f32),
            pltpu.VMEM((LENGTH, BLOCK), f32),
            pltpu.VMEM((LENGTH // BLOCK, 8, BLOCK), f32),
            pltpu.VMEM((WIDTH, LENGTH), bf16),
            pltpu.VMEM((LENGTH, 256), f32),
            pltpu.VMEM((WIDTH, BLOCK), f32),
        ],
        compiler_params=pltpu.CompilerParams(vmem_limit_bytes=48 * 1024 * 1024),
        cost_estimate=pl.CostEstimate(
            flops=12_000_000_000, bytes_accessed=6_000_000, transcendentals=5_000_000
        ),
    )(arrived, turned, kv, cosine, sine)


def project_body(order_ref, nlat_ref, *refs):
    weights, rest = refs[:NDP], refs[NDP:]
    nlat = nlat_ref[...]
    if len(rest) == 3:
        rest[1][:, :, 0:128] = rest[0][...]
    out_ref, own_ref = rest[-2:]
    base = out_ref.shape[2] - 128
    for step in range(NDP):
        made = lax.dot_general(nlat, weights[step][...], (((1,), (1,)), ((), ())), preferred_element_type=f32)
        slot = 2 * order_ref[step]
        out_ref[slot, :, base : base + 128] = made[:, 0:128].astype(bf16)
        out_ref[slot + 1, :, base : base + 128] = made[:, 128:256].astype(bf16)
        for half in range(2):

            @pl.when(slot + half == order_ref[NDP])
            def _():
                own_ref[...] = weights[step][128 * half : 128 * half + 128, :]


def project(order, nlat, weights, extra):
    extras = [] if extra is None else [extra]
    memory = pl.BlockSpec(memory_space=pltpu.VMEM)
    return pl.pallas_call(
        project_body,
        in_specs=[pl.BlockSpec(memory_space=pltpu.SMEM)] + [memory] * (1 + NDP + len(extras)),
        out_specs=[memory, memory],
        out_shape=[
            jax.ShapeDtypeStruct((NSP, TOKENS, 128 * (1 + len(extras))), bf16),
            jax.ShapeDtypeStruct((128, LATENT), bf16),
        ],
        cost_estimate=pl.CostEstimate(flops=2_000_000_000, bytes_accessed=6_000_000, transcendentals=0),
        name="project",
    )(order, nlat, *weights, *extras)


def finish_body(order_ref, r0_ref, r1_ref, lat_ref, gain_ref, cos_ref, sin_ref, *refs):
    evens, odds = refs[:NDP], refs[NDP : 2 * NDP]
    dq_ref, dlat_ref, drope_ref, acc = refs[2 * NDP :]
    lane = lanes_of((TOKENS, 128))
    rope = jnp.zeros((TOKENS, 128), f32)
    for step in range(NDP):
        slot = 2 * order_ref[step]
        tiles = []
        for half in range(2):
            r0 = r0_ref[slot + half]
            r1 = r1_ref[slot + half]
            rows = slice(128 * half, 128 * half + 128)
            both = jnp.concatenate([r0[:, 0:128], r1[:, 0:128]], axis=1)
            weights = jnp.concatenate([evens[step][rows, :], odds[step][rows, :]], axis=0)
            added = jnp.dot(both, weights, preferred_element_type=f32)
            if step == 0 and half == 0:
                acc[...] = added
            else:
                acc[...] += added
            t0 = r0[:, 128:256].astype(f32)
            t1 = r1[:, 128:256].astype(f32)
            rope = rope + jnp.where(lane < ROPE, t0, jnp.where(lane >= 96, t1, 0.0))
            tiles.append((t0, t1))
        (x0, x1), (y0, y1) = tiles
        dq = [
            jnp.where(lane < 96, pltpu.roll(x0, 96, 1), pltpu.roll(x1, 96, 1)),
            jnp.where(lane < 64, pltpu.roll(x1, 96, 1), pltpu.roll(y0, 32, 1)),
            jnp.where(lane < 32, pltpu.roll(y0, 32, 1), pltpu.roll(y1, 32, 1)),
        ]
        start = pl.multiple_of(384 * order_ref[step], 128)
        dq_ref[:, pl.ds(start, 384)] = jnp.concatenate(dq, axis=1).astype(bf16)

    lat = lat_ref[...].astype(f32)
    inv_rms = lax.rsqrt(jnp.mean(lat * lat, axis=-1, keepdims=True) + eps)
    normed = lat * inv_rms
    scaled = acc[...] * gain_ref[...]
    dlat_ref[...] = inv_rms * (scaled - normed * jnp.mean(scaled * normed, axis=-1, keepdims=True))
    x = rope + pltpu.roll(rope, 32, 1)
    swapped = jnp.where(lane < HALF, pltpu.roll(x, 128 - HALF, 1), pltpu.roll(x, HALF, 1))
    drope_ref[...] = (x * cos_ref[...] - swapped * sin_ref[...])[:, 0:ROPE]


def finish(order, r0, r1, latent, gain, cosine, sine, evens, odds):
    memory = pl.BlockSpec(memory_space=pltpu.VMEM)
    return pl.pallas_call(
        finish_body,
        in_specs=[pl.BlockSpec(memory_space=pltpu.SMEM)] + [memory] * (6 + 2 * NDP),
        out_specs=[memory] * 3,
        out_shape=[
            jax.ShapeDtypeStruct((TOKENS, ATTENTION_HEADS * WIDTH), bf16),
            jax.ShapeDtypeStruct((TOKENS, LATENT), f32),
            jax.ShapeDtypeStruct((TOKENS, ROPE), f32),
        ],
        scratch_shapes=[pltpu.VMEM((TOKENS, LATENT), f32)],
        cost_estimate=pl.CostEstimate(flops=2_000_000_000, bytes_accessed=14_000_000, transcendentals=0),
        name="finish",
    )(order, r0, r1, latent, gain, cosine, sine, *evens, *odds)


def to_heads():
    return [(NDP * a + d, NDP * (2 * d + a // 8) + a % 8) for a in range(NSP) for d in range(NDP)]


def to_rows():
    return [(b, a) for a, b in to_heads()]


def everyone(value, axes, size):
    return lax.all_to_all(jnp.broadcast_to(value[None], (size, *value.shape)), axes, 0, 0, tiled=True)


def shifted(value, axis, k):
    return lax.ppermute(value, axis, [(i, (i + k) % 4) for i in range(4)])


SWAP = [(0, 1), (1, 0)]


def all_shards(rows):
    near = [rows] + [shifted(rows, "dp_0", k) for k in (1, 3, 2)]
    return near + [lax.ppermute(piece, "dp_1", SWAP) for piece in near]


def as_rows(value):
    top = lax.reduce_precision(value, 8, 7)
    return jnp.stack([top, lax.reduce_precision(value - top, 8, 7)] + [jnp.zeros_like(value)] * 14).astype(bf16)


def reduce_over_rows(pieces, small):
    across, core = lax.axis_index("dp_0"), lax.axis_index("dp_1")
    pairs = pieces.reshape(4, 2, *pieces.shape[1:])
    kept = lax.dynamic_index_in_dim(pairs, core, 1, keepdims=False)
    given = lax.dynamic_index_in_dim(pairs, 1 - core, 1, keepdims=False)
    extra = jnp.pad(as_rows(small)[None], ((0, 0), (0, 16), (0, 0)))
    got = lax.ppermute(jnp.concatenate([given, extra]), "dp_1", SWAP).astype(f32)
    small = small + (got[4, 0] + got[4, 1])
    kept = kept.astype(f32) + got[:4]
    extra = as_rows(small)
    arrived = []
    for k in (1, 2, 3):
        sent = lax.dynamic_index_in_dim(kept, (across + k) & 3, 0, keepdims=False).astype(bf16)
        arrived.append(shifted(jnp.concatenate([sent, extra]), "dp_0", k).astype(f32))
    total = lax.dynamic_index_in_dim(kept, across, 0, keepdims=False)
    total = (total + arrived[1][:32]) + (arrived[0][:32] + arrived[2][:32])
    others = [got[32] + got[33] for got in arrived]
    small = (small + others[1]) + (others[0] + others[2])
    return total.astype(bf16), small


def program(query, latent, rope_key, gain, key_up, value_up, out_grad):
    place = lax.axis_index(SP)
    gain_row = gain[None, :]
    lat = latent[0].astype(f32)
    inv_rms = lax.rsqrt(jnp.mean(lat * lat, axis=-1, keepdims=True) + eps)
    nlat = (lat * inv_rms * gain_row).astype(bf16)
    rows = jnp.stack([key_up.reshape(4, 64, LATENT), value_up.reshape(4, 64, LATENT)], axis=1)
    rows = rows.reshape(512, LATENT)
    across, core = lax.axis_index("dp_0"), lax.axis_index("dp_1")
    shards = ((across + jnp.array([0, -1, 1, 2], jnp.int32)) & 3) * 2
    order = jnp.concatenate([shards + core, shards + 1 - core, place[None]])
    by_head = rows.reshape(2, 2, 128, LATENT)
    evens = all_shards(by_head[:, 0].reshape(256, LATENT))
    odds = all_shards(by_head[:, 1].reshape(256, LATENT))
    lane = jnp.arange(128)
    turned = (place * TOKENS + jnp.arange(TOKENS)).astype(f32)[:, None] * inverse_of(lane)[None, :]
    cos_lanes = jnp.cos(turned)
    sin_lanes = jnp.sin(turned) * jnp.where(lane % ROPE < HALF, -1.0, 1.0)[None, :]
    key = jnp.pad(rope_key[0].astype(f32), ((0, 0), (0, 96)))
    first, second = pack(query[0], out_grad[0], key, cos_lanes, sin_lanes)
    first = lax.all_to_all(first, SP, 0, 0, tiled=True).reshape(LENGTH, 256)
    kv0, own0 = project(order, nlat, evens, None)
    late, second = lax.optimization_barrier((nlat, second))
    nlat_all = lax.all_gather(late, SP, axis=0, tiled=True)
    kv0 = lax.all_to_all(kv0, SP, 0, 0, tiled=True).reshape(LENGTH, 128)
    second, own1 = project(order, nlat, odds, second)
    second = lax.all_to_all(second, SP, 0, 0, tiled=True).reshape(LENGTH, 256)
    turned = jnp.arange(LENGTH).astype(f32)[None, :] * inverse_of(jnp.arange(HALF))[:, None]
    cos_all, sin_all = jnp.cos(turned), jnp.sin(turned)
    g0 = attend(0, first, first, kv0, cos_all, sin_all)
    second, g0 = lax.optimization_barrier((second, g0))
    r0 = lax.all_to_all(g0.reshape(NSP, TOKENS, 256), SP, 0, 0, tiled=True)
    g1 = attend(1, second, first, second, cos_all, sin_all)
    r0, g1 = lax.optimization_barrier((r0, g1))
    r1 = lax.all_to_all(g1.reshape(NSP, TOKENS, 256), SP, 0, 0, tiled=True)

    parts = [
        lax.dot_general(g[:, 0:128], nlat_all, (((0,), (0,)), ((), ())), preferred_element_type=f32)
        for g in (g0, g1)
    ]
    part = jnp.concatenate(parts, axis=0)
    pieces = part.astype(bf16).reshape(2, 2, 4, 16, LATENT).transpose(0, 2, 1, 3, 4).reshape(NDP, 32, LATENT)
    own = jnp.concatenate([own0, own1], axis=0)
    gain_part = jnp.sum(part * own.astype(f32), axis=0) / gain
    piece, gain_part = reduce_over_rows(pieces, gain_part)
    piece = lax.ppermute(piece, ALL, to_rows())
    r1, piece = lax.optimization_barrier((r1, piece))
    piece = jnp.concatenate([piece, as_rows(gain_part)])
    got = everyone(piece, SP, NSP)
    grads = got[:, :32].reshape(NSP, 2, 16, LATENT)
    gain_grad = got[:, 32:34].astype(f32).sum(axis=(0, 1))
    key_grad = grads[:, 0].reshape(256, LATENT).astype(f32)
    value_grad = grads[:, 1].reshape(256, LATENT).astype(f32)

    dq, dlat, drope = finish(order, r0, r1, latent[0], gain_row, cos_lanes, sin_lanes, evens, odds)
    return dq[None], dlat[None], drope[None], key_grad, value_grad, gain_grad


def solution(mesh):
    split = Mesh(mesh.devices.reshape(4, 4, 4, 2), ("sp_0", "sp_1", "dp_0", "dp_1"))
    in_specs = (
        P(DP, SP, None),
        P(DP, SP, None),
        P(DP, SP, None),
        P(),
        P(DP, None),
        P(DP, None),
        P(DP, SP, None),
    )
    out_specs = (P(DP, SP, None), P(DP, SP, None), P(DP, SP, None), P(DP, None), P(DP, None), P())
    return jax.shard_map(program, mesh=split, in_specs=in_specs, out_specs=out_specs, check_vma=False)
```

```python
import functools

import jax
import jax.numpy as jnp
from jax import lax
from jax.experimental import pallas as pl
from jax.experimental.pallas import tpu as pltpu
from jax.sharding import Mesh
from jax.sharding import PartitionSpec as P

ATTENTION_HEADS = 32
PLAIN = 64
ROPE = 32
HALF = ROPE // 2
WIDTH = PLAIN + ROPE
LATENT = 1024
SPAN = 64
LENGTH = 3072
DP = ("dp_0", "dp_1")
SP = ("sp_0", "sp_1")
ALL = SP + DP
NSP = 16
NDP = 8
TOKENS = LENGTH // NSP
BLOCK = 768
SCALE = WIDTH**-0.5
LOG2E = 1.4426950408889634

eps = 1e-06
rope_base = 10000.0
f32 = jnp.float32
bf16 = jnp.bfloat16


def inverse_of(index):
    return 1.0 / rope_base ** ((2 * (index % HALF)).astype(f32) / ROPE)


def lanes_of(shape):
    return lax.broadcasted_iota(jnp.int32, shape, 1)


def pack_body(q_ref, g_ref, kr_ref, cos_ref, sin_ref, out_ref, other_ref):
    lane = lanes_of((TOKENS, 128))
    cosine = cos_ref[...]
    sine = sin_ref[...]

    def turn(x):
        inside = (lane % ROPE) < HALF
        swapped = jnp.where(inside, pltpu.roll(x, 128 - HALF, 1), pltpu.roll(x, HALF, 1))
        return x * cosine + swapped * sine

    key = turn(kr_ref[...])
    key = pltpu.roll(key, ROPE, 1)

    def emit(slot, qn0, qr0, qn1, qr1, grads):
        first = jnp.where(lane < PLAIN, qn0, pltpu.roll(grads, PLAIN, 1))
        second = jnp.where(lane < PLAIN, qn1, grads)
        third = turn(jnp.where(lane < ROPE, qr0, jnp.where(lane >= 96, qr1, 0.0)))
        third = jnp.where((lane >= ROPE) & (lane < 2 * ROPE), key, third)
        out_ref[slot, :, 0:128] = first.astype(bf16)
        out_ref[slot, :, 128:256] = third.astype(bf16)
        other_ref[slot] = second.astype(bf16)

    for pair in range(NSP // 2):
        a0, a1, a2 = [
            q_ref[:, 384 * pair + 128 * k : 384 * pair + 128 * (k + 1)].astype(f32) for k in range(3)
        ]
        g0 = g_ref[:, 256 * pair : 256 * pair + 128].astype(f32)
        g1 = g_ref[:, 256 * pair + 128 : 256 * pair + 256].astype(f32)
        qn1 = jnp.where(lane < ROPE, pltpu.roll(a0, ROPE, 1), pltpu.roll(a1, ROPE, 1))
        emit(2 * pair, a0, pltpu.roll(a0, 64, 1), qn1, pltpu.roll(a1, 64, 1), g0)
        emit(2 * pair + 1, pltpu.roll(a1, 64, 1), a2, pltpu.roll(a2, 96, 1), a2, g1)


def pack(query, grads, key, cosine, sine):
    return pl.pallas_call(
        pack_body,
        out_shape=[
            jax.ShapeDtypeStruct((NSP, TOKENS, 256), bf16),
            jax.ShapeDtypeStruct((NSP, TOKENS, 128), bf16),
        ],
        cost_estimate=pl.CostEstimate(flops=2_000_000_000, bytes_accessed=5_000_000, transcendentals=0),
        name="pack",
    )(query, grads, key, cosine, sine)


def attend_body(head, qd_ref, rt_ref, kv_ref, cos_ref, sin_ref, out_ref, p_buf, dp_buf, m_buf, kt_buf, acc, dq_acc):
    blocks = LENGTH // BLOCK
    lane = lanes_of((BLOCK, 128))
    factor = SCALE * LOG2E
    low = 0 if head == 0 else 96

    def prepare(j, carry):
        rows = pl.ds(pl.multiple_of(j * BLOCK, BLOCK), BLOCK)
        kt = kv_ref[rows, :].astype(f32).T
        rt = rt_ref[rows, :].astype(f32).T
        kt_buf[:, rows] = jnp.concatenate([kt[0:PLAIN], rt[ROPE : 2 * ROPE]], axis=0).astype(bf16)
        acc[rows, :] = jnp.zeros((BLOCK, 256), f32)
        return carry

    lax.fori_loop(0, blocks, prepare, 0)

    def one_block(i, carry):
        rows = pl.ds(pl.multiple_of(i * BLOCK, BLOCK), BLOCK)
        qd = qd_ref[rows, :].astype(f32)
        rt = rt_ref[rows, :].astype(f32)
        qdt = qd.T
        rtt = rt.T
        none = jnp.zeros((32, BLOCK), f32)
        left = jnp.concatenate(
            [qdt[0:PLAIN], none, none, none, rtt[low : low + ROPE], none, none], axis=0
        ).astype(bf16)
        left_d = jnp.concatenate([none, none, qdt[PLAIN:128]], axis=0).astype(bf16)
        right = jnp.concatenate(
            [jnp.where(lane < PLAIN, qd, 0.0), jnp.where((lane >= low) & (lane < low + ROPE), rt, 0.0)], axis=1
        ).astype(bf16)
        right_d = jnp.where(lane < PLAIN, 0.0, qd).astype(bf16)

        def gather_stats(keys, j, stats, masked, columns):
            top, total, inner = stats
            kv = kv_ref[keys, :]
            both = jnp.concatenate([kv, rt_ref[keys, :]], axis=1)
            scores = jnp.dot(both, left[:, columns], preferred_element_type=f32) * factor
            if masked:
                key_seg = lax.broadcasted_iota(jnp.int32, scores.shape, 0) // SPAN
                query_seg = lax.broadcasted_iota(jnp.int32, scores.shape, 1) // SPAN
                scores = jnp.where(key_seg <= query_seg, scores, -jnp.inf)
            d_probs = jnp.dot(kv, left_d[:, columns], preferred_element_type=f32)
            new_top = jnp.maximum(top, jnp.max(scores, axis=0, keepdims=True))
            probs = jnp.exp2(scores - new_top)
            shrink = jnp.exp2(top - new_top)
            total = total * shrink + jnp.sum(probs, axis=0, keepdims=True)
            inner = inner * shrink + jnp.sum(probs * d_probs, axis=0, keepdims=True)
            p_buf[keys, columns] = probs
            dp_buf[keys, columns] = d_probs
            m_buf[j, :, columns] = jnp.broadcast_to(new_top, (8, new_top.shape[1]))
            return new_top, total, inner

        start = (
            jnp.full((1, BLOCK), jnp.finfo(f32).min, f32),
            jnp.zeros((1, BLOCK), f32),
            jnp.zeros((1, BLOCK), f32),
        )
        half = BLOCK // 2
        whole, after = slice(0, BLOCK), slice(half, BLOCK)

        def plain_stats(j, stats):
            return gather_stats(pl.ds(pl.multiple_of(j * BLOCK, BLOCK), BLOCK), j, stats, False, whole)

        upper = pl.ds(pl.multiple_of(i * BLOCK, half), half)
        lower = pl.ds(pl.multiple_of(i * BLOCK + half, half), half)
        stats = lax.fori_loop(0, i, plain_stats, start)
        stats = gather_stats(upper, i, stats, True, whole)
        later = gather_stats(lower, blocks, [x[:, half:] for x in stats], True, after)
        top, total, inner = [jnp.concatenate([x[:, :half], y], axis=1) for x, y in zip(stats, later)]
        inverse = 1.0 / total
        inner = inner * inverse
        dq_acc[...] = jnp.zeros((WIDTH, BLOCK), f32)

        def gradients(keys, j, columns):
            grow = jnp.exp2(m_buf[j, 0:1, columns] - top[:, columns]) * inverse[:, columns]
            probs = p_buf[keys, columns] * grow
            ds = (probs * (dp_buf[keys, columns] - inner[:, columns])).astype(bf16)
            pb = probs.astype(bf16)
            dq_acc[:, columns] += jnp.dot(kt_buf[:, keys], ds, preferred_element_type=f32)
            acc[keys, :] += jnp.dot(ds, right[columns], preferred_element_type=f32)
            acc[keys, 0:128] += jnp.dot(pb, right_d[columns], preferred_element_type=f32)

        def plain_gradients(j, carry):
            gradients(pl.ds(pl.multiple_of(j * BLOCK, BLOCK), BLOCK), j, whole)
            return carry

        lax.fori_loop(0, i, plain_gradients, 0)
        gradients(upper, i, whole)
        gradients(lower, blocks, after)
        dq = dq_acc[...] * SCALE
        cosine = cos_ref[:, rows]
        sine = sin_ref[:, rows]
        first, second = dq[PLAIN : PLAIN + HALF], dq[PLAIN + HALF : WIDTH]
        pieces = [dq[0:PLAIN], first * cosine + second * sine, second * cosine - first * sine]
        pieces = [none] + pieces if head == 0 else pieces + [none]
        out_ref[rows, 128:256] = jnp.concatenate(pieces, axis=0).T.astype(bf16)
        return carry

    lax.fori_loop(0, blocks, one_block, 0)

    def finish(j, carry):
        rows = pl.ds(pl.multiple_of(j * BLOCK, BLOCK), BLOCK)
        plain = acc[rows, 0:128]
        out_ref[rows, 0:128] = jnp.where(lane < PLAIN, plain * SCALE, plain).astype(bf16)
        turned = acc[rows, 128:256] * SCALE
        kept = out_ref[rows, 128:256].astype(f32)
        mine = (lane >= low) & (lane < low + ROPE)
        out_ref[rows, 128:256] = jnp.where(mine, turned, kept).astype(bf16)
        return carry

    lax.fori_loop(0, blocks, finish, 0)


def attend(head, arrived, turned, kv, cosine, sine):
    return pl.pallas_call(
        functools.partial(attend_body, head),
        grid=(1,),
        in_specs=[
            pl.BlockSpec((LENGTH, 128), lambda g: (0, 0)),
            pl.BlockSpec((LENGTH, 128), lambda g: (0, 1)),
            pl.BlockSpec((LENGTH, 128), lambda g: (0, head)),
            pl.BlockSpec((HALF, LENGTH), lambda g: (0, 0)),
            pl.BlockSpec((HALF, LENGTH), lambda g: (0, 0)),
        ],
        out_specs=pl.BlockSpec((LENGTH, 256), lambda g: (0, 0)),
        out_shape=jax.ShapeDtypeStruct((LENGTH, 256), bf16),
        scratch_shapes=[
            pltpu.VMEM((LENGTH, BLOCK), f32),
            pltpu.VMEM((LENGTH, BLOCK), f32),
            pltpu.VMEM((LENGTH // BLOCK + 1, 8, BLOCK), f32),
            pltpu.VMEM((WIDTH, LENGTH), bf16),
            pltpu.VMEM((LENGTH, 256), f32),
            pltpu.VMEM((WIDTH, BLOCK), f32),
        ],
        compiler_params=pltpu.CompilerParams(vmem_limit_bytes=60 * 1024 * 1024),
        cost_estimate=pl.CostEstimate(
            flops=12_000_000_000, bytes_accessed=6_000_000, transcendentals=5_000_000
        ),
    )(arrived, turned, kv, cosine, sine)


def project_body(order_ref, nlat_ref, *refs):
    weights, rest = refs[:NDP], refs[NDP:]
    nlat = nlat_ref[...]
    if len(rest) == 3:
        rest[1][:, :, 0:128] = rest[0][...]
    out_ref, own_ref = rest[-2:]
    base = out_ref.shape[2] - 128
    for step in range(NDP):
        made = lax.dot_general(nlat, weights[step][...], (((1,), (1,)), ((), ())), preferred_element_type=f32)
        slot = 2 * order_ref[step]
        out_ref[slot, :, base : base + 128] = made[:, 0:128].astype(bf16)
        out_ref[slot + 1, :, base : base + 128] = made[:, 128:256].astype(bf16)
        for half in range(2):

            @pl.when(slot + half == order_ref[NDP])
            def _():
                own_ref[...] = weights[step][128 * half : 128 * half + 128, :]


def project(order, nlat, weights, extra):
    extras = [] if extra is None else [extra]
    memory = pl.BlockSpec(memory_space=pltpu.VMEM)
    return pl.pallas_call(
        project_body,
        in_specs=[pl.BlockSpec(memory_space=pltpu.SMEM)] + [memory] * (1 + NDP + len(extras)),
        out_specs=[memory, memory],
        out_shape=[
            jax.ShapeDtypeStruct((NSP, TOKENS, 128 * (1 + len(extras))), bf16),
            jax.ShapeDtypeStruct((128, LATENT), bf16),
        ],
        cost_estimate=pl.CostEstimate(flops=2_000_000_000, bytes_accessed=6_000_000, transcendentals=0),
        name="project",
    )(order, nlat, *weights, *extras)


def finish_body(order_ref, r0_ref, r1_ref, lat_ref, gain_ref, cos_ref, sin_ref, *refs):
    evens, odds = refs[:NDP], refs[NDP : 2 * NDP]
    dq_ref, dlat_ref, drope_ref, acc = refs[2 * NDP :]
    lane = lanes_of((TOKENS, 128))
    rope = jnp.zeros((TOKENS, 128), f32)
    for step in range(NDP):
        slot = 2 * order_ref[step]
        tiles = []
        for half in range(2):
            r0 = r0_ref[slot + half]
            r1 = r1_ref[slot + half]
            rows = slice(128 * half, 128 * half + 128)
            both = jnp.concatenate([r0[:, 0:128], r1[:, 0:128]], axis=1)
            weights = jnp.concatenate([evens[step][rows, :], odds[step][rows, :]], axis=0)
            added = jnp.dot(both, weights, preferred_element_type=f32)
            if step == 0 and half == 0:
                acc[...] = added
            else:
                acc[...] += added
            t0 = r0[:, 128:256].astype(f32)
            t1 = r1[:, 128:256].astype(f32)
            rope = rope + jnp.where(lane < ROPE, t0, jnp.where(lane >= 96, t1, 0.0))
            tiles.append((t0, t1))
        (x0, x1), (y0, y1) = tiles
        dq = [
            jnp.where(lane < 96, pltpu.roll(x0, 96, 1), pltpu.roll(x1, 96, 1)),
            jnp.where(lane < 64, pltpu.roll(x1, 96, 1), pltpu.roll(y0, 32, 1)),
            jnp.where(lane < 32, pltpu.roll(y0, 32, 1), pltpu.roll(y1, 32, 1)),
        ]
        start = pl.multiple_of(384 * order_ref[step], 128)
        dq_ref[:, pl.ds(start, 384)] = jnp.concatenate(dq, axis=1).astype(bf16)

    lat = lat_ref[...].astype(f32)
    inv_rms = lax.rsqrt(jnp.mean(lat * lat, axis=-1, keepdims=True) + eps)
    normed = lat * inv_rms
    scaled = acc[...] * gain_ref[...]
    dlat_ref[...] = inv_rms * (scaled - normed * jnp.mean(scaled * normed, axis=-1, keepdims=True))
    x = rope + pltpu.roll(rope, 32, 1)
    swapped = jnp.where(lane < HALF, pltpu.roll(x, 128 - HALF, 1), pltpu.roll(x, HALF, 1))
    drope_ref[...] = (x * cos_ref[...] - swapped * sin_ref[...])[:, 0:ROPE]


def finish(order, r0, r1, latent, gain, cosine, sine, evens, odds):
    memory = pl.BlockSpec(memory_space=pltpu.VMEM)
    return pl.pallas_call(
        finish_body,
        in_specs=[pl.BlockSpec(memory_space=pltpu.SMEM)] + [memory] * (6 + 2 * NDP),
        out_specs=[memory] * 3,
        out_shape=[
            jax.ShapeDtypeStruct((TOKENS, ATTENTION_HEADS * WIDTH), bf16),
            jax.ShapeDtypeStruct((TOKENS, LATENT), f32),
            jax.ShapeDtypeStruct((TOKENS, ROPE), f32),
        ],
        scratch_shapes=[pltpu.VMEM((TOKENS, LATENT), f32)],
        cost_estimate=pl.CostEstimate(flops=2_000_000_000, bytes_accessed=14_000_000, transcendentals=0),
        name="finish",
    )(order, r0, r1, latent, gain, cosine, sine, *evens, *odds)


def to_heads():
    return [(NDP * a + d, NDP * (2 * d + a // 8) + a % 8) for a in range(NSP) for d in range(NDP)]


def to_rows():
    return [(b, a) for a, b in to_heads()]


def everyone(value, axes, size):
    return lax.all_to_all(jnp.broadcast_to(value[None], (size, *value.shape)), axes, 0, 0, tiled=True)


def shifted(value, axis, k):
    return lax.ppermute(value, axis, [(i, (i + k) % 4) for i in range(4)])


SWAP = [(0, 1), (1, 0)]


def all_shards(rows):
    near = [rows] + [shifted(rows, "dp_0", k) for k in (1, 3, 2)]
    return near + [lax.ppermute(piece, "dp_1", SWAP) for piece in near]


def as_rows(value):
    top = lax.reduce_precision(value, 8, 7)
    return jnp.stack([top, lax.reduce_precision(value - top, 8, 7)] + [jnp.zeros_like(value)] * 6).astype(bf16)


def reduce_over_rows(pieces, small):
    across, core = lax.axis_index("dp_0"), lax.axis_index("dp_1")
    pairs = pieces.reshape(4, 2, *pieces.shape[1:])
    kept = lax.dynamic_index_in_dim(pairs, core, 1, keepdims=False)
    given = lax.dynamic_index_in_dim(pairs, 1 - core, 1, keepdims=False)
    extra = jnp.pad(as_rows(small)[None], ((0, 0), (0, 24), (0, 0)))
    got = lax.ppermute(jnp.concatenate([given, extra]), "dp_1", SWAP).astype(f32)
    small = small + (got[4, 0] + got[4, 1])
    kept = kept.astype(f32) + got[:4]
    extra = as_rows(small)
    arrived = []
    for k in (1, 2, 3):
        sent = lax.dynamic_index_in_dim(kept, (across + k) & 3, 0, keepdims=False).astype(bf16)
        arrived.append(shifted(jnp.concatenate([sent, extra]), "dp_0", k).astype(f32))
    total = lax.dynamic_index_in_dim(kept, across, 0, keepdims=False)
    total = (total + arrived[1][:32]) + (arrived[0][:32] + arrived[2][:32])
    others = [got[32] + got[33] for got in arrived]
    small = (small + others[1]) + (others[0] + others[2])
    return total.astype(bf16), small


def program(query, latent, rope_key, gain, key_up, value_up, out_grad):
    place = lax.axis_index(SP)
    gain_row = gain[None, :]
    lat = latent[0].astype(f32)
    inv_rms = lax.rsqrt(jnp.mean(lat * lat, axis=-1, keepdims=True) + eps)
    nlat = (lat * inv_rms * gain_row).astype(bf16)
    rows = jnp.stack([key_up.reshape(4, 64, LATENT), value_up.reshape(4, 64, LATENT)], axis=1)
    rows = rows.reshape(512, LATENT)
    across, core = lax.axis_index("dp_0"), lax.axis_index("dp_1")
    shards = ((across + jnp.array([0, -1, 1, 2], jnp.int32)) & 3) * 2
    order = jnp.concatenate([shards + core, shards + 1 - core, place[None]])
    by_head = rows.reshape(2, 2, 128, LATENT)
    evens = all_shards(by_head[:, 0].reshape(256, LATENT))
    odds = all_shards(by_head[:, 1].reshape(256, LATENT))
    lane = jnp.arange(128)
    turned = (place * TOKENS + jnp.arange(TOKENS)).astype(f32)[:, None] * inverse_of(lane)[None, :]
    cos_lanes = jnp.cos(turned)
    sin_lanes = jnp.sin(turned) * jnp.where(lane % ROPE < HALF, -1.0, 1.0)[None, :]
    key = jnp.pad(rope_key[0].astype(f32), ((0, 0), (0, 96)))
    first, second = pack(query[0], out_grad[0], key, cos_lanes, sin_lanes)
    first = lax.all_to_all(first, SP, 0, 0, tiled=True).reshape(LENGTH, 256)
    kv0, own0 = project(order, nlat, evens, None)
    late, second = lax.optimization_barrier((nlat, second))
    nlat_all = lax.all_gather(late, SP, axis=0, tiled=True)
    kv0 = lax.all_to_all(kv0, SP, 0, 0, tiled=True).reshape(LENGTH, 128)
    second, own1 = project(order, nlat, odds, second)
    second = lax.all_to_all(second, SP, 0, 0, tiled=True).reshape(LENGTH, 256)
    turned = jnp.arange(LENGTH).astype(f32)[None, :] * inverse_of(jnp.arange(HALF))[:, None]
    cos_all, sin_all = jnp.cos(turned), jnp.sin(turned)
    g0 = attend(0, first, first, kv0, cos_all, sin_all)
    second, g0 = lax.optimization_barrier((second, g0))
    r0 = lax.all_to_all(g0.reshape(NSP, TOKENS, 256), SP, 0, 0, tiled=True)
    g1 = attend(1, second, first, second, cos_all, sin_all)
    r0, g1 = lax.optimization_barrier((r0, g1))
    r1 = lax.all_to_all(g1.reshape(NSP, TOKENS, 256), SP, 0, 0, tiled=True)

    parts = [
        lax.dot_general(g[:, 0:128], nlat_all, (((0,), (0,)), ((), ())), preferred_element_type=f32)
        for g in (g0, g1)
    ]
    part = jnp.concatenate(parts, axis=0)
    pieces = part.astype(bf16).reshape(2, 2, 4, 16, LATENT).transpose(0, 2, 1, 3, 4).reshape(NDP, 32, LATENT)
    own = jnp.concatenate([own0, own1], axis=0)
    gain_part = jnp.sum(part * own.astype(f32), axis=0) / gain
    piece, gain_part = reduce_over_rows(pieces, gain_part)
    piece = lax.ppermute(piece, ALL, to_rows())
    r1, piece = lax.optimization_barrier((r1, piece))
    piece = jnp.concatenate([piece, as_rows(gain_part)])
    got = everyone(piece, SP, NSP)
    grads = got[:, :32].reshape(NSP, 2, 16, LATENT)
    gain_grad = got[:, 32:34].astype(f32).sum(axis=(0, 1))
    key_grad = grads[:, 0].reshape(256, LATENT).astype(f32)
    value_grad = grads[:, 1].reshape(256, LATENT).astype(f32)

    dq, dlat, drope = finish(order, r0, r1, latent[0], gain_row, cos_lanes, sin_lanes, evens, odds)
    return dq[None], dlat[None], drope[None], key_grad, value_grad, gain_grad


def solution(mesh):
    split = Mesh(mesh.devices.reshape(4, 4, 4, 2), ("sp_0", "sp_1", "dp_0", "dp_1"))
    in_specs = (
        P(DP, SP, None),
        P(DP, SP, None),
        P(DP, SP, None),
        P(),
        P(DP, None),
        P(DP, None),
        P(DP, SP, None),
    )
    out_specs = (P(DP, SP, None), P(DP, SP, None), P(DP, SP, None), P(DP, None), P(DP, None), P())
    return jax.shard_map(program, mesh=split, in_specs=in_specs, out_specs=out_specs, check_vma=False)
```

```python
import functools

import jax
import jax.numpy as jnp
from jax import lax
from jax.experimental import pallas as pl
from jax.experimental.pallas import tpu as pltpu
from jax.sharding import Mesh
from jax.sharding import PartitionSpec as P

ATTENTION_HEADS = 32
PLAIN = 64
ROPE = 32
HALF = ROPE // 2
WIDTH = PLAIN + ROPE
LATENT = 1024
SPAN = 64
LENGTH = 3072
DP = ("dp_0", "dp_1")
SP = ("sp_0", "sp_1")
ALL = SP + DP
NSP = 16
NDP = 8
TOKENS = LENGTH // NSP
BLOCK = 768
SCALE = WIDTH**-0.5
LOG2E = 1.4426950408889634

eps = 1e-06
rope_base = 10000.0
f32 = jnp.float32
bf16 = jnp.bfloat16


def inverse_of(index):
    return 1.0 / rope_base ** ((2 * (index % HALF)).astype(f32) / ROPE)


def lanes_of(shape):
    return lax.broadcasted_iota(jnp.int32, shape, 1)


def pack_body(q_ref, g_ref, kr_ref, cos_ref, sin_ref, out_ref, other_ref):
    lane = lanes_of((TOKENS, 128))
    cosine = cos_ref[...]
    sine = sin_ref[...]

    def turn(x):
        inside = (lane % ROPE) < HALF
        swapped = jnp.where(inside, pltpu.roll(x, 128 - HALF, 1), pltpu.roll(x, HALF, 1))
        return x * cosine + swapped * sine

    key = turn(kr_ref[...])
    key = pltpu.roll(key, ROPE, 1)

    def emit(slot, qn0, qr0, qn1, qr1, grads):
        first = jnp.where(lane < PLAIN, qn0, pltpu.roll(grads, PLAIN, 1))
        second = jnp.where(lane < PLAIN, qn1, grads)
        third = turn(jnp.where(lane < ROPE, qr0, jnp.where(lane >= 96, qr1, 0.0)))
        third = jnp.where((lane >= ROPE) & (lane < 2 * ROPE), key, third)
        out_ref[slot, :, 0:128] = first.astype(bf16)
        out_ref[slot, :, 128:256] = third.astype(bf16)
        other_ref[slot] = second.astype(bf16)

    def one_pair(pair, carry):
        a0, a1, a2 = [
            q_ref[:, pl.ds(pl.multiple_of(384 * pair + 128 * k, 128), 128)].astype(f32) for k in range(3)
        ]
        g0, g1 = [g_ref[:, pl.ds(pl.multiple_of(256 * pair + 128 * k, 128), 128)].astype(f32) for k in range(2)]
        qn1 = jnp.where(lane < ROPE, pltpu.roll(a0, ROPE, 1), pltpu.roll(a1, ROPE, 1))
        emit(2 * pair, a0, pltpu.roll(a0, 64, 1), qn1, pltpu.roll(a1, 64, 1), g0)
        emit(2 * pair + 1, pltpu.roll(a1, 64, 1), a2, pltpu.roll(a2, 96, 1), a2, g1)
        return carry

    lax.fori_loop(0, NSP // 2, one_pair, 0)


def pack(query, grads, key, cosine, sine):
    return pl.pallas_call(
        pack_body,
        out_shape=[
            jax.ShapeDtypeStruct((NSP, TOKENS, 256), bf16),
            jax.ShapeDtypeStruct((NSP, TOKENS, 128), bf16),
        ],
        cost_estimate=pl.CostEstimate(flops=2_000_000_000, bytes_accessed=5_000_000, transcendentals=0),
        name="pack",
    )(query, grads, key, cosine, sine)


def attend_body(head, qd_ref, rt_ref, kv_ref, cos_ref, sin_ref, out_ref, p_buf, dp_buf, m_buf, kt_buf, acc, dq_acc):
    blocks = LENGTH // BLOCK
    lane = lanes_of((BLOCK, 128))
    factor = SCALE * LOG2E
    low = 0 if head == 0 else 96

    def prepare(j, carry):
        rows = pl.ds(pl.multiple_of(j * BLOCK, BLOCK), BLOCK)
        kt = kv_ref[rows, :].astype(f32).T
        rt = rt_ref[rows, :].astype(f32).T
        kt_buf[:, rows] = jnp.concatenate([kt[0:PLAIN], rt[ROPE : 2 * ROPE]], axis=0).astype(bf16)
        acc[rows, :] = jnp.zeros((BLOCK, 256), f32)
        return carry

    lax.fori_loop(0, blocks, prepare, 0)

    def one_block(i, carry):
        rows = pl.ds(pl.multiple_of(i * BLOCK, BLOCK), BLOCK)
        qd = qd_ref[rows, :].astype(f32)
        rt = rt_ref[rows, :].astype(f32)
        qdt = qd.T
        rtt = rt.T
        none = jnp.zeros((32, BLOCK), f32)
        left = jnp.concatenate(
            [qdt[0:PLAIN], none, none, none, rtt[low : low + ROPE], none, none], axis=0
        ).astype(bf16)
        left_d = jnp.concatenate([none, none, qdt[PLAIN:128]], axis=0).astype(bf16)
        right = jnp.concatenate(
            [jnp.where(lane < PLAIN, qd, 0.0), jnp.where((lane >= low) & (lane < low + ROPE), rt, 0.0)], axis=1
        ).astype(bf16)
        right_d = jnp.where(lane < PLAIN, 0.0, qd).astype(bf16)

        def gather_stats(keys, j, stats, masked, columns):
            top, total, inner = stats
            kv = kv_ref[keys, :]
            both = jnp.concatenate([kv, rt_ref[keys, :]], axis=1)
            scores = jnp.dot(both, left[:, columns], preferred_element_type=f32) * factor
            if masked:
                key_seg = lax.broadcasted_iota(jnp.int32, scores.shape, 0) // SPAN
                query_seg = lax.broadcasted_iota(jnp.int32, scores.shape, 1) // SPAN
                scores = jnp.where(key_seg <= query_seg, scores, -jnp.inf)
            d_probs = jnp.dot(kv, left_d[:, columns], preferred_element_type=f32)
            new_top = jnp.maximum(top, jnp.max(scores, axis=0, keepdims=True))
            probs = jnp.exp2(scores - new_top)
            shrink = jnp.exp2(top - new_top)
            total = total * shrink + jnp.sum(probs, axis=0, keepdims=True)
            inner = inner * shrink + jnp.sum(probs * d_probs, axis=0, keepdims=True)
            p_buf[keys, columns] = probs
            dp_buf[keys, columns] = d_probs
            m_buf[j, :, columns] = jnp.broadcast_to(new_top, (8, new_top.shape[1]))
            return new_top, total, inner

        start = (
            jnp.full((1, BLOCK), jnp.finfo(f32).min, f32),
            jnp.zeros((1, BLOCK), f32),
            jnp.zeros((1, BLOCK), f32),
        )
        half = BLOCK // 2
        whole, after = slice(0, BLOCK), slice(half, BLOCK)

        def plain_stats(j, stats):
            return gather_stats(pl.ds(pl.multiple_of(j * BLOCK, BLOCK), BLOCK), j, stats, False, whole)

        upper = pl.ds(pl.multiple_of(i * BLOCK, half), half)
        lower = pl.ds(pl.multiple_of(i * BLOCK + half, half), half)
        stats = lax.fori_loop(0, i, plain_stats, start)
        stats = gather_stats(upper, i, stats, True, whole)
        later = gather_stats(lower, blocks, [x[:, half:] for x in stats], True, after)
        top, total, inner = [jnp.concatenate([x[:, :half], y], axis=1) for x, y in zip(stats, later)]
        inverse = 1.0 / total
        inner = inner * inverse
        dq_acc[...] = jnp.zeros((WIDTH, BLOCK), f32)

        def gradients(keys, j, columns):
            grow = jnp.exp2(m_buf[j, 0:1, columns] - top[:, columns]) * inverse[:, columns]
            probs = p_buf[keys, columns] * grow
            ds = (probs * (dp_buf[keys, columns] - inner[:, columns])).astype(bf16)
            pb = probs.astype(bf16)
            dq_acc[:, columns] += jnp.dot(kt_buf[:, keys], ds, preferred_element_type=f32)
            acc[keys, :] += jnp.dot(ds, right[columns], preferred_element_type=f32)
            acc[keys, 0:128] += jnp.dot(pb, right_d[columns], preferred_element_type=f32)

        def plain_gradients(j, carry):
            gradients(pl.ds(pl.multiple_of(j * BLOCK, BLOCK), BLOCK), j, whole)
            return carry

        lax.fori_loop(0, i, plain_gradients, 0)
        gradients(upper, i, whole)
        gradients(lower, blocks, after)
        dq = dq_acc[...] * SCALE
        cosine = cos_ref[:, rows]
        sine = sin_ref[:, rows]
        first, second = dq[PLAIN : PLAIN + HALF], dq[PLAIN + HALF : WIDTH]
        pieces = [dq[0:PLAIN], first * cosine + second * sine, second * cosine - first * sine]
        pieces = [none] + pieces if head == 0 else pieces + [none]
        out_ref[rows, 128:256] = jnp.concatenate(pieces, axis=0).T.astype(bf16)
        return carry

    lax.fori_loop(0, blocks, one_block, 0)

    def finish(j, carry):
        rows = pl.ds(pl.multiple_of(j * BLOCK, BLOCK), BLOCK)
        plain = acc[rows, 0:128]
        out_ref[rows, 0:128] = jnp.where(lane < PLAIN, plain * SCALE, plain).astype(bf16)
        turned = acc[rows, 128:256] * SCALE
        kept = out_ref[rows, 128:256].astype(f32)
        mine = (lane >= low) & (lane < low + ROPE)
        out_ref[rows, 128:256] = jnp.where(mine, turned, kept).astype(bf16)
        return carry

    lax.fori_loop(0, blocks, finish, 0)


def attend(head, arrived, turned, kv, cosine, sine):
    return pl.pallas_call(
        functools.partial(attend_body, head),
        grid=(1,),
        in_specs=[
            pl.BlockSpec((LENGTH, 128), lambda g: (0, 0)),
            pl.BlockSpec((LENGTH, 128), lambda g: (0, 1)),
            pl.BlockSpec((LENGTH, 128), lambda g: (0, head)),
            pl.BlockSpec((HALF, LENGTH), lambda g: (0, 0)),
            pl.BlockSpec((HALF, LENGTH), lambda g: (0, 0)),
        ],
        out_specs=pl.BlockSpec((LENGTH, 256), lambda g: (0, 0)),
        out_shape=jax.ShapeDtypeStruct((LENGTH, 256), bf16),
        scratch_shapes=[
            pltpu.VMEM((LENGTH, BLOCK), f32),
            pltpu.VMEM((LENGTH, BLOCK), f32),
            pltpu.VMEM((LENGTH // BLOCK + 1, 8, BLOCK), f32),
            pltpu.VMEM((WIDTH, LENGTH), bf16),
            pltpu.VMEM((LENGTH, 256), f32),
            pltpu.VMEM((WIDTH, BLOCK), f32),
        ],
        compiler_params=pltpu.CompilerParams(vmem_limit_bytes=36 * 1024 * 1024),
        cost_estimate=pl.CostEstimate(
            flops=12_000_000_000, bytes_accessed=6_000_000, transcendentals=5_000_000
        ),
    )(arrived, turned, kv, cosine, sine)


def project_body(order_ref, nlat_ref, *refs):
    weights, rest = refs[:NDP], refs[NDP:]
    nlat = nlat_ref[...]
    if len(rest) == 3:
        rest[1][:, :, 0:128] = rest[0][...]
    out_ref, own_ref = rest[-2:]
    base = out_ref.shape[2] - 128
    for step in range(NDP):
        made = lax.dot_general(nlat, weights[step][...], (((1,), (1,)), ((), ())), preferred_element_type=f32)
        slot = 2 * order_ref[step]
        out_ref[slot, :, base : base + 128] = made[:, 0:128].astype(bf16)
        out_ref[slot + 1, :, base : base + 128] = made[:, 128:256].astype(bf16)
        for half in range(2):

            @pl.when(slot + half == order_ref[NDP])
            def _():
                own_ref[...] = weights[step][128 * half : 128 * half + 128, :]


def project(order, nlat, weights, extra):
    extras = [] if extra is None else [extra]
    memory = pl.BlockSpec(memory_space=pltpu.VMEM)
    return pl.pallas_call(
        project_body,
        in_specs=[pl.BlockSpec(memory_space=pltpu.SMEM)] + [memory] * (1 + NDP + len(extras)),
        out_specs=[memory, memory],
        out_shape=[
            jax.ShapeDtypeStruct((NSP, TOKENS, 128 * (1 + len(extras))), bf16),
            jax.ShapeDtypeStruct((128, LATENT), bf16),
        ],
        cost_estimate=pl.CostEstimate(flops=2_000_000_000, bytes_accessed=6_000_000, transcendentals=0),
        name="project",
    )(order, nlat, *weights, *extras)


def finish_body(order_ref, r0_ref, r1_ref, lat_ref, gain_ref, cos_ref, sin_ref, *refs):
    evens, odds = refs[:NDP], refs[NDP : 2 * NDP]
    dq_ref, dlat_ref, drope_ref, acc = refs[2 * NDP :]
    lane = lanes_of((TOKENS, 128))
    rope = jnp.zeros((TOKENS, 128), f32)
    for step in range(NDP):
        slot = 2 * order_ref[step]
        tiles = []
        for half in range(2):
            r0 = r0_ref[slot + half]
            r1 = r1_ref[slot + half]
            rows = slice(128 * half, 128 * half + 128)
            both = jnp.concatenate([r0[:, 0:128], r1[:, 0:128]], axis=1)
            weights = jnp.concatenate([evens[step][rows, :], odds[step][rows, :]], axis=0)
            added = jnp.dot(both, weights, preferred_element_type=f32)
            if step == 0 and half == 0:
                acc[...] = added
            else:
                acc[...] += added
            t0 = r0[:, 128:256].astype(f32)
            t1 = r1[:, 128:256].astype(f32)
            rope = rope + jnp.where(lane < ROPE, t0, jnp.where(lane >= 96, t1, 0.0))
            tiles.append((t0, t1))
        (x0, x1), (y0, y1) = tiles
        dq = [
            jnp.where(lane < 96, pltpu.roll(x0, 96, 1), pltpu.roll(x1, 96, 1)),
            jnp.where(lane < 64, pltpu.roll(x1, 96, 1), pltpu.roll(y0, 32, 1)),
            jnp.where(lane < 32, pltpu.roll(y0, 32, 1), pltpu.roll(y1, 32, 1)),
        ]
        start = pl.multiple_of(384 * order_ref[step], 128)
        dq_ref[:, pl.ds(start, 384)] = jnp.concatenate(dq, axis=1).astype(bf16)

    lat = lat_ref[...].astype(f32)
    inv_rms = lax.rsqrt(jnp.mean(lat * lat, axis=-1, keepdims=True) + eps)
    normed = lat * inv_rms
    scaled = acc[...] * gain_ref[...]
    dlat_ref[...] = inv_rms * (scaled - normed * jnp.mean(scaled * normed, axis=-1, keepdims=True))
    x = rope + pltpu.roll(rope, 32, 1)
    swapped = jnp.where(lane < HALF, pltpu.roll(x, 128 - HALF, 1), pltpu.roll(x, HALF, 1))
    drope_ref[...] = (x * cos_ref[...] - swapped * sin_ref[...])[:, 0:ROPE]


def finish(order, r0, r1, latent, gain, cosine, sine, evens, odds):
    memory = pl.BlockSpec(memory_space=pltpu.VMEM)
    return pl.pallas_call(
        finish_body,
        in_specs=[pl.BlockSpec(memory_space=pltpu.SMEM)] + [memory] * (6 + 2 * NDP),
        out_specs=[memory] * 3,
        out_shape=[
            jax.ShapeDtypeStruct((TOKENS, ATTENTION_HEADS * WIDTH), bf16),
            jax.ShapeDtypeStruct((TOKENS, LATENT), f32),
            jax.ShapeDtypeStruct((TOKENS, ROPE), f32),
        ],
        scratch_shapes=[pltpu.VMEM((TOKENS, LATENT), f32)],
        cost_estimate=pl.CostEstimate(flops=2_000_000_000, bytes_accessed=14_000_000, transcendentals=0),
        name="finish",
    )(order, r0, r1, latent, gain, cosine, sine, *evens, *odds)


def to_heads():
    return [(NDP * a + d, NDP * (2 * d + a // 8) + a % 8) for a in range(NSP) for d in range(NDP)]


def to_rows():
    return [(b, a) for a, b in to_heads()]


def everyone(value, axes, size):
    return lax.all_to_all(jnp.broadcast_to(value[None], (size, *value.shape)), axes, 0, 0, tiled=True)


def shifted(value, axis, k):
    return lax.ppermute(value, axis, [(i, (i + k) % 4) for i in range(4)])


SWAP = [(0, 1), (1, 0)]


def all_shards(rows):
    near = [rows] + [shifted(rows, "dp_0", k) for k in (1, 3, 2)]
    return near + [lax.ppermute(piece, "dp_1", SWAP) for piece in near]


def as_rows(value):
    top = lax.reduce_precision(value, 8, 7)
    return jnp.stack([top, lax.reduce_precision(value - top, 8, 7)] + [jnp.zeros_like(value)] * 6).astype(bf16)


def reduce_over_rows(pieces, small):
    across, core = lax.axis_index("dp_0"), lax.axis_index("dp_1")
    pairs = pieces.reshape(4, 2, *pieces.shape[1:])
    kept = lax.dynamic_index_in_dim(pairs, core, 1, keepdims=False)
    given = lax.dynamic_index_in_dim(pairs, 1 - core, 1, keepdims=False)
    extra = jnp.pad(as_rows(small)[None], ((0, 0), (0, 24), (0, 0)))
    got = lax.ppermute(jnp.concatenate([given, extra]), "dp_1", SWAP).astype(f32)
    small = small + (got[4, 0] + got[4, 1])
    kept = kept.astype(f32) + got[:4]
    extra = as_rows(small)
    arrived = []
    for k in (1, 2, 3):
        sent = lax.dynamic_index_in_dim(kept, (across + k) & 3, 0, keepdims=False).astype(bf16)
        arrived.append(shifted(jnp.concatenate([sent, extra]), "dp_0", k).astype(f32))
    total = lax.dynamic_index_in_dim(kept, across, 0, keepdims=False)
    total = (total + arrived[1][:32]) + (arrived[0][:32] + arrived[2][:32])
    others = [got[32] + got[33] for got in arrived]
    small = (small + others[1]) + (others[0] + others[2])
    return total.astype(bf16), small


def program(query, latent, rope_key, gain, key_up, value_up, out_grad):
    place = lax.axis_index(SP)
    gain_row = gain[None, :]
    lat = latent[0].astype(f32)
    inv_rms = lax.rsqrt(jnp.mean(lat * lat, axis=-1, keepdims=True) + eps)
    nlat = (lat * inv_rms * gain_row).astype(bf16)
    rows = jnp.stack([key_up.reshape(4, 64, LATENT), value_up.reshape(4, 64, LATENT)], axis=1)
    rows = rows.reshape(512, LATENT)
    across, core = lax.axis_index("dp_0"), lax.axis_index("dp_1")
    shards = ((across + jnp.array([0, -1, 1, 2], jnp.int32)) & 3) * 2
    order = jnp.concatenate([shards + core, shards + 1 - core, place[None]])
    by_head = rows.reshape(2, 2, 128, LATENT)
    evens = all_shards(by_head[:, 0].reshape(256, LATENT))
    odds = all_shards(by_head[:, 1].reshape(256, LATENT))
    lane = jnp.arange(128)
    turned = (place * TOKENS + jnp.arange(TOKENS)).astype(f32)[:, None] * inverse_of(lane)[None, :]
    cos_lanes = jnp.cos(turned)
    sin_lanes = jnp.sin(turned) * jnp.where(lane % ROPE < HALF, -1.0, 1.0)[None, :]
    key = jnp.pad(rope_key[0].astype(f32), ((0, 0), (0, 96)))
    first, second = pack(query[0], out_grad[0], key, cos_lanes, sin_lanes)
    first = lax.all_to_all(first, SP, 0, 0, tiled=True).reshape(LENGTH, 256)
    kv0, own0 = project(order, nlat, evens, None)
    late, second = lax.optimization_barrier((nlat, second))
    nlat_all = lax.all_gather(late, SP, axis=0, tiled=True)
    kv0 = lax.all_to_all(kv0, SP, 0, 0, tiled=True).reshape(LENGTH, 128)
    second, own1 = project(order, nlat, odds, second)
    second = lax.all_to_all(second, SP, 0, 0, tiled=True).reshape(LENGTH, 256)
    turned = jnp.arange(LENGTH).astype(f32)[None, :] * inverse_of(jnp.arange(HALF))[:, None]
    cos_all, sin_all = jnp.cos(turned), jnp.sin(turned)
    g0 = attend(0, first, first, kv0, cos_all, sin_all)
    second, g0 = lax.optimization_barrier((second, g0))
    r0 = lax.all_to_all(g0.reshape(NSP, TOKENS, 256), SP, 0, 0, tiled=True)
    g1 = attend(1, second, first, second, cos_all, sin_all)
    r0, g1 = lax.optimization_barrier((r0, g1))
    r1 = lax.all_to_all(g1.reshape(NSP, TOKENS, 256), SP, 0, 0, tiled=True)

    parts = [
        lax.dot_general(g[:, 0:128], nlat_all, (((0,), (0,)), ((), ())), preferred_element_type=f32)
        for g in (g0, g1)
    ]
    part = jnp.concatenate(parts, axis=0)
    pieces = part.astype(bf16).reshape(2, 2, 4, 16, LATENT).transpose(0, 2, 1, 3, 4).reshape(NDP, 32, LATENT)
    own = jnp.concatenate([own0, own1], axis=0)
    gain_part = jnp.sum(part * own.astype(f32), axis=0) / gain
    piece, gain_part = reduce_over_rows(pieces, gain_part)
    piece = lax.ppermute(piece, ALL, to_rows())
    r1, piece = lax.optimization_barrier((r1, piece))
    piece = jnp.concatenate([piece, as_rows(gain_part)])
    got = everyone(piece, SP, NSP)
    grads = got[:, :32].reshape(NSP, 2, 16, LATENT)
    gain_grad = got[:, 32:34].astype(f32).sum(axis=(0, 1))
    key_grad = grads[:, 0].reshape(256, LATENT).astype(f32)
    value_grad = grads[:, 1].reshape(256, LATENT).astype(f32)

    dq, dlat, drope = finish(order, r0, r1, latent[0], gain_row, cos_lanes, sin_lanes, evens, odds)
    return dq[None], dlat[None], drope[None], key_grad, value_grad, gain_grad


def solution(mesh):
    split = Mesh(mesh.devices.reshape(4, 4, 4, 2), ("sp_0", "sp_1", "dp_0", "dp_1"))
    in_specs = (
        P(DP, SP, None),
        P(DP, SP, None),
        P(DP, SP, None),
        P(),
        P(DP, None),
        P(DP, None),
        P(DP, SP, None),
    )
    out_specs = (P(DP, SP, None), P(DP, SP, None), P(DP, SP, None), P(DP, None), P(DP, None), P())
    return jax.shard_map(program, mesh=split, in_specs=in_specs, out_specs=out_specs, check_vma=False)
```

```python
import functools

import jax
import jax.numpy as jnp
from jax import lax
from jax.experimental import pallas as pl
from jax.experimental.pallas import tpu as pltpu
from jax.sharding import Mesh
from jax.sharding import PartitionSpec as P

ATTENTION_HEADS = 32
PLAIN = 64
ROPE = 32
HALF = ROPE // 2
WIDTH = PLAIN + ROPE
LATENT = 1024
SPAN = 64
LENGTH = 3072
DP = ("dp_0", "dp_1")
SP = ("sp_0", "sp_1")
ALL = SP + DP
NSP = 16
NDP = 8
TOKENS = LENGTH // NSP
BLOCK = 768
SCALE = WIDTH**-0.5
LOG2E = 1.4426950408889634

eps = 1e-06
rope_base = 10000.0
f32 = jnp.float32
bf16 = jnp.bfloat16


def inverse_of(index):
    return 1.0 / rope_base ** ((2 * (index % HALF)).astype(f32) / ROPE)


def lanes_of(shape):
    return lax.broadcasted_iota(jnp.int32, shape, 1)


def pack_body(q_ref, g_ref, kr_ref, cos_ref, sin_ref, out_ref, other_ref):
    lane = lanes_of((TOKENS, 128))
    cosine = cos_ref[...]
    sine = sin_ref[...]

    def turn(x):
        inside = (lane % ROPE) < HALF
        swapped = jnp.where(inside, pltpu.roll(x, 128 - HALF, 1), pltpu.roll(x, HALF, 1))
        return x * cosine + swapped * sine

    key = turn(kr_ref[...])
    key = pltpu.roll(key, ROPE, 1)

    def emit(slot, qn0, qr0, qn1, qr1, grads):
        first = jnp.where(lane < PLAIN, qn0, pltpu.roll(grads, PLAIN, 1))
        second = jnp.where(lane < PLAIN, qn1, grads)
        third = turn(jnp.where(lane < ROPE, qr0, jnp.where(lane >= 96, qr1, 0.0)))
        third = jnp.where((lane >= ROPE) & (lane < 2 * ROPE), key, third)
        out_ref[slot, :, 0:128] = first.astype(bf16)
        out_ref[slot, :, 128:256] = third.astype(bf16)
        other_ref[slot] = second.astype(bf16)

    def one_pair(pair, carry):
        a0, a1, a2 = [
            q_ref[:, pl.ds(pl.multiple_of(384 * pair + 128 * k, 128), 128)].astype(f32) for k in range(3)
        ]
        g0, g1 = [g_ref[:, pl.ds(pl.multiple_of(256 * pair + 128 * k, 128), 128)].astype(f32) for k in range(2)]
        qn1 = jnp.where(lane < ROPE, pltpu.roll(a0, ROPE, 1), pltpu.roll(a1, ROPE, 1))
        emit(2 * pair, a0, pltpu.roll(a0, 64, 1), qn1, pltpu.roll(a1, 64, 1), g0)
        emit(2 * pair + 1, pltpu.roll(a1, 64, 1), a2, pltpu.roll(a2, 96, 1), a2, g1)
        return carry

    lax.fori_loop(0, NSP // 2, one_pair, 0)


def pack(query, grads, key, cosine, sine):
    return pl.pallas_call(
        pack_body,
        out_shape=[
            jax.ShapeDtypeStruct((NSP, TOKENS, 256), bf16),
            jax.ShapeDtypeStruct((NSP, TOKENS, 128), bf16),
        ],
        cost_estimate=pl.CostEstimate(flops=2_000_000_000, bytes_accessed=5_000_000, transcendentals=0),
        name="pack",
    )(query, grads, key, cosine, sine)


def attend_body(head, qd_ref, rt_ref, kv_ref, cos_ref, sin_ref, out_ref, p_buf, dp_buf, m_buf, kt_buf, acc, dq_acc):
    blocks = LENGTH // BLOCK
    lane = lanes_of((BLOCK, 128))
    factor = SCALE * LOG2E
    low = 0 if head == 0 else 96

    def prepare(j, carry):
        rows = pl.ds(pl.multiple_of(j * BLOCK, BLOCK), BLOCK)
        kt = kv_ref[rows, :].astype(f32).T
        rt = rt_ref[rows, :].astype(f32).T
        kt_buf[:, rows] = jnp.concatenate([kt[0:PLAIN], rt[ROPE : 2 * ROPE]], axis=0).astype(bf16)
        acc[rows, :] = jnp.zeros((BLOCK, 256), f32)
        return carry

    lax.fori_loop(0, blocks, prepare, 0)

    def one_block(i, carry):
        rows = pl.ds(pl.multiple_of(i * BLOCK, BLOCK), BLOCK)
        qd = qd_ref[rows, :].astype(f32)
        rt = rt_ref[rows, :].astype(f32)
        qdt = qd.T
        rtt = rt.T
        none = jnp.zeros((32, BLOCK), f32)
        left = jnp.concatenate(
            [qdt[0:PLAIN], none, none, none, rtt[low : low + ROPE], none, none], axis=0
        ).astype(bf16)
        left_d = jnp.concatenate([none, none, qdt[PLAIN:128]], axis=0).astype(bf16)
        right = jnp.concatenate(
            [jnp.where(lane < PLAIN, qd, 0.0), jnp.where((lane >= low) & (lane < low + ROPE), rt, 0.0)], axis=1
        ).astype(bf16)
        right_d = jnp.where(lane < PLAIN, 0.0, qd).astype(bf16)

        def gather_stats(keys, j, stats, masked, columns):
            top, total, inner = stats
            kv = kv_ref[keys, :]
            both = jnp.concatenate([kv, rt_ref[keys, :]], axis=1)
            scores = jnp.dot(both, left[:, columns], preferred_element_type=f32) * factor
            if masked:
                key_seg = lax.broadcasted_iota(jnp.int32, scores.shape, 0) // SPAN
                query_seg = lax.broadcasted_iota(jnp.int32, scores.shape, 1) // SPAN
                scores = jnp.where(key_seg <= query_seg, scores, -jnp.inf)
            d_probs = jnp.dot(kv, left_d[:, columns], preferred_element_type=f32)
            new_top = jnp.maximum(top, jnp.max(scores, axis=0, keepdims=True))
            probs = jnp.exp2(scores - new_top)
            shrink = jnp.exp2(top - new_top)
            total = total * shrink + jnp.sum(probs, axis=0, keepdims=True)
            inner = inner * shrink + jnp.sum(probs * d_probs, axis=0, keepdims=True)
            p_buf[keys, columns] = probs
            dp_buf[keys, columns] = d_probs
            m_buf[j, :, columns] = jnp.broadcast_to(new_top, (8, new_top.shape[1]))
            return new_top, total, inner

        start = (
            jnp.full((1, BLOCK), jnp.finfo(f32).min, f32),
            jnp.zeros((1, BLOCK), f32),
            jnp.zeros((1, BLOCK), f32),
        )
        half = BLOCK // 2
        whole, after = slice(0, BLOCK), slice(half, BLOCK)

        def plain_stats(j, stats):
            return gather_stats(pl.ds(pl.multiple_of(j * BLOCK, BLOCK), BLOCK), j, stats, False, whole)

        upper = pl.ds(pl.multiple_of(i * BLOCK, half), half)
        lower = pl.ds(pl.multiple_of(i * BLOCK + half, half), half)
        stats = lax.fori_loop(0, i, plain_stats, start)
        stats = gather_stats(upper, i, stats, True, whole)
        later = gather_stats(lower, blocks, [x[:, half:] for x in stats], True, after)
        top, total, inner = [jnp.concatenate([x[:, :half], y], axis=1) for x, y in zip(stats, later)]
        inverse = 1.0 / total
        inner = inner * inverse
        dq_acc[...] = jnp.zeros((WIDTH, BLOCK), f32)

        def gradients(keys, j, columns):
            grow = jnp.exp2(m_buf[j, 0:1, columns] - top[:, columns]) * inverse[:, columns]
            probs = p_buf[keys, columns] * grow
            ds = (probs * (dp_buf[keys, columns] - inner[:, columns])).astype(bf16)
            pb = probs.astype(bf16)
            dq_acc[:, columns] += jnp.dot(kt_buf[:, keys], ds, preferred_element_type=f32)
            acc[keys, :] += jnp.dot(ds, right[columns], preferred_element_type=f32)
            acc[keys, 0:128] += jnp.dot(pb, right_d[columns], preferred_element_type=f32)

        def plain_gradients(j, carry):
            gradients(pl.ds(pl.multiple_of(j * BLOCK, BLOCK), BLOCK), j, whole)
            return carry

        lax.fori_loop(0, i, plain_gradients, 0)
        gradients(upper, i, whole)
        gradients(lower, blocks, after)
        dq = dq_acc[...] * SCALE
        cosine = cos_ref[:, rows]
        sine = sin_ref[:, rows]
        first, second = dq[PLAIN : PLAIN + HALF], dq[PLAIN + HALF : WIDTH]
        pieces = [dq[0:PLAIN], first * cosine + second * sine, second * cosine - first * sine]
        pieces = [none] + pieces if head == 0 else pieces + [none]
        out_ref[rows, 128:256] = jnp.concatenate(pieces, axis=0).T.astype(bf16)
        return carry

    lax.fori_loop(0, blocks, one_block, 0)

    def finish(j, carry):
        rows = pl.ds(pl.multiple_of(j * BLOCK, BLOCK), BLOCK)
        plain = acc[rows, 0:128]
        out_ref[rows, 0:128] = jnp.where(lane < PLAIN, plain * SCALE, plain).astype(bf16)
        turned = acc[rows, 128:256] * SCALE
        kept = out_ref[rows, 128:256].astype(f32)
        mine = (lane >= low) & (lane < low + ROPE)
        out_ref[rows, 128:256] = jnp.where(mine, turned, kept).astype(bf16)
        return carry

    lax.fori_loop(0, blocks, finish, 0)


def attend(head, arrived, turned, kv, cosine, sine):
    return pl.pallas_call(
        functools.partial(attend_body, head),
        grid=(1,),
        in_specs=[
            pl.BlockSpec((LENGTH, 128), lambda g: (0, 0)),
            pl.BlockSpec((LENGTH, 128), lambda g: (0, 1)),
            pl.BlockSpec((LENGTH, 128), lambda g: (0, head)),
            pl.BlockSpec((HALF, LENGTH), lambda g: (0, 0)),
            pl.BlockSpec((HALF, LENGTH), lambda g: (0, 0)),
        ],
        out_specs=pl.BlockSpec((LENGTH, 256), lambda g: (0, 0)),
        out_shape=jax.ShapeDtypeStruct((LENGTH, 256), bf16),
        scratch_shapes=[
            pltpu.VMEM((LENGTH, BLOCK), f32),
            pltpu.VMEM((LENGTH, BLOCK), f32),
            pltpu.VMEM((LENGTH // BLOCK + 1, 8, BLOCK), f32),
            pltpu.VMEM((WIDTH, LENGTH), bf16),
            pltpu.VMEM((LENGTH, 256), f32),
            pltpu.VMEM((WIDTH, BLOCK), f32),
        ],
        compiler_params=pltpu.CompilerParams(vmem_limit_bytes=36 * 1024 * 1024),
        cost_estimate=pl.CostEstimate(
            flops=12_000_000_000, bytes_accessed=6_000_000, transcendentals=5_000_000
        ),
    )(arrived, turned, kv, cosine, sine)


def project_body(order_ref, nlat_ref, *refs):
    weights, rest = refs[:NDP], refs[NDP:]
    nlat = nlat_ref[...]
    if len(rest) == 3:
        rest[1][:, :, 0:128] = rest[0][...]
    out_ref, own_ref = rest[-2:]
    base = out_ref.shape[2] - 128
    for step in range(NDP):
        made = lax.dot_general(nlat, weights[step][...], (((1,), (1,)), ((), ())), preferred_element_type=f32)
        slot = 2 * order_ref[step]
        out_ref[slot, :, base : base + 128] = made[:, 0:128].astype(bf16)
        out_ref[slot + 1, :, base : base + 128] = made[:, 128:256].astype(bf16)
        for half in range(2):

            @pl.when(slot + half == order_ref[NDP])
            def _():
                own_ref[...] = weights[step][128 * half : 128 * half + 128, :]


def project(order, nlat, weights, extra):
    extras = [] if extra is None else [extra]
    memory = pl.BlockSpec(memory_space=pltpu.VMEM)
    return pl.pallas_call(
        project_body,
        in_specs=[pl.BlockSpec(memory_space=pltpu.SMEM)] + [memory] * (1 + NDP + len(extras)),
        out_specs=[memory, memory],
        out_shape=[
            jax.ShapeDtypeStruct((NSP, TOKENS, 128 * (1 + len(extras))), bf16),
            jax.ShapeDtypeStruct((128, LATENT), bf16),
        ],
        cost_estimate=pl.CostEstimate(flops=2_000_000_000, bytes_accessed=6_000_000, transcendentals=0),
        name="project",
    )(order, nlat, *weights, *extras)


def finish_body(order_ref, r0_ref, r1_ref, lat_ref, gain_ref, cos_ref, sin_ref, *refs):
    evens, odds = refs[:NDP], refs[NDP : 2 * NDP]
    dq_ref, dlat_ref, drope_ref, acc = refs[2 * NDP :]
    lane = lanes_of((TOKENS, 128))
    rope = jnp.zeros((TOKENS, 128), f32)
    for step in range(NDP):
        slot = 2 * order_ref[step]
        tiles = []
        for half in range(2):
            r0 = r0_ref[slot + half]
            r1 = r1_ref[slot + half]
            rows = slice(128 * half, 128 * half + 128)
            both = jnp.concatenate([r0[:, 0:128], r1[:, 0:128]], axis=1)
            weights = jnp.concatenate([evens[step][rows, :], odds[step][rows, :]], axis=0)
            added = jnp.dot(both, weights, preferred_element_type=f32)
            if step == 0 and half == 0:
                acc[...] = added
            else:
                acc[...] += added
            t0 = r0[:, 128:256].astype(f32)
            t1 = r1[:, 128:256].astype(f32)
            rope = rope + jnp.where(lane < ROPE, t0, jnp.where(lane >= 96, t1, 0.0))
            tiles.append((t0, t1))
        (x0, x1), (y0, y1) = tiles
        dq = [
            jnp.where(lane < 96, pltpu.roll(x0, 96, 1), pltpu.roll(x1, 96, 1)),
            jnp.where(lane < 64, pltpu.roll(x1, 96, 1), pltpu.roll(y0, 32, 1)),
            jnp.where(lane < 32, pltpu.roll(y0, 32, 1), pltpu.roll(y1, 32, 1)),
        ]
        start = pl.multiple_of(384 * order_ref[step], 128)
        dq_ref[:, pl.ds(start, 384)] = jnp.concatenate(dq, axis=1).astype(bf16)

    lat = lat_ref[...].astype(f32)
    inv_rms = lax.rsqrt(jnp.mean(lat * lat, axis=-1, keepdims=True) + eps)
    normed = lat * inv_rms
    scaled = acc[...] * gain_ref[...]
    dlat_ref[...] = inv_rms * (scaled - normed * jnp.mean(scaled * normed, axis=-1, keepdims=True))
    x = rope + pltpu.roll(rope, 32, 1)
    swapped = jnp.where(lane < HALF, pltpu.roll(x, 128 - HALF, 1), pltpu.roll(x, HALF, 1))
    drope_ref[...] = (x * cos_ref[...] - swapped * sin_ref[...])[:, 0:ROPE]


def finish(order, r0, r1, latent, gain, cosine, sine, evens, odds):
    memory = pl.BlockSpec(memory_space=pltpu.VMEM)
    return pl.pallas_call(
        finish_body,
        in_specs=[pl.BlockSpec(memory_space=pltpu.SMEM)] + [memory] * (6 + 2 * NDP),
        out_specs=[memory] * 3,
        out_shape=[
            jax.ShapeDtypeStruct((TOKENS, ATTENTION_HEADS * WIDTH), bf16),
            jax.ShapeDtypeStruct((TOKENS, LATENT), f32),
            jax.ShapeDtypeStruct((TOKENS, ROPE), f32),
        ],
        scratch_shapes=[pltpu.VMEM((TOKENS, LATENT), f32)],
        cost_estimate=pl.CostEstimate(flops=2_000_000_000, bytes_accessed=14_000_000, transcendentals=0),
        name="finish",
    )(order, r0, r1, latent, gain, cosine, sine, *evens, *odds)


def weigh_body(g0_ref, g1_ref, nlat_ref, own0_ref, own1_ref, gain_ref, out_ref, small_ref, acc):
    step = pl.program_id(0)
    both = jnp.concatenate([g0_ref[...], g1_ref[...]], axis=1)
    added = lax.dot_general(both, nlat_ref[...], (((0,), (0,)), ((), ())), preferred_element_type=f32)

    @pl.when(step == 0)
    def _():
        acc[...] = added

    @pl.when(step > 0)
    def _():
        acc[...] += added

    @pl.when(step == pl.num_programs(0) - 1)
    def _():
        small = jnp.zeros((1, LATENT), f32)
        for head, own_ref in enumerate((own0_ref, own1_ref)):
            rows = slice(128 * head, 128 * head + 128)
            small = small + jnp.sum(acc[rows, :] * own_ref[...].astype(f32), axis=0, keepdims=True)
            for piece in range(4):
                for kind in range(2):
                    start = 128 * head + 64 * kind + 16 * piece
                    out_ref[4 * head + piece, 16 * kind : 16 * kind + 16] = acc[start : start + 16, :].astype(bf16)
        small_ref[...] = small / gain_ref[...]


def weigh(g0, g1, nlat_all, own0, own1, gain):
    return pl.pallas_call(
        weigh_body,
        grid=(LENGTH // BLOCK,),
        in_specs=[
            pl.BlockSpec((BLOCK, 128), lambda g: (g, 0)),
            pl.BlockSpec((BLOCK, 128), lambda g: (g, 0)),
            pl.BlockSpec((BLOCK, LATENT), lambda g: (g, 0)),
            pl.BlockSpec((128, LATENT), lambda g: (0, 0)),
            pl.BlockSpec((128, LATENT), lambda g: (0, 0)),
            pl.BlockSpec((1, LATENT), lambda g: (0, 0)),
        ],
        out_specs=[
            pl.BlockSpec((NDP, 32, LATENT), lambda g: (0, 0, 0)),
            pl.BlockSpec((1, LATENT), lambda g: (0, 0)),
        ],
        out_shape=[jax.ShapeDtypeStruct((NDP, 32, LATENT), bf16), jax.ShapeDtypeStruct((1, LATENT), f32)],
        scratch_shapes=[pltpu.VMEM((256, LATENT), f32)],
        cost_estimate=pl.CostEstimate(flops=2_000_000_000, bytes_accessed=9_000_000, transcendentals=0),
        name="weigh",
    )(g0, g1, nlat_all, own0, own1, gain)


def to_heads():
    return [(NDP * a + d, NDP * (2 * d + a // 8) + a % 8) for a in range(NSP) for d in range(NDP)]


def to_rows():
    return [(b, a) for a, b in to_heads()]


def everyone(value, axes, size):
    return lax.all_to_all(jnp.broadcast_to(value[None], (size, *value.shape)), axes, 0, 0, tiled=True)


def shifted(value, axis, k):
    return lax.ppermute(value, axis, [(i, (i + k) % 4) for i in range(4)])


SWAP = [(0, 1), (1, 0)]


def all_shards(rows):
    near = [rows] + [shifted(rows, "dp_0", k) for k in (1, 3, 2)]
    return near + [lax.ppermute(piece, "dp_1", SWAP) for piece in near]


def as_rows(value):
    top = lax.reduce_precision(value, 8, 7)
    return jnp.stack([top, lax.reduce_precision(value - top, 8, 7)] + [jnp.zeros_like(value)] * 6).astype(bf16)


def reduce_over_rows(pieces, small):
    across, core = lax.axis_index("dp_0"), lax.axis_index("dp_1")
    pairs = pieces.reshape(4, 2, *pieces.shape[1:])
    kept = lax.dynamic_index_in_dim(pairs, core, 1, keepdims=False)
    given = lax.dynamic_index_in_dim(pairs, 1 - core, 1, keepdims=False)
    extra = jnp.pad(as_rows(small)[None], ((0, 0), (0, 24), (0, 0)))
    got = lax.ppermute(jnp.concatenate([given, extra]), "dp_1", SWAP).astype(f32)
    small = small + (got[4, 0] + got[4, 1])
    kept = kept.astype(f32) + got[:4]
    extra = as_rows(small)
    arrived = []
    for k in (1, 2, 3):
        sent = lax.dynamic_index_in_dim(kept, (across + k) & 3, 0, keepdims=False).astype(bf16)
        arrived.append(shifted(jnp.concatenate([sent, extra]), "dp_0", k).astype(f32))
    total = lax.dynamic_index_in_dim(kept, across, 0, keepdims=False)
    total = (total + arrived[1][:32]) + (arrived[0][:32] + arrived[2][:32])
    others = [got[32] + got[33] for got in arrived]
    small = (small + others[1]) + (others[0] + others[2])
    return total.astype(bf16), small


def program(query, latent, rope_key, gain, key_up, value_up, out_grad):
    place = lax.axis_index(SP)
    gain_row = gain[None, :]
    lat = latent[0].astype(f32)
    inv_rms = lax.rsqrt(jnp.mean(lat * lat, axis=-1, keepdims=True) + eps)
    nlat = (lat * inv_rms * gain_row).astype(bf16)
    rows = jnp.stack([key_up.reshape(4, 64, LATENT), value_up.reshape(4, 64, LATENT)], axis=1)
    rows = rows.reshape(512, LATENT)
    across, core = lax.axis_index("dp_0"), lax.axis_index("dp_1")
    shards = ((across + jnp.array([0, -1, 1, 2], jnp.int32)) & 3) * 2
    order = jnp.concatenate([shards + core, shards + 1 - core, place[None]])
    by_head = rows.reshape(2, 2, 128, LATENT)
    evens = all_shards(by_head[:, 0].reshape(256, LATENT))
    odds = all_shards(by_head[:, 1].reshape(256, LATENT))
    lane = jnp.arange(128)
    turned = (place * TOKENS + jnp.arange(TOKENS)).astype(f32)[:, None] * inverse_of(lane)[None, :]
    cos_lanes = jnp.cos(turned)
    sin_lanes = jnp.sin(turned) * jnp.where(lane % ROPE < HALF, -1.0, 1.0)[None, :]
    key = jnp.pad(rope_key[0].astype(f32), ((0, 0), (0, 96)))
    first, second = pack(query[0], out_grad[0], key, cos_lanes, sin_lanes)
    first = lax.all_to_all(first, SP, 0, 0, tiled=True).reshape(LENGTH, 256)
    kv0, own0 = project(order, nlat, evens, None)
    late, second = lax.optimization_barrier((nlat, second))
    nlat_all = lax.all_gather(late, SP, axis=0, tiled=True)
    kv0 = lax.all_to_all(kv0, SP, 0, 0, tiled=True).reshape(LENGTH, 128)
    second, own1 = project(order, nlat, odds, second)
    second = lax.all_to_all(second, SP, 0, 0, tiled=True).reshape(LENGTH, 256)
    turned = jnp.arange(LENGTH).astype(f32)[None, :] * inverse_of(jnp.arange(HALF))[:, None]
    cos_all, sin_all = jnp.cos(turned), jnp.sin(turned)
    g0 = attend(0, first, first, kv0, cos_all, sin_all)
    second, g0 = lax.optimization_barrier((second, g0))
    r0 = lax.all_to_all(g0.reshape(NSP, TOKENS, 256), SP, 0, 0, tiled=True)
    g1 = attend(1, second, first, second, cos_all, sin_all)
    r0, g1 = lax.optimization_barrier((r0, g1))
    r1 = lax.all_to_all(g1.reshape(NSP, TOKENS, 256), SP, 0, 0, tiled=True)

    pieces, gain_part = weigh(g0, g1, nlat_all, own0, own1, gain_row)
    piece, gain_part = reduce_over_rows(pieces, gain_part[0])
    piece = lax.ppermute(piece, ALL, to_rows())
    r1, piece = lax.optimization_barrier((r1, piece))
    piece = jnp.concatenate([piece, as_rows(gain_part)])
    got = everyone(piece, SP, NSP)
    grads = got[:, :32].reshape(NSP, 2, 16, LATENT)
    gain_grad = got[:, 32:34].astype(f32).sum(axis=(0, 1))
    key_grad = grads[:, 0].reshape(256, LATENT).astype(f32)
    value_grad = grads[:, 1].reshape(256, LATENT).astype(f32)

    dq, dlat, drope = finish(order, r0, r1, latent[0], gain_row, cos_lanes, sin_lanes, evens, odds)
    return dq[None], dlat[None], drope[None], key_grad, value_grad, gain_grad


def solution(mesh):
    split = Mesh(mesh.devices.reshape(4, 4, 4, 2), ("sp_0", "sp_1", "dp_0", "dp_1"))
    in_specs = (
        P(DP, SP, None),
        P(DP, SP, None),
        P(DP, SP, None),
        P(),
        P(DP, None),
        P(DP, None),
        P(DP, SP, None),
    )
    out_specs = (P(DP, SP, None), P(DP, SP, None), P(DP, SP, None), P(DP, None), P(DP, None), P())
    return jax.shard_map(program, mesh=split, in_specs=in_specs, out_specs=out_specs, check_vma=False)
```

```python
import functools

import jax
import jax.numpy as jnp
from jax import lax
from jax.experimental import pallas as pl
from jax.experimental.pallas import tpu as pltpu
from jax.sharding import Mesh
from jax.sharding import PartitionSpec as P

ATTENTION_HEADS = 32
PLAIN = 64
ROPE = 32
HALF = ROPE // 2
WIDTH = PLAIN + ROPE
LATENT = 1024
SPAN = 64
LENGTH = 3072
DP = ("dp_0", "dp_1")
SP = ("sp_0", "sp_1")
ALL = SP + DP
NSP = 16
NDP = 8
TOKENS = LENGTH // NSP
BLOCK = 768
BLOCKS = (768, 1024)
SCALE = WIDTH**-0.5
LOG2E = 1.4426950408889634

eps = 1e-06
rope_base = 10000.0
f32 = jnp.float32
bf16 = jnp.bfloat16


def inverse_of(index):
    return 1.0 / rope_base ** ((2 * (index % HALF)).astype(f32) / ROPE)


def lanes_of(shape):
    return lax.broadcasted_iota(jnp.int32, shape, 1)


def pack_body(q_ref, g_ref, kr_ref, cos_ref, sin_ref, out_ref, other_ref):
    lane = lanes_of((TOKENS, 128))
    cosine = cos_ref[...]
    sine = sin_ref[...]

    def turn(x):
        inside = (lane % ROPE) < HALF
        swapped = jnp.where(inside, pltpu.roll(x, 128 - HALF, 1), pltpu.roll(x, HALF, 1))
        return x * cosine + swapped * sine

    key = turn(kr_ref[...])
    key = pltpu.roll(key, ROPE, 1)

    def emit(slot, qn0, qr0, qn1, qr1, grads):
        first = jnp.where(lane < PLAIN, qn0, pltpu.roll(grads, PLAIN, 1))
        second = jnp.where(lane < PLAIN, qn1, grads)
        third = turn(jnp.where(lane < ROPE, qr0, jnp.where(lane >= 96, qr1, 0.0)))
        third = jnp.where((lane >= ROPE) & (lane < 2 * ROPE), key, third)
        out_ref[slot, :, 0:128] = first.astype(bf16)
        out_ref[slot, :, 128:256] = third.astype(bf16)
        other_ref[slot] = second.astype(bf16)

    def one_pair(pair, carry):
        a0, a1, a2 = [
            q_ref[:, pl.ds(pl.multiple_of(384 * pair + 128 * k, 128), 128)].astype(f32) for k in range(3)
        ]
        g0, g1 = [g_ref[:, pl.ds(pl.multiple_of(256 * pair + 128 * k, 128), 128)].astype(f32) for k in range(2)]
        qn1 = jnp.where(lane < ROPE, pltpu.roll(a0, ROPE, 1), pltpu.roll(a1, ROPE, 1))
        emit(2 * pair, a0, pltpu.roll(a0, 64, 1), qn1, pltpu.roll(a1, 64, 1), g0)
        emit(2 * pair + 1, pltpu.roll(a1, 64, 1), a2, pltpu.roll(a2, 96, 1), a2, g1)
        return carry

    lax.fori_loop(0, NSP // 2, one_pair, 0)


def pack(query, grads, key, cosine, sine):
    return pl.pallas_call(
        pack_body,
        out_shape=[
            jax.ShapeDtypeStruct((NSP, TOKENS, 256), bf16),
            jax.ShapeDtypeStruct((NSP, TOKENS, 128), bf16),
        ],
        cost_estimate=pl.CostEstimate(flops=2_000_000_000, bytes_accessed=5_000_000, transcendentals=0),
        name="pack",
    )(query, grads, key, cosine, sine)


def attend_body(head, qd_ref, rt_ref, kv_ref, cos_ref, sin_ref, out_ref, p_buf, dp_buf, m_buf, kt_buf, acc, dq_acc):
    block = BLOCKS[head]
    blocks = LENGTH // block
    lane = lanes_of((block, 128))
    factor = SCALE * LOG2E
    low = 0 if head == 0 else 96

    def prepare(j, carry):
        rows = pl.ds(pl.multiple_of(j * block, block), block)
        kt = kv_ref[rows, :].astype(f32).T
        rt = rt_ref[rows, :].astype(f32).T
        kt_buf[:, rows] = jnp.concatenate([kt[0:PLAIN], rt[ROPE : 2 * ROPE]], axis=0).astype(bf16)
        acc[rows, :] = jnp.zeros((block, 256), f32)
        return carry

    lax.fori_loop(0, blocks, prepare, 0)

    def one_block(i, carry):
        rows = pl.ds(pl.multiple_of(i * block, block), block)
        qd = qd_ref[rows, :].astype(f32)
        rt = rt_ref[rows, :].astype(f32)
        qdt = qd.T
        rtt = rt.T
        none = jnp.zeros((32, block), f32)
        left = jnp.concatenate(
            [qdt[0:PLAIN], none, none, none, rtt[low : low + ROPE], none, none], axis=0
        ).astype(bf16)
        left_d = jnp.concatenate([none, none, qdt[PLAIN:128]], axis=0).astype(bf16)
        right = jnp.concatenate(
            [jnp.where(lane < PLAIN, qd, 0.0), jnp.where((lane >= low) & (lane < low + ROPE), rt, 0.0)], axis=1
        ).astype(bf16)
        right_d = jnp.where(lane < PLAIN, 0.0, qd).astype(bf16)

        def gather_stats(keys, j, stats, masked, columns):
            top, total, inner = stats
            kv = kv_ref[keys, :]
            both = jnp.concatenate([kv, rt_ref[keys, :]], axis=1)
            scores = jnp.dot(both, left[:, columns], preferred_element_type=f32) * factor
            if masked:
                key_seg = lax.broadcasted_iota(jnp.int32, scores.shape, 0) // SPAN
                query_seg = lax.broadcasted_iota(jnp.int32, scores.shape, 1) // SPAN
                scores = jnp.where(key_seg <= query_seg, scores, -jnp.inf)
            d_probs = jnp.dot(kv, left_d[:, columns], preferred_element_type=f32)
            new_top = jnp.maximum(top, jnp.max(scores, axis=0, keepdims=True))
            probs = jnp.exp2(scores - new_top)
            shrink = jnp.exp2(top - new_top)
            total = total * shrink + jnp.sum(probs, axis=0, keepdims=True)
            inner = inner * shrink + jnp.sum(probs * d_probs, axis=0, keepdims=True)
            p_buf[keys, columns] = probs
            dp_buf[keys, columns] = d_probs
            m_buf[j, :, columns] = jnp.broadcast_to(new_top, (8, new_top.shape[1]))
            return new_top, total, inner

        start = (
            jnp.full((1, block), jnp.finfo(f32).min, f32),
            jnp.zeros((1, block), f32),
            jnp.zeros((1, block), f32),
        )
        half = block // 2
        whole, after = slice(0, block), slice(half, block)

        def plain_stats(j, stats):
            return gather_stats(pl.ds(pl.multiple_of(j * block, block), block), j, stats, False, whole)

        upper = pl.ds(pl.multiple_of(i * block, half), half)
        lower = pl.ds(pl.multiple_of(i * block + half, half), half)
        stats = lax.fori_loop(0, i, plain_stats, start)
        stats = gather_stats(upper, i, stats, True, whole)
        later = gather_stats(lower, blocks, [x[:, half:] for x in stats], True, after)
        top, total, inner = [jnp.concatenate([x[:, :half], y], axis=1) for x, y in zip(stats, later)]
        inverse = 1.0 / total
        inner = inner * inverse
        dq_acc[...] = jnp.zeros((WIDTH, block), f32)

        def gradients(keys, j, columns):
            grow = jnp.exp2(m_buf[j, 0:1, columns] - top[:, columns]) * inverse[:, columns]
            probs = p_buf[keys, columns] * grow
            ds = (probs * (dp_buf[keys, columns] - inner[:, columns])).astype(bf16)
            pb = probs.astype(bf16)
            dq_acc[:, columns] += jnp.dot(kt_buf[:, keys], ds, preferred_element_type=f32)
            acc[keys, :] += jnp.dot(ds, right[columns], preferred_element_type=f32)
            acc[keys, 0:128] += jnp.dot(pb, right_d[columns], preferred_element_type=f32)

        def plain_gradients(j, carry):
            gradients(pl.ds(pl.multiple_of(j * block, block), block), j, whole)
            return carry

        lax.fori_loop(0, i, plain_gradients, 0)
        gradients(upper, i, whole)
        gradients(lower, blocks, after)
        dq = dq_acc[...] * SCALE
        cosine = cos_ref[:, rows]
        sine = sin_ref[:, rows]
        first, second = dq[PLAIN : PLAIN + HALF], dq[PLAIN + HALF : WIDTH]
        pieces = [dq[0:PLAIN], first * cosine + second * sine, second * cosine - first * sine]
        pieces = [none] + pieces if head == 0 else pieces + [none]
        out_ref[rows, 128:256] = jnp.concatenate(pieces, axis=0).T.astype(bf16)
        return carry

    lax.fori_loop(0, blocks, one_block, 0)

    def finish(j, carry):
        rows = pl.ds(pl.multiple_of(j * block, block), block)
        plain = acc[rows, 0:128]
        out_ref[rows, 0:128] = jnp.where(lane < PLAIN, plain * SCALE, plain).astype(bf16)
        turned = acc[rows, 128:256] * SCALE
        kept = out_ref[rows, 128:256].astype(f32)
        mine = (lane >= low) & (lane < low + ROPE)
        out_ref[rows, 128:256] = jnp.where(mine, turned, kept).astype(bf16)
        return carry

    lax.fori_loop(0, blocks, finish, 0)


def attend(head, arrived, turned, kv, cosine, sine):
    block = BLOCKS[head]
    return pl.pallas_call(
        functools.partial(attend_body, head),
        grid=(1,),
        in_specs=[
            pl.BlockSpec((LENGTH, 128), lambda g: (0, 0)),
            pl.BlockSpec((LENGTH, 128), lambda g: (0, 1)),
            pl.BlockSpec((LENGTH, 128), lambda g: (0, head)),
            pl.BlockSpec((HALF, LENGTH), lambda g: (0, 0)),
            pl.BlockSpec((HALF, LENGTH), lambda g: (0, 0)),
        ],
        out_specs=pl.BlockSpec((LENGTH, 256), lambda g: (0, 0)),
        out_shape=jax.ShapeDtypeStruct((LENGTH, 256), bf16),
        scratch_shapes=[
            pltpu.VMEM((LENGTH, block), f32),
            pltpu.VMEM((LENGTH, block), f32),
            pltpu.VMEM((LENGTH // block + 1, 8, block), f32),
            pltpu.VMEM((WIDTH, LENGTH), bf16),
            pltpu.VMEM((LENGTH, 256), f32),
            pltpu.VMEM((WIDTH, block), f32),
        ],
        compiler_params=pltpu.CompilerParams(vmem_limit_bytes=(36, 46)[head] * 1024 * 1024),
        cost_estimate=pl.CostEstimate(
            flops=12_000_000_000, bytes_accessed=6_000_000, transcendentals=5_000_000
        ),
    )(arrived, turned, kv, cosine, sine)


def project_body(order_ref, nlat_ref, *refs):
    weights, rest = refs[:NDP], refs[NDP:]
    nlat = nlat_ref[...]
    if len(rest) == 3:
        rest[1][:, :, 0:128] = rest[0][...]
    out_ref, own_ref = rest[-2:]
    base = out_ref.shape[2] - 128
    for step in range(NDP):
        made = lax.dot_general(nlat, weights[step][...], (((1,), (1,)), ((), ())), preferred_element_type=f32)
        slot = 2 * order_ref[step]
        out_ref[slot, :, base : base + 128] = made[:, 0:128].astype(bf16)
        out_ref[slot + 1, :, base : base + 128] = made[:, 128:256].astype(bf16)
        for half in range(2):

            @pl.when(slot + half == order_ref[NDP])
            def _():
                own_ref[...] = weights[step][128 * half : 128 * half + 128, :]


def project(order, nlat, weights, extra):
    extras = [] if extra is None else [extra]
    memory = pl.BlockSpec(memory_space=pltpu.VMEM)
    return pl.pallas_call(
        project_body,
        in_specs=[pl.BlockSpec(memory_space=pltpu.SMEM)] + [memory] * (1 + NDP + len(extras)),
        out_specs=[memory, memory],
        out_shape=[
            jax.ShapeDtypeStruct((NSP, TOKENS, 128 * (1 + len(extras))), bf16),
            jax.ShapeDtypeStruct((128, LATENT), bf16),
        ],
        cost_estimate=pl.CostEstimate(flops=2_000_000_000, bytes_accessed=6_000_000, transcendentals=0),
        name="project",
    )(order, nlat, *weights, *extras)


def finish_body(order_ref, r0_ref, r1_ref, lat_ref, gain_ref, cos_ref, sin_ref, *refs):
    evens, odds = refs[:NDP], refs[NDP : 2 * NDP]
    dq_ref, dlat_ref, drope_ref, acc = refs[2 * NDP :]
    lane = lanes_of((TOKENS, 128))
    rope = jnp.zeros((TOKENS, 128), f32)
    for step in range(NDP):
        slot = 2 * order_ref[step]
        tiles = []
        for half in range(2):
            r0 = r0_ref[slot + half]
            r1 = r1_ref[slot + half]
            rows = slice(128 * half, 128 * half + 128)
            both = jnp.concatenate([r0[:, 0:128], r1[:, 0:128]], axis=1)
            weights = jnp.concatenate([evens[step][rows, :], odds[step][rows, :]], axis=0)
            added = jnp.dot(both, weights, preferred_element_type=f32)
            if step == 0 and half == 0:
                acc[...] = added
            else:
                acc[...] += added
            t0 = r0[:, 128:256].astype(f32)
            t1 = r1[:, 128:256].astype(f32)
            rope = rope + jnp.where(lane < ROPE, t0, jnp.where(lane >= 96, t1, 0.0))
            tiles.append((t0, t1))
        (x0, x1), (y0, y1) = tiles
        dq = [
            jnp.where(lane < 96, pltpu.roll(x0, 96, 1), pltpu.roll(x1, 96, 1)),
            jnp.where(lane < 64, pltpu.roll(x1, 96, 1), pltpu.roll(y0, 32, 1)),
            jnp.where(lane < 32, pltpu.roll(y0, 32, 1), pltpu.roll(y1, 32, 1)),
        ]
        start = pl.multiple_of(384 * order_ref[step], 128)
        dq_ref[:, pl.ds(start, 384)] = jnp.concatenate(dq, axis=1).astype(bf16)

    lat = lat_ref[...].astype(f32)
    inv_rms = lax.rsqrt(jnp.mean(lat * lat, axis=-1, keepdims=True) + eps)
    normed = lat * inv_rms
    scaled = acc[...] * gain_ref[...]
    dlat_ref[...] = inv_rms * (scaled - normed * jnp.mean(scaled * normed, axis=-1, keepdims=True))
    x = rope + pltpu.roll(rope, 32, 1)
    swapped = jnp.where(lane < HALF, pltpu.roll(x, 128 - HALF, 1), pltpu.roll(x, HALF, 1))
    drope_ref[...] = (x * cos_ref[...] - swapped * sin_ref[...])[:, 0:ROPE]


def finish(order, r0, r1, latent, gain, cosine, sine, evens, odds):
    memory = pl.BlockSpec(memory_space=pltpu.VMEM)
    return pl.pallas_call(
        finish_body,
        in_specs=[pl.BlockSpec(memory_space=pltpu.SMEM)] + [memory] * (6 + 2 * NDP),
        out_specs=[memory] * 3,
        out_shape=[
            jax.ShapeDtypeStruct((TOKENS, ATTENTION_HEADS * WIDTH), bf16),
            jax.ShapeDtypeStruct((TOKENS, LATENT), f32),
            jax.ShapeDtypeStruct((TOKENS, ROPE), f32),
        ],
        scratch_shapes=[pltpu.VMEM((TOKENS, LATENT), f32)],
        cost_estimate=pl.CostEstimate(flops=2_000_000_000, bytes_accessed=14_000_000, transcendentals=0),
        name="finish",
    )(order, r0, r1, latent, gain, cosine, sine, *evens, *odds)


def weigh_body(g0_ref, g1_ref, nlat_ref, own0_ref, own1_ref, gain_ref, out_ref, small_ref, acc):
    step = pl.program_id(0)
    both = jnp.concatenate([g0_ref[...], g1_ref[...]], axis=1)
    added = lax.dot_general(both, nlat_ref[...], (((0,), (0,)), ((), ())), preferred_element_type=f32)

    @pl.when(step == 0)
    def _():
        acc[...] = added

    @pl.when(step > 0)
    def _():
        acc[...] += added

    @pl.when(step == pl.num_programs(0) - 1)
    def _():
        small = jnp.zeros((1, LATENT), f32)
        for head, own_ref in enumerate((own0_ref, own1_ref)):
            rows = slice(128 * head, 128 * head + 128)
            small = small + jnp.sum(acc[rows, :] * own_ref[...].astype(f32), axis=0, keepdims=True)
            for piece in range(4):
                for kind in range(2):
                    start = 128 * head + 64 * kind + 16 * piece
                    out_ref[4 * head + piece, 16 * kind : 16 * kind + 16] = acc[start : start + 16, :].astype(bf16)
        small_ref[...] = small / gain_ref[...]


def weigh(g0, g1, nlat_all, own0, own1, gain):
    return pl.pallas_call(
        weigh_body,
        grid=(LENGTH // BLOCK,),
        in_specs=[
            pl.BlockSpec((BLOCK, 128), lambda g: (g, 0)),
            pl.BlockSpec((BLOCK, 128), lambda g: (g, 0)),
            pl.BlockSpec((BLOCK, LATENT), lambda g: (g, 0)),
            pl.BlockSpec((128, LATENT), lambda g: (0, 0)),
            pl.BlockSpec((128, LATENT), lambda g: (0, 0)),
            pl.BlockSpec((1, LATENT), lambda g: (0, 0)),
        ],
        out_specs=[
            pl.BlockSpec((NDP, 32, LATENT), lambda g: (0, 0, 0)),
            pl.BlockSpec((1, LATENT), lambda g: (0, 0)),
        ],
        out_shape=[jax.ShapeDtypeStruct((NDP, 32, LATENT), bf16), jax.ShapeDtypeStruct((1, LATENT), f32)],
        scratch_shapes=[pltpu.VMEM((256, LATENT), f32)],
        cost_estimate=pl.CostEstimate(flops=2_000_000_000, bytes_accessed=9_000_000, transcendentals=0),
        name="weigh",
    )(g0, g1, nlat_all, own0, own1, gain)


def to_heads():
    return [(NDP * a + d, NDP * (2 * d + a // 8) + a % 8) for a in range(NSP) for d in range(NDP)]


def to_rows():
    return [(b, a) for a, b in to_heads()]


def everyone(value, axes, size):
    return lax.all_to_all(jnp.broadcast_to(value[None], (size, *value.shape)), axes, 0, 0, tiled=True)


def shifted(value, axis, k):
    return lax.ppermute(value, axis, [(i, (i + k) % 4) for i in range(4)])


SWAP = [(0, 1), (1, 0)]


def all_shards(rows):
    near = [rows] + [shifted(rows, "dp_0", k) for k in (1, 3, 2)]
    return near + [lax.ppermute(piece, "dp_1", SWAP) for piece in near]


def as_rows(value):
    top = lax.reduce_precision(value, 8, 7)
    return jnp.stack([top, lax.reduce_precision(value - top, 8, 7)] + [jnp.zeros_like(value)] * 6).astype(bf16)


def reduce_over_rows(pieces, small):
    across, core = lax.axis_index("dp_0"), lax.axis_index("dp_1")
    pairs = pieces.reshape(4, 2, *pieces.shape[1:])
    kept = lax.dynamic_index_in_dim(pairs, core, 1, keepdims=False)
    given = lax.dynamic_index_in_dim(pairs, 1 - core, 1, keepdims=False)
    extra = jnp.pad(as_rows(small)[None], ((0, 0), (0, 24), (0, 0)))
    got = lax.ppermute(jnp.concatenate([given, extra]), "dp_1", SWAP).astype(f32)
    small = small + (got[4, 0] + got[4, 1])
    kept = kept.astype(f32) + got[:4]
    extra = as_rows(small)
    arrived = []
    for k in (1, 2, 3):
        sent = lax.dynamic_index_in_dim(kept, (across + k) & 3, 0, keepdims=False).astype(bf16)
        arrived.append(shifted(jnp.concatenate([sent, extra]), "dp_0", k).astype(f32))
    total = lax.dynamic_index_in_dim(kept, across, 0, keepdims=False)
    total = (total + arrived[1][:32]) + (arrived[0][:32] + arrived[2][:32])
    others = [got[32] + got[33] for got in arrived]
    small = (small + others[1]) + (others[0] + others[2])
    return total.astype(bf16), small


def program(query, latent, rope_key, gain, key_up, value_up, out_grad):
    place = lax.axis_index(SP)
    gain_row = gain[None, :]
    lat = latent[0].astype(f32)
    inv_rms = lax.rsqrt(jnp.mean(lat * lat, axis=-1, keepdims=True) + eps)
    nlat = (lat * inv_rms * gain_row).astype(bf16)
    rows = jnp.stack([key_up.reshape(4, 64, LATENT), value_up.reshape(4, 64, LATENT)], axis=1)
    rows = rows.reshape(512, LATENT)
    across, core = lax.axis_index("dp_0"), lax.axis_index("dp_1")
    shards = ((across + jnp.array([0, -1, 1, 2], jnp.int32)) & 3) * 2
    order = jnp.concatenate([shards + core, shards + 1 - core, place[None]])
    by_head = rows.reshape(2, 2, 128, LATENT)
    evens = all_shards(by_head[:, 0].reshape(256, LATENT))
    odds = all_shards(by_head[:, 1].reshape(256, LATENT))
    lane = jnp.arange(128)
    turned = (place * TOKENS + jnp.arange(TOKENS)).astype(f32)[:, None] * inverse_of(lane)[None, :]
    cos_lanes = jnp.cos(turned)
    sin_lanes = jnp.sin(turned) * jnp.where(lane % ROPE < HALF, -1.0, 1.0)[None, :]
    key = jnp.pad(rope_key[0].astype(f32), ((0, 0), (0, 96)))
    first, second = pack(query[0], out_grad[0], key, cos_lanes, sin_lanes)
    first = lax.all_to_all(first, SP, 0, 0, tiled=True).reshape(LENGTH, 256)
    kv0, own0 = project(order, nlat, evens, None)
    late, second = lax.optimization_barrier((nlat, second))
    nlat_all = lax.all_gather(late, SP, axis=0, tiled=True)
    kv0 = lax.all_to_all(kv0, SP, 0, 0, tiled=True).reshape(LENGTH, 128)
    second, own1 = project(order, nlat, odds, second)
    second = lax.all_to_all(second, SP, 0, 0, tiled=True).reshape(LENGTH, 256)
    turned = jnp.arange(LENGTH).astype(f32)[None, :] * inverse_of(jnp.arange(HALF))[:, None]
    cos_all, sin_all = jnp.cos(turned), jnp.sin(turned)
    g0 = attend(0, first, first, kv0, cos_all, sin_all)
    second, g0 = lax.optimization_barrier((second, g0))
    r0 = lax.all_to_all(g0.reshape(NSP, TOKENS, 256), SP, 0, 0, tiled=True)
    g1 = attend(1, second, first, second, cos_all, sin_all)
    r0, g1 = lax.optimization_barrier((r0, g1))
    r1 = lax.all_to_all(g1.reshape(NSP, TOKENS, 256), SP, 0, 0, tiled=True)

    pieces, gain_part = weigh(g0, g1, nlat_all, own0, own1, gain_row)
    piece, gain_part = reduce_over_rows(pieces, gain_part[0])
    piece = lax.ppermute(piece, ALL, to_rows())
    r1, piece = lax.optimization_barrier((r1, piece))
    piece = jnp.concatenate([piece, as_rows(gain_part)])
    got = everyone(piece, SP, NSP)
    grads = got[:, :32].reshape(NSP, 2, 16, LATENT)
    gain_grad = got[:, 32:34].astype(f32).sum(axis=(0, 1))
    key_grad = grads[:, 0].reshape(256, LATENT).astype(f32)
    value_grad = grads[:, 1].reshape(256, LATENT).astype(f32)

    dq, dlat, drope = finish(order, r0, r1, latent[0], gain_row, cos_lanes, sin_lanes, evens, odds)
    return dq[None], dlat[None], drope[None], key_grad, value_grad, gain_grad


def solution(mesh):
    split = Mesh(mesh.devices.reshape(4, 4, 4, 2), ("sp_0", "sp_1", "dp_0", "dp_1"))
    in_specs = (
        P(DP, SP, None),
        P(DP, SP, None),
        P(DP, SP, None),
        P(),
        P(DP, None),
        P(DP, None),
        P(DP, SP, None),
    )
    out_specs = (P(DP, SP, None), P(DP, SP, None), P(DP, SP, None), P(DP, None), P(DP, None), P())
    return jax.shard_map(program, mesh=split, in_specs=in_specs, out_specs=out_specs, check_vma=False)
```
